32 devices in a mesh: sp: 16 (over z, y, x), tp: 2 (over core).
Axes of the slice: x: 2, y: 2, z: 4, core: 2. Of those that a mesh axis runs over, the one named last changes fastest.
Arguments:
- tokens: bfloat16 [4096, 2048], P(('sp', 'tp')), may hold values from -6 to 6
- gain: float32 [2048], replicated, may hold values from 0.1 to 1.9
- w_ret_q: bfloat16 [2048, 2048], P(None, 'tp'), may hold values from -0.125 to 0.125
- w_ret_k: bfloat16 [2048, 2048], P(None, 'tp'), may hold values from -0.125 to 0.125
- w_ret_v: bfloat16 [2048, 2048], P(None, 'tp'), may hold values from -0.125 to 0.125
- w_fox_q: bfloat16 [2048, 1024], P(None, 'tp'), may hold values from -0.125 to 0.125
- w_fox_k: bfloat16 [2048, 1024], P(None, 'tp'), may hold values from -0.125 to 0.125
- w_fox_v: bfloat16 [2048, 1024], P(None, 'tp'), may hold values from -0.125 to 0.125
- fox_gates: float32 [4096, 8], P('sp', 'tp'), may hold values from -4096 to 0, as said below
- w_out_ret: bfloat16 [2048, 2048], P('tp', 'sp'), may hold values from -0.109375 to 0.109375
- w_out_fox: bfloat16 [1024, 2048], P('tp', 'sp'), may hold values from -0.109375 to 0.109375
Outputs:
- mixed: bfloat16 [4096, 2048], P(('sp', 'tp'))
The draws below stay inside these ranges and needn't reach their ends.
Inputs may be any that keep to these rules, and one draw needn't show every extreme that they name: `fox_gates`: each head's values never rise along positions.
All inputs are finite; a program needn't handle non-finite values.
Results may differ from the reference program's by a relative error of at most 0.02.
Values may be sent and summed in bfloat16 or wider, within the bound.
A program may use at most 128 MiB of HBM per device.

```python
import math
import jax
import jax.numpy as jnp
from jax import lax

D = 2048
RET_HEADS = 8
RET_DIM = 256
FORGET_HEADS = 8
FOX_DIM = 128
BLOCK = 128
TOK_DEV = 256
SEQUENCE_TOKENS = 4096
N_TP = 2


def draw_fox_gates(key, part):
    ranking = jax.random.permutation(jax.random.fold_in(key, 11), FORGET_HEADS)
    slow_heads = ranking < FORGET_HEADS // 2
    roughness = jax.random.uniform(jax.random.fold_in(key, 14), (SEQUENCE_TOKENS, FORGET_HEADS), jnp.float32, 0.5, 1.5)
    fast_rate = 1.0 / jax.random.uniform(jax.random.fold_in(key, 12), (FORGET_HEADS,), jnp.float32, 30.0, 50.0)
    slow_rate = jax.random.uniform(jax.random.fold_in(key, 13), (FORGET_HEADS,), jnp.float32, 0.1, 0.4) / SEQUENCE_TOKENS
    base_rate = jnp.where(slow_heads, slow_rate, fast_rate)
    block_count = SEQUENCE_TOKENS // TOK_DEV
    block_factor = jnp.exp(jax.random.uniform(jax.random.fold_in(key, 15), (block_count, FORGET_HEADS), jnp.float32, 0.0, math.log(4.0)))
    block_factor = jnp.repeat(block_factor, TOK_DEV, axis=0)
    forget_strength = base_rate[None, :] * roughness * block_factor
    spike_locations = jax.random.randint(jax.random.fold_in(key, 16), (2, FORGET_HEADS), 0, SEQUENCE_TOKENS)
    token_positions = jnp.arange(SEQUENCE_TOKENS, dtype=jnp.int32)
    spike_mask = jnp.any(token_positions[None, :, None] == spike_locations[:, None, :], axis=0)
    retain_fraction = jax.random.uniform(jax.random.fold_in(key, 17), (SEQUENCE_TOKENS, FORGET_HEADS), jnp.float32, 0.5, 0.8)
    forget_strength = forget_strength + jnp.where(spike_mask, -jnp.log(retain_fraction), 0.0)
    return -jnp.cumsum(forget_strength, axis=0)


def block_scale(key, dims, pieces, smallest, high):
    factor_of, own = 1.0, jax.random.fold_in(key, 6)
    for position, parts in pieces:
        draws = jnp.exp(jax.random.uniform(jax.random.fold_in(own, position), (parts,), jnp.float32, smallest / len(pieces), high / len(pieces)))
        factor_of = factor_of * jnp.repeat(draws, dims[position] // parts).reshape([-1 if axis == position else 1 for axis in range(len(dims))])
    return factor_of


def bell_draw(rng, dims, scale, limit, split=(), kind=jnp.bfloat16):
    result = scale * jax.random.normal(rng, dims, jnp.float32)
    if split:
        result = result * block_scale(rng, dims, split, -0.22, 0.18)
    return jnp.clip(result, -limit, limit).astype(kind)


def setup_inputs(seed: int = 0) -> dict:
    splits = jax.random.split(jax.random.key(seed), 12)
    return {
        "tokens": bell_draw(splits[0], (SEQUENCE_TOKENS, D), 1.0, 6.0, ((0, 32),)),
        "gain": jnp.clip(1.0 + 0.18 * jax.random.normal(splits[1], (D,), jnp.float32), 0.1, 1.9),
        "w_ret_q": bell_draw(splits[2], (D, RET_HEADS * RET_DIM), D ** -0.5, 0.125, ((1, 2),)),
        "w_ret_k": bell_draw(splits[3], (D, RET_HEADS * RET_DIM), D ** -0.5, 0.125, ((1, 2),)),
        "w_ret_v": bell_draw(splits[4], (D, RET_HEADS * RET_DIM), D ** -0.5, 0.125, ((1, 2),)),
        "w_fox_q": bell_draw(splits[5], (D, FORGET_HEADS * FOX_DIM), D ** -0.5, 0.125, ((1, 2),)),
        "w_fox_k": bell_draw(splits[6], (D, FORGET_HEADS * FOX_DIM), D ** -0.5, 0.125, ((1, 2),)),
        "w_fox_v": bell_draw(splits[7], (D, FORGET_HEADS * FOX_DIM), D ** -0.5, 0.125, ((1, 2),)),
        "fox_gates": draw_fox_gates(jax.random.fold_in(splits[11], 71), 0),
        "w_out_ret": bell_draw(splits[9], (RET_HEADS * RET_DIM, D), (RET_HEADS * RET_DIM + FORGET_HEADS * FOX_DIM) ** -0.5, 0.109375, ((0, 2), (1, 16))),
        "w_out_fox": bell_draw(splits[10], (FORGET_HEADS * FOX_DIM, D), (RET_HEADS * RET_DIM + FORGET_HEADS * FOX_DIM) ** -0.5, 0.109375, ((0, 2), (1, 16))),
    }


eps = 1e-06

def to_half(values):
    return lax.optimization_barrier(values.astype(jnp.bfloat16))

def head_norm(values, width):
    rows_here = values.shape[0]
    grouped = values.reshape(rows_here, -1, width)
    scaled = grouped * lax.rsqrt(lax.optimization_barrier(jnp.mean(grouped * grouped, axis=2, keepdims=True)) + eps)
    return scaled.reshape(rows_here, -1).astype(jnp.bfloat16)

def rotate(values, token_positions, width):
    rows_here = values.shape[0]
    half_width = width // 2
    inverse = 10000.0 ** (-jnp.arange(half_width, dtype=jnp.float32) / half_width)
    angles = token_positions.astype(jnp.float32)[:, None] * inverse[None, :]
    cosine = jnp.cos(angles)[:, None, :]
    sine = jnp.sin(angles)[:, None, :]
    grouped = values.astype(jnp.float32).reshape(rows_here, -1, width)
    first_half = grouped[..., :half_width]
    second_half = grouped[..., half_width:]
    turned = jnp.concatenate([first_half * cosine - second_half * sine, first_half * sine + second_half * cosine], axis=-1)
    return turned.reshape(rows_here, -1)

def decay_rates(head_ids, total):
    heads_float = head_ids.astype(jnp.float32)
    middle = RET_HEADS // 2
    fast_rate = 1.0 / (32.0 + 16.0 * heads_float)
    slow_rate = jnp.exp2(-(heads_float - middle)) / total
    return jnp.where(head_ids < middle, fast_rate, slow_rate)

def decay_tables(rates):
    offsets = jnp.arange(BLOCK, dtype=jnp.float32)
    spread = offsets[:, None] - offsets[None, :]
    causal = spread >= 0
    within = jnp.where(causal[None], jnp.exp(-rates[:, None, None] * jnp.where(causal, spread, 0.0)[None]), 0.0)
    query_decay = jnp.exp(-rates[None, :] * (offsets[:, None] + 1.0))
    key_decay = jnp.exp(-rates[None, :] * (BLOCK - 1.0 - offsets[:, None]))
    block_decay = jnp.exp(-rates * BLOCK)
    return (within, query_decay, key_decay, block_decay)

def retention(queries, keys, values, rates):
    heads = RET_HEADS
    within, query_decay, key_decay, block_decay = decay_tables(rates)
    count = queries.shape[0] // BLOCK

    def shaped(array):
        return array.astype(jnp.float32).reshape(count, BLOCK, heads, RET_DIM)

    def step(carry, blocks):
        query_block, key_block, value_block = blocks
        scores = jnp.einsum('thd,shd->hts', query_block, key_block, precision=lax.Precision.HIGHEST) * within
        inner = jnp.einsum('hts,she->the', to_half(scores).astype(jnp.float32), value_block, precision=lax.Precision.HIGHEST)
        cross = jnp.einsum('thd,hde->the', query_block, carry, precision=lax.Precision.HIGHEST) * query_decay[:, :, None]
        scaled = to_half(key_block * key_decay[:, :, None]).astype(jnp.float32)
        new_state = carry * block_decay[:, None, None] + jnp.einsum('shd,she->hde', scaled, value_block, precision=lax.Precision.HIGHEST)
        return (new_state, inner + cross)
    start_state = jnp.zeros((heads, RET_DIM, RET_DIM), jnp.float32)
    _, outputs = lax.scan(step, start_state, (shaped(queries), shaped(keys), shaped(values)))
    return outputs.reshape(count * BLOCK, heads * RET_DIM)

def forgetting(queries, keys, values, gates):
    total = queries.shape[0]
    heads = FORGET_HEADS
    width = math.gcd(total, 512)
    query3 = queries.astype(jnp.float32).reshape(total, heads, FOX_DIM)
    key3 = keys.astype(jnp.float32).reshape(total, heads, FOX_DIM)
    value3 = values.astype(jnp.float32).reshape(total, heads, FOX_DIM)
    key_pos = jnp.arange(total, dtype=jnp.int32)

    def one_block(index):
        begin = (index * width).astype(jnp.int32)
        block = lax.dynamic_slice_in_dim(query3, begin, width, 0)
        query_gates = lax.dynamic_slice_in_dim(gates, begin, width, 0)
        scores = jnp.einsum('qhd,khd->hqk', block, key3, precision=lax.Precision.HIGHEST) * FOX_DIM ** (-0.5)
        scores = scores + query_gates.T[:, :, None] - gates.T[:, None, :]
        query_pos = begin + jnp.arange(width, dtype=jnp.int32)
        allowed = key_pos[None, :] <= query_pos[:, None]
        weights = jnp.exp(jnp.where(allowed[None], scores, -jnp.inf))
        denom = lax.optimization_barrier(jnp.sum(weights, axis=2))
        numer = jnp.einsum('hqk,khd->qhd', to_half(weights).astype(jnp.float32), value3, precision=lax.Precision.HIGHEST)
        return numer / denom.T[:, :, None]
    outputs = lax.map(one_block, jnp.arange(total // width, dtype=jnp.int32))
    return outputs.reshape(total, heads * FOX_DIM)

def reference(tokens, gain, w_ret_q, w_ret_k, w_ret_v, w_fox_q, w_fox_k, w_fox_v, fox_gates, w_out_ret, w_out_fox):
    inputs = tokens.astype(jnp.float32)
    normed = (inputs * lax.rsqrt(lax.optimization_barrier(jnp.mean(inputs * inputs, axis=1, keepdims=True)) + eps) * gain).astype(jnp.bfloat16)
    ret_query = to_half(jnp.dot(normed, w_ret_q, preferred_element_type=jnp.float32))
    ret_key = to_half(jnp.dot(normed, w_ret_k, preferred_element_type=jnp.float32))
    ret_value = to_half(jnp.dot(normed, w_ret_v, preferred_element_type=jnp.float32))
    fox_query = to_half(jnp.dot(normed, w_fox_q, preferred_element_type=jnp.float32))
    fox_key = to_half(jnp.dot(normed, w_fox_k, preferred_element_type=jnp.float32))
    fox_value = to_half(jnp.dot(normed, w_fox_v, preferred_element_type=jnp.float32))
    token_positions = jnp.arange(SEQUENCE_TOKENS, dtype=jnp.int32)
    query_rot = to_half(rotate(ret_query, token_positions, RET_DIM))
    key_rot = to_half(rotate(ret_key, token_positions, RET_DIM) * RET_DIM ** (-0.5))
    rates = decay_rates(jnp.arange(RET_HEADS, dtype=jnp.int32), float(SEQUENCE_TOKENS))
    ret_mixed = head_norm(retention(query_rot, key_rot, ret_value, rates), RET_DIM)
    fox_mixed = head_norm(forgetting(fox_query, fox_key, fox_value, fox_gates), FOX_DIM)
    ret_run = ret_mixed.shape[1] // N_TP
    fox_run = fox_mixed.shape[1] // N_TP

    def group(total, index):
        ret_rows = lax.dynamic_slice_in_dim(ret_mixed, index * ret_run, ret_run, 1)
        ret_weight = lax.dynamic_slice_in_dim(w_out_ret, index * ret_run, ret_run, 0)
        fox_rows = lax.dynamic_slice_in_dim(fox_mixed, index * fox_run, fox_run, 1)
        fox_weight = lax.dynamic_slice_in_dim(w_out_fox, index * fox_run, fox_run, 0)
        partial_sum = jnp.dot(ret_rows, ret_weight, preferred_element_type=jnp.float32) + jnp.dot(fox_rows, fox_weight, preferred_element_type=jnp.float32)
        return (total + to_half(partial_sum).astype(jnp.float32), None)
    summed, _ = lax.scan(group, jnp.zeros((SEQUENCE_TOKENS, D), jnp.float32), jnp.arange(N_TP, dtype=jnp.int32))
    return summed.astype(jnp.bfloat16)
```

```python
import functools
import math

import jax
import jax.numpy as jnp
from jax import lax
from jax.experimental import pallas as pl
from jax.experimental.pallas import tpu as pltpu
from jax.sharding import PartitionSpec as P

RET_HEADS = 8
RET_DIM = 256
FOX_DIM = 128
BLOCK = 128
MESH = pl.DeviceIdType.MESH
VMEM_LIMIT = 60 * 1024 * 1024

eps = 1e-06


def remote(src, dst, send, recv, sp, tp):
    return pltpu.make_async_remote_copy(
        src_ref=src,
        dst_ref=dst,
        send_sem=send,
        recv_sem=recv,
        device_id=(sp, tp),
        device_id_type=MESH,
    )


def gather_kernel(
    n_sp,
    n_tp,
    group,
    tok_ref,
    gain_ref,
    gates_ref,
    wr_ref,
    wf_ref,
    cos_ref,
    sin_ref,
    w_in,
    rq,
    rk,
    rv,
    fq,
    fkv,
    gall,
    wz,
    own,
    xall,
    w_ret,
    w_fox,
    local_sem,
    in_sem,
    tsend,
    trecv,
    dsend,
    drecv,
    psend,
    precv,
    gsend,
    grecv,
    usend,
    urecv,
    nsend,
    nrecv,
):
    sp = lax.axis_index("sp")
    tp = lax.axis_index("tp")
    g = lax.rem(sp, group)
    z = sp // group
    depth = n_sp // group
    rows = tok_ref.shape[0]
    half = rows // 2
    krows = wr_ref.shape[0]

    barrier = pltpu.get_barrier_semaphore()
    for i in range(1, n_sp):
        pl.semaphore_signal(
            barrier, inc=1, device_id=(lax.rem(sp + i, n_sp), tp), device_id_type=MESH
        )
    for i in range(1, n_tp):
        pl.semaphore_signal(
            barrier, inc=1, device_id=(sp, lax.rem(tp + i, n_tp)), device_id_type=MESH
        )

    loads = []
    for i in range(6):
        cut = w_ret if i < 3 else w_fox
        size = cut.shape[2]
        columns = pl.ds(pl.multiple_of(g * size, 128), size)
        loads.append(
            pltpu.make_async_copy(w_in[i].at[:, columns], cut.at[i % 3], in_sem.at[i])
        )

    values = tok_ref[...].astype(jnp.float32)
    scale = lax.rsqrt(jnp.mean(values * values, axis=1, keepdims=True) + eps)
    own[...] = (values * scale * gain_ref[...]).astype(jnp.bfloat16)
    copies = [
        pltpu.make_async_copy(wr_ref, wz.at[z, pl.ds(0, krows)], local_sem.at[0]),
        pltpu.make_async_copy(
            wf_ref, wz.at[z, pl.ds(krows, wf_ref.shape[0])], local_sem.at[1]
        ),
        pltpu.make_async_copy(gates_ref, gall.at[sp], local_sem.at[2]),
    ]
    for copy in copies + loads:
        copy.start()
    pl.semaphore_wait(barrier, n_sp + n_tp - 2)

    def slot(which, core):
        return xall.at[which * n_tp + core]

    mine = pltpu.make_async_copy(own, slot(g, tp), local_sem.at[3])
    mine.start()

    def peer(other):
        return z * group + other

    hyper = group == 4
    direct = []
    for i in range(1, group):
        if hyper and i == 3:
            continue
        other = lax.bitwise_xor(g, i) if hyper else lax.rem(g + i, group)
        direct.append(
            remote(own, slot(g, tp), tsend.at[i], trecv.at[i], peer(other), tp)
        )
    for copy in direct:
        copy.start()
    pair = []
    for i in range(1, n_tp):
        copy = remote(
            own, slot(g, tp), psend.at[0, i], precv.at[0, i], sp, lax.rem(tp + i, n_tp)
        )
        copy.start()
        pair.append(copy)
    gate_copies = []
    for i in range(1, n_sp):
        copy = remote(
            gates_ref, gall.at[sp], gsend.at[i], grecv.at[i], lax.rem(sp + i, n_sp), tp
        )
        copy.start()
        gate_copies.append(copy)

    copies[0].wait()
    copies[1].wait()

    def up(block):
        return remote(
            wz.at[block],
            wz.at[block],
            usend.at[block],
            urecv.at[block],
            lax.rem(sp + group, n_sp),
            tp,
        )

    def down(block):
        return remote(
            wz.at[block],
            wz.at[block],
            nsend.at[block],
            nrecv.at[block],
            lax.rem(sp + n_sp - group, n_sp),
            tp,
        )

    @pl.when(z < depth - 1)
    def _():
        up(z).start()

    @pl.when(z > 0)
    def _():
        down(z).start()

    ready = {0: pair[:]}

    def forward(which, row):
        ready[row] = []
        for i in range(1, n_tp):
            copy = remote(
                slot(which, tp),
                slot(which, tp),
                psend.at[row, i],
                precv.at[row, i],
                sp,
                lax.rem(tp + i, n_tp),
            )
            copy.start()
            pair.append(copy)
            ready[row].append(copy)

    count = n_tp * rows
    half_head = RET_DIM // 2

    def project(which, row):
        for copy in ready[row]:
            copy.wait_recv()
        x = xall[pl.ds(which * n_tp, n_tp)].reshape(count, xall.shape[2])
        span = pl.ds(pl.multiple_of(which * count, count), count)
        for i in range(6):
            cut = w_ret if i < 3 else w_fox
            y = jnp.dot(x, cut[i % 3], preferred_element_type=jnp.float32)
            y = y.astype(jnp.bfloat16)
            if i < 2:
                cosine = cos_ref[span, :]
                sine = sin_ref[span, :]
            for h in range(rq.shape[0] if i < 3 else fq.shape[0]):
                if i < 2:
                    lo = h * RET_DIM
                    a = y[:, lo : lo + half_head].astype(jnp.float32)
                    b = y[:, lo + half_head : lo + RET_DIM].astype(jnp.float32)
                    to = rq if i == 0 else rk
                    by = 1.0 if i == 0 else RET_DIM ** (-0.5)
                    first = (a * cosine - b * sine) * by
                    second = (a * sine + b * cosine) * by
                    to[h, span, :half_head] = first.astype(jnp.bfloat16)
                    to[h, span, half_head:] = second.astype(jnp.bfloat16)
                elif i == 2:
                    rv[h, span, :] = y[:, h * RET_DIM : (h + 1) * RET_DIM]
                elif i == 3:
                    fq[h, span, :] = y[:, h * FOX_DIM : (h + 1) * FOX_DIM]
                else:
                    fkv[i - 4, h, span, :] = y[:, h * FOX_DIM : (h + 1) * FOX_DIM]

    mine.wait()
    for copy in loads:
        copy.wait()
    if not hyper:
        project(g, 0)

    if hyper:
        relays = []
        for i in (1, 2):
            direct[i - 1].wait_recv()
            source = lax.bitwise_xor(g, i)
            target = lax.bitwise_xor(g, 3 - i)
            part = pl.ds((i - 1) * half, half)
            copy = remote(
                slot(source, tp).at[part],
                slot(source, tp).at[part],
                dsend.at[i],
                drecv.at[i],
                peer(target),
                tp,
            )
            copy.start()
            relays.append(copy)
            forward(source, i)
        project(g, 0)
    else:
        for i in range(1, group):
            direct[i - 1].wait_recv()
            forward(lax.rem(g + group - i, group), i)
            project(lax.rem(g + group - i, group), i)

    def line(step, carry):
        below = z - step
        above = z + step

        @pl.when(below >= 0)
        def _():
            up(below).wait_recv()

            @pl.when(z < depth - 1)
            def _():
                up(below).start()

        @pl.when(above <= depth - 1)
        def _():
            down(above).wait_recv()

            @pl.when(z > 0)
            def _():
                down(above).start()

        return carry

    split = depth // 2 if hyper else depth
    lax.fori_loop(1, split, line, 0)
    if hyper:
        project(lax.bitwise_xor(g, 1), 1)
        for copy in relays:
            copy.wait_recv()
        forward(lax.bitwise_xor(g, 3), 3)
    lax.fori_loop(split, depth - 1, line, 0)
    if hyper:
        project(lax.bitwise_xor(g, 2), 2)
        project(lax.bitwise_xor(g, 3), 3)
    lax.fori_loop(max(split, depth - 1), depth, line, 0)

    def settle(step, carry):
        @pl.when((z < depth - 1) & (step <= z))
        def _():
            up(step).wait_send()

        @pl.when((z > 0) & (step >= z))
        def _():
            down(step).wait_send()

        return carry

    lax.fori_loop(0, depth, settle, 0)
    for copy in direct:
        copy.wait_send()
    if hyper:
        for copy in relays:
            copy.wait_send()
    for copy in gate_copies:
        copy.wait()
    for copy in pair:
        copy.wait_send()
    copies[2].wait()


def gather(
    tokens, gain, gates, w_ret, w_fox, cosine, sine, w_in, hret, hfox, n_sp, n_tp, group
):
    rows, width = tokens.shape
    depth = n_sp // group
    out_rows = w_ret.shape[0] + w_fox.shape[0]
    vmem = pl.BlockSpec(memory_space=pltpu.VMEM)
    hbm = pl.BlockSpec(memory_space=pl.ANY)
    dma = pltpu.SemaphoreType.DMA
    run = rows * n_tp * group
    bf16 = jnp.bfloat16

    def body(*refs):
        gather_kernel(n_sp, n_tp, group, *refs[:7], refs[7:13], *refs[13:])

    return pl.pallas_call(
        body,
        out_shape=(
            jax.ShapeDtypeStruct((hret, run, RET_DIM), bf16),
            jax.ShapeDtypeStruct((hret, run, RET_DIM), bf16),
            jax.ShapeDtypeStruct((hret, run, RET_DIM), bf16),
            jax.ShapeDtypeStruct((hfox, run, FOX_DIM), bf16),
            jax.ShapeDtypeStruct((2, hfox, run, FOX_DIM), bf16),
            jax.ShapeDtypeStruct((n_sp,) + gates.shape, jnp.float32),
            jax.ShapeDtypeStruct((depth, out_rows, w_ret.shape[1]), jnp.bfloat16),
        ),
        in_specs=[vmem, vmem, vmem, hbm, hbm, vmem, vmem] + [hbm] * 6,
        out_specs=(vmem,) * 7,
        scratch_shapes=[
            pltpu.VMEM((rows, width), bf16),
            pltpu.VMEM((group * n_tp, rows, width), bf16),
            pltpu.VMEM((3, width, hret * RET_DIM), bf16),
            pltpu.VMEM((3, width, hfox * FOX_DIM), bf16),
            dma((4,)),
            dma((6,)),
            dma((max(group, 2),)),
            dma((max(group, 2),)),
            dma((3,)),
            dma((3,)),
            dma((group, n_tp)),
            dma((group, n_tp)),
            dma((n_sp,)),
            dma((n_sp,)),
            dma((depth,)),
            dma((depth,)),
            dma((depth,)),
            dma((depth,)),
        ],
        compiler_params=pltpu.CompilerParams(
            collective_id=0, has_side_effects=True, vmem_limit_bytes=VMEM_LIMIT
        ),
        name="gather",
    )(tokens, gain, gates, w_ret, w_fox, cosine, sine, *w_in)


def normalize(values):
    return (
        values * lax.rsqrt(jnp.mean(values * values, axis=1, keepdims=True) + eps)
    ).astype(jnp.bfloat16)


def mixer_kernel(
    n_sp,
    n_tp,
    group,
    rq,
    rk,
    rv,
    fq,
    fkv,
    gq,
    gk,
    within,
    qdec,
    kdec,
    bdec,
    wz,
    out,
    w_all,
    slots,
    raw,
    state,
    state_in,
    state_out,
    numer,
    denom,
    ret_buf,
    fox_buf,
    mixed,
    part,
    got,
    local_sem,
    ksend,
    krecv,
    ssend,
    srecv,
    wsend,
    wrecv,
    dsend,
    drecv,
    asend,
    arecv,
    osend,
    orecv,
):
    sp = lax.axis_index("sp")
    tp = lax.axis_index("tp")
    g = lax.rem(sp, group)
    z = sp // group
    depth = n_sp // group
    hret = rq.shape[0]
    hfox = fq.shape[0]
    run = rq.shape[1]
    tok = run // group
    rows = out.shape[0]
    after = lax.rem(sp + group, n_sp)
    before = lax.rem(sp + n_sp - group, n_sp)
    f32 = jnp.float32

    def peer(other):
        return z * group + other

    barrier = pltpu.get_barrier_semaphore()
    for i in range(1, group):
        pl.semaphore_signal(
            barrier, inc=1, device_id=(peer(lax.rem(g + i, group)), tp), device_id_type=MESH
        )
    for i in range(1, n_tp):
        pl.semaphore_signal(
            barrier, inc=1, device_id=(sp, lax.rem(tp + i, n_tp)), device_id_type=MESH
        )
    if depth > 1:

        @pl.when(z < depth - 1)
        def _():
            pl.semaphore_signal(barrier, inc=1, device_id=(after, tp), device_id_type=MESH)

        @pl.when(z > 0)
        def _():
            pl.semaphore_signal(barrier, inc=1, device_id=(before, tp), device_id_type=MESH)

    ends = (z + depth - 1) // depth + (2 * depth - 2 - z) // depth
    pl.semaphore_wait(barrier, group + n_tp - 2 + ends)

    def first_hop():
        return remote(fkv, slots.at[z], ksend.at[z], krecv.at[z], after, tp)

    def hop(block):
        return remote(
            slots.at[block], slots.at[block], ksend.at[block], krecv.at[block], after, tp
        )

    if depth > 1:

        @pl.when(z < depth - 1)
        def _():
            first_hop().start()

    hyper = group == 4
    mine = pltpu.make_async_copy(wz, w_all.at[g], local_sem.at[0])
    mine.start()
    direct = []
    for i in range(1, group):
        if hyper and i == 3:
            continue
        other = lax.bitwise_xor(g, i) if hyper else lax.rem(g + i, group)
        direct.append(
            remote(wz, w_all.at[g], wsend.at[i], wrecv.at[i], peer(other), tp)
        )
    for copy in direct:
        copy.start()

    def relay(i):
        source = lax.bitwise_xor(g, i)
        target = lax.bitwise_xor(g, 3 - i)
        span = pl.ds((i - 1) * (depth // 2), depth // 2)
        return remote(
            w_all.at[source, span],
            w_all.at[source, span],
            dsend.at[i],
            drecv.at[i],
            peer(target),
            tp,
        )

    for h in range(hret):
        state[h] = jnp.zeros(state.shape[1:], f32)

        def ret_step(b, carry):
            span = pl.ds(pl.multiple_of(b * BLOCK, BLOCK), BLOCK)
            q = rq[h, span, :]
            k = rk[h, span, :]
            v = rv[h, span, :]
            scores = (
                lax.dot_general(q, k, (((1,), (1,)), ((), ())), preferred_element_type=f32)
                * within[h]
            )
            inner = jnp.dot(scores.astype(jnp.bfloat16), v, preferred_element_type=f32)
            held = state[h]
            cross = jnp.dot(q, held.astype(jnp.bfloat16), preferred_element_type=f32)
            raw[h, span, :] = inner + cross * qdec[h, pl.ds(0, BLOCK), :]
            scaled = (k.astype(f32) * kdec[h]).astype(jnp.bfloat16)
            update = lax.dot_general(
                scaled, v, (((0,), (0,)), ((), ())), preferred_element_type=f32
            )
            state[h] = held * bdec[h, 0:1, :] + update
            return carry

        lax.fori_loop(0, run // BLOCK, ret_step, 0)

    def state_hop():
        return remote(state_out, state_in, ssend.at[0], srecv.at[0], after, tp)

    if depth > 1:

        @pl.when(z == 0)
        def _():
            state_out[...] = state[...]
            state_hop().start()

    tile = math.gcd(run, 256)
    inverse = FOX_DIM ** (-0.5)

    def attend(h, t, keys, values, key_gates, diagonal, fresh):
        span = pl.ds(pl.multiple_of(t * tile, tile), tile)
        scores = (
            lax.dot_general(
                fq[h, span, :], keys, (((1,), (1,)), ((), ())), preferred_element_type=f32
            )
            * inverse
        )
        scores = scores + gq[h, span, :] - key_gates
        if diagonal:
            row = lax.broadcasted_iota(jnp.int32, scores.shape, 0)
            col = lax.broadcasted_iota(jnp.int32, scores.shape, 1)
            scores = jnp.where(col <= row, scores, -jnp.inf)
        weights = jnp.exp(scores)
        total = jnp.sum(weights, axis=1, keepdims=True)
        product = jnp.dot(weights.astype(jnp.bfloat16), values, preferred_element_type=f32)
        if fresh:
            numer[h, span, :] = product
            denom[h, span, :] = total
        else:
            numer[h, span, :] += product
            denom[h, span, :] += total

    for h in range(hfox):
        for t in range(run // tile):
            for s in range(t, -1, -1):
                span = pl.ds(s * tile, tile)
                attend(
                    h,
                    t,
                    fkv[0, h, span, :],
                    fkv[1, h, span, :],
                    gk[h, z, :, span],
                    s == t,
                    s == t,
                )

    def carried():
        state_hop().wait_recv()

        @pl.when(z < depth - 1)
        def _():
            for h in range(hret):
                state_out[h] = state_in[h] * bdec[h, 1:2, :] + state[h]
            state_hop().start()

        for h in range(hret):
            held = state_in[h].astype(jnp.bfloat16)

            def cross_step(b, carry):
                span = pl.ds(pl.multiple_of(b * tile, tile), tile)
                cross = jnp.dot(rq[h, span, :], held, preferred_element_type=f32)
                raw[h, span, :] += cross * qdec[h, span, :]
                return carry

            lax.fori_loop(0, run // tile, cross_step, 0)

    def earlier(step, carry):
        @pl.when(step <= z)
        def _():
            block = z - step
            hop(block).wait_recv()

            @pl.when(z < depth - 1)
            def _():
                hop(block).start()

            for h in range(hfox):

                def query_step(t, c):
                    attend(
                        h,
                        t,
                        slots[block, 0, h],
                        slots[block, 1, h],
                        gk[h, block],
                        False,
                        False,
                    )
                    return c

                lax.fori_loop(0, run // tile, query_step, 0)

        return carry

    if depth > 1:
        lax.fori_loop(1, 2, earlier, 0)

        @pl.when(z > 0)
        def _():
            carried()

        if hyper:
            direct[0].wait_recv()
            relay(1).start()
            direct[1].wait_recv()
            relay(2).start()
        lax.fori_loop(2, depth, earlier, 0)
    elif hyper:
        direct[0].wait_recv()
        relay(1).start()
        direct[1].wait_recv()
        relay(2).start()

    rw = hret * RET_DIM
    fw = hfox * FOX_DIM
    for t in range(group):
        span = pl.ds(t * tok, tok)
        for h in range(hret):
            ret_buf[t, :, h * RET_DIM : (h + 1) * RET_DIM] = normalize(raw[h, span, :])
        for h in range(hfox):
            fox_buf[t, :, h * FOX_DIM : (h + 1) * FOX_DIM] = normalize(
                numer[h, span, :] / denom[h, span, :]
            )
    ret_cols = pl.ds(pl.multiple_of(g * rw, 128), rw)
    fox_cols = pl.ds(pl.multiple_of(group * rw + g * fw, 128), fw)
    exchange = []
    for i in range(1, group):
        other = lax.rem(g + i, group)
        for kind, (buf, cols) in enumerate(((ret_buf, ret_cols), (fox_buf, fox_cols))):
            copy = remote(
                buf.at[other],
                mixed.at[:, cols],
                asend.at[kind, i],
                arecv.at[kind, i],
                peer(other),
                tp,
            )
            copy.start()
            exchange.append(copy)
    mixed[:, ret_cols] = ret_buf[g]
    mixed[:, fox_cols] = fox_buf[g]
    for copy in exchange:
        copy.wait_recv()
    mine.wait()
    if hyper:
        relay(1).wait_recv()
        relay(2).wait_recv()
    else:
        for copy in direct:
            copy.wait_recv()

    cols = w_all.shape[3]
    pack = max(1, 128 // cols)
    wide = pack * cols
    for t in range(n_tp):
        left = mixed[t * rows : (t + 1) * rows, :]

        def column(p, carry, left=left, t=t):
            blocks = [
                w_all[lax.rem(p * pack + i, group), (p * pack + i) // group]
                for i in range(pack)
            ]
            right = blocks[0] if pack == 1 else jnp.concatenate(blocks, axis=1)
            product = jnp.dot(left, right, preferred_element_type=f32)
            at = pl.ds(pl.multiple_of(p * wide, wide), wide)
            part[t, :, at] = product.astype(jnp.bfloat16)
            return carry

        lax.fori_loop(0, n_sp // pack, column, 0)
    final = []
    for i in range(1, n_tp):
        other = lax.rem(tp + i, n_tp)
        copy = remote(part.at[other], got.at[i], osend.at[i], orecv.at[i], sp, other)
        copy.start()
        final.append(copy)
    total = part[tp].astype(f32)
    for i in range(1, n_tp):
        final[i - 1].wait_recv()
        total = total + got[i].astype(f32)
    out[...] = total.astype(jnp.bfloat16)

    for copy in final + exchange + direct:
        copy.wait_send()
    if hyper:
        relay(1).wait_send()
        relay(2).wait_send()
    if depth > 1:

        @pl.when(z < depth - 1)
        def _():
            first_hop().wait_send()
            state_hop().wait_send()

            def settle(block, carry):
                @pl.when(block < z)
                def _():
                    hop(block).wait_send()

                return carry

            lax.fori_loop(0, depth, settle, 0)


def mixer(rq, rk, rv, fq, fkv, gq, gk, within, qdec, kdec, bdec, wz, rows, n_sp, n_tp, group):
    depth = n_sp // group
    hret, run, _ = rq.shape
    hfox = fq.shape[0]
    tok = run // group
    out_rows, cols = wz.shape[1:]
    width = n_sp * cols
    vmem = pl.BlockSpec(memory_space=pltpu.VMEM)
    dma = pltpu.SemaphoreType.DMA
    f32 = jnp.float32
    bf16 = jnp.bfloat16
    square = (hret, RET_DIM, RET_DIM)
    return pl.pallas_call(
        functools.partial(mixer_kernel, n_sp, n_tp, group),
        out_shape=jax.ShapeDtypeStruct((rows, width), bf16),
        in_specs=[vmem] * 11 + [pl.BlockSpec(memory_space=pl.ANY)],
        out_specs=vmem,
        scratch_shapes=[
            pltpu.VMEM((group,) + wz.shape, bf16),
            pltpu.VMEM((depth,) + fkv.shape, bf16),
            pltpu.VMEM((hret, run, RET_DIM), f32),
            pltpu.VMEM(square, f32),
            pltpu.VMEM(square, f32),
            pltpu.VMEM(square, f32),
            pltpu.VMEM((hfox, run, FOX_DIM), f32),
            pltpu.VMEM((hfox, run, 1), f32),
            pltpu.VMEM((group, tok, hret * RET_DIM), bf16),
            pltpu.VMEM((group, tok, hfox * FOX_DIM), bf16),
            pltpu.VMEM((tok, out_rows), bf16),
            pltpu.VMEM((n_tp, rows, width), bf16),
            pltpu.VMEM((n_tp, rows, width), bf16),
            dma((1,)),
            dma((depth,)),
            dma((depth,)),
            dma((1,)),
            dma((1,)),
            dma((max(group, 2),)),
            dma((max(group, 2),)),
            dma((3,)),
            dma((3,)),
            dma((2, group)),
            dma((2, group)),
            dma((n_tp,)),
            dma((n_tp,)),
        ],
        compiler_params=pltpu.CompilerParams(
            collective_id=1, has_side_effects=True, vmem_limit_bytes=VMEM_LIMIT
        ),
        name="mixer",
    )(rq, rk, rv, fq, fkv, gq, gk, within, qdec, kdec, bdec, wz)


def fused_kernel(
    n_sp,
    total,
    tok_ref,
    gain_ref,
    gates_ref,
    inv_ref,
    wr_ref,
    wf_ref,
    w_in,
    out,
    xall,
    w_ret,
    w_fox,
    wrs,
    wret,
    wfox,
    gall,
    ctab,
    stab,
    within,
    qdec,
    kdec,
    rq,
    rk,
    rv,
    fq,
    guest,
    kv,
    raw,
    update,
    state_in,
    state_out,
    carry_state,
    gcol,
    guest_col,
    numer,
    guest_numer,
    num_out,
    num_in,
    den_out,
    den_in,
    part,
    part_in,
    rsum,
    xa,
    yb,
    second_out,
    second_in,
    fox_buf,
    mixed,
    fpart,
    fgot,
    local_sem,
    tsend,
    trecv,
    dsend,
    drecv,
    psend,
    precv,
    gsend,
    grecv,
    asend,
    arecv,
    usend,
    urecv,
    nsend,
    nrecv,
    fsend,
    frecv,
    ksend,
    krecv,
    qsend,
    qrecv,
    ssend,
    srecv,
    osend,
    orecv,
    psum_send,
    psum_recv,
    rsend,
    rrecv,
    esend,
    erecv,
):
    f32 = jnp.float32
    bf16 = jnp.bfloat16
    group = 4
    sp = lax.axis_index("sp")
    tp = lax.axis_index("tp")
    other_core = 1 - tp
    g = lax.rem(sp, group)
    z = sp // group
    depth = n_sp // group
    last = depth - 1
    host = depth - 2
    rows = tok_ref.shape[0]
    tok = 2 * rows
    hret = rq.shape[1]
    hfox = fq.shape[1]
    ret_rows = hret * RET_DIM
    after = lax.rem(sp + group, n_sp)
    before = lax.rem(sp + n_sp - group, n_sp)

    def near(i):
        return lax.bitwise_xor(g, i)

    def peer(i):
        return z * group + near(i)

    barrier = pltpu.get_barrier_semaphore()
    for i in range(1, n_sp):
        pl.semaphore_signal(
            barrier, inc=1, device_id=(lax.rem(sp + i, n_sp), tp), device_id_type=MESH
        )
    pl.semaphore_signal(barrier, inc=1, device_id=(sp, other_core), device_id_type=MESH)

    locals_ = [
        pltpu.make_async_copy(wr_ref, wrs, local_sem.at[0]),
        pltpu.make_async_copy(
            wr_ref.at[pl.ds(pl.multiple_of(g * ret_rows, ret_rows), ret_rows)],
            wret.at[z, 0],
            local_sem.at[1],
        ),
        pltpu.make_async_copy(wf_ref, wfox.at[0, z], local_sem.at[2]),
    ]
    loads = []
    for i in range(6):
        cut = w_ret if i < 3 else w_fox
        size = cut.shape[2]
        columns = pl.ds(pl.multiple_of(g * size, 128), size)
        loads.append(
            pltpu.make_async_copy(
                w_in[i].at[:, columns], cut.at[i % 3], local_sem.at[3 + i]
            )
        )
    for copy in locals_ + loads:
        copy.start()

    values = tok_ref[...].astype(f32)
    scale = lax.rsqrt(jnp.mean(values * values, axis=1, keepdims=True) + eps)
    xall[0, tp] = (values * scale * gain_ref[...]).astype(bf16)
    gall[sp] = gates_ref[...]
    pl.semaphore_wait(barrier, n_sp)

    def token_copy(i):
        return remote(xall.at[0, tp], xall.at[i, tp], tsend.at[i], trecv.at[i], peer(i), tp)

    def token_relay(i):
        span = pl.ds((i - 1) * (rows // 2), rows // 2)
        return remote(
            xall.at[i, tp, span],
            xall.at[3, tp, span],
            dsend.at[i],
            drecv.at[i],
            peer(3 - i),
            tp,
        )

    def pair_copy(i):
        return remote(
            xall.at[i, tp], xall.at[i, tp], psend.at[i], precv.at[i], sp, other_core
        )

    def gate_copy(i):
        return remote(
            gates_ref, gall.at[sp], gsend.at[i], grecv.at[i], lax.rem(sp + i, n_sp), tp
        )

    def rows_copy(i):
        span = pl.ds(pl.multiple_of(near(i) * ret_rows, ret_rows), ret_rows)
        return remote(wrs.at[span], wret.at[z, i], asend.at[i], arecv.at[i], peer(i), tp)

    def cut_of(kind, block):
        if kind == 0:
            return wfox.at[0, block]
        if kind == 1:
            return wret.at[block, 0]
        return wret.at[block, pl.ds(1, group - 1)]

    def up(kind, block):
        ref = cut_of(kind, block)
        return remote(ref, ref, usend.at[kind, block], urecv.at[kind, block], after, tp)

    def down(kind, block):
        ref = cut_of(kind, block)
        return remote(ref, ref, nsend.at[kind, block], nrecv.at[kind, block], before, tp)

    def begin_line(kind):
        @pl.when(z < last)
        def _():
            up(kind, z).start()

        @pl.when(z > 0)
        def _():
            down(kind, z).start()

    def line(kind, step):
        below = z - step
        above = z + step

        @pl.when(below >= 0)
        def _():
            up(kind, below).wait_recv()

            @pl.when(z < last)
            def _():
                up(kind, below).start()

        @pl.when(above <= last)
        def _():
            down(kind, above).wait_recv()

            @pl.when(z > 0)
            def _():
                down(kind, above).start()

    def settle_line(kind):
        for block in range(depth):

            @pl.when((z < last) & (block <= z))
            def _():
                up(kind, block).wait_send()

            @pl.when((z > 0) & (block >= z))
            def _():
                down(kind, block).wait_send()

    def plane_copy(i):
        return remote(wfox.at[0], wfox.at[i], fsend.at[i], frecv.at[i], peer(i), tp)

    def plane_relay(i):
        span = pl.ds(0, depth // 2) if i == 1 else pl.ds(depth // 2, depth - depth // 2)
        return remote(
            wfox.at[i, span],
            wfox.at[3, span],
            fsend.at[2 + i],
            frecv.at[2 + i],
            peer(3 - i),
            tp,
        )

    def kv_hop(block, i):
        ref = kv.at[block, i]
        return remote(ref, ref, ksend.at[block, i], krecv.at[block, i], after, tp)

    def query_hop(i):
        return remote(fq.at[i], guest.at[i], qsend.at[i], qrecv.at[i], before, tp)

    def state_hop():
        return remote(state_out, state_in, ssend.at[0], srecv.at[0], after, tp)

    def num_hop(i):
        return remote(num_out.at[i], num_in.at[i], osend.at[i], orecv.at[i], after, tp)

    def den_hop():
        return remote(den_out, den_in, osend.at[group], orecv.at[group], after, tp)

    def part_copy(i):
        return remote(
            part.at[i, other_core],
            part_in.at[i],
            psum_send.at[i],
            psum_recv.at[i],
            sp,
            other_core,
        )

    width = out.shape[1]
    half = width // 2
    first_cols = pl.ds(0, half)
    last_cols = pl.ds(half, half)

    def scatter_x(k):
        return remote(
            rsum.at[1 + 2 * k, :, first_cols],
            xa.at[k],
            rsend.at[k],
            rrecv.at[k],
            peer(1),
            tp,
        )

    def scatter_y(k):
        return remote(
            rsum.at[2 + k, :, last_cols],
            yb.at[k],
            rsend.at[2 + k],
            rrecv.at[2 + k],
            peer(2),
            tp,
        )

    def scatter_second(k):
        return remote(
            second_out.at[k],
            second_in.at[k],
            rsend.at[4 + k],
            rrecv.at[4 + k],
            peer(2 if k == 0 else 1),
            tp,
        )

    fw = hfox * FOX_DIM
    my_cols = pl.ds(pl.multiple_of(g * fw, 128), fw)

    def mixed_copy(i):
        return remote(
            fox_buf.at[i], mixed.at[:, my_cols], esend.at[i], erecv.at[i], peer(i), tp
        )

    def final_copy():
        return remote(
            fpart.at[other_core], fgot, esend.at[0], erecv.at[0], sp, other_core
        )

    for i in (1, 2):
        token_copy(i).start()
    pair_copy(0).start()
    for i in range(1, n_sp):
        gate_copy(i).start()
    for copy in locals_:
        copy.wait()
    for i in range(1, group):
        rows_copy(i).start()
    begin_line(0)
    begin_line(1)

    head_of = [tp * (group * hret) + g * hret + h for h in range(hret)]
    rates = []
    for h in range(hret):
        ids = jnp.full((1, RET_DIM), head_of[h], jnp.int32)
        heads_float = ids.astype(f32)
        middle = RET_HEADS // 2
        fast_rate = 1.0 / (32.0 + 16.0 * heads_float)
        slow_rate = jnp.exp2(-(heads_float - middle)) / total
        rates.append(jnp.where(ids < middle, fast_rate, slow_rate))
    square = (tok, RET_DIM)
    offset = lax.broadcasted_iota(jnp.int32, square, 0)
    column = lax.broadcasted_iota(jnp.int32, (tok, tok), 1)
    row = lax.broadcasted_iota(jnp.int32, (tok, tok), 0)
    for h in range(hret):
        rate = rates[h]
        spread = jnp.maximum(row - column, 0).astype(f32)
        within[h] = jnp.where(row >= column, jnp.exp(-rate[:, :1] * spread), 0.0)
        steps = offset.astype(f32)
        qdec[h] = jnp.exp(-rate * (steps + 1.0))
        kdec[h] = jnp.exp(-rate * (tok - 1.0 - steps))
    inverse_freq = inv_ref[...]
    unit = 16
    low = lax.broadcasted_iota(jnp.int32, (unit, RET_DIM // 2), 0).astype(f32)
    high = lax.broadcasted_iota(jnp.int32, (tok // unit, RET_DIM // 2), 0).astype(f32)
    cos_low, sin_low = jnp.cos(low * inverse_freq), jnp.sin(low * inverse_freq)
    high = high * float(unit) * inverse_freq
    cos_high, sin_high = jnp.cos(high), jnp.sin(high)
    for a in range(tok // unit):
        ca, sa = cos_high[a : a + 1], sin_high[a : a + 1]
        ctab[a * unit : (a + 1) * unit] = cos_low * ca - sin_low * sa
        stab[a * unit : (a + 1) * unit] = sin_low * ca + cos_low * sa

    half_head = RET_DIM // 2

    def retain(i):
        for h in range(hret):
            q = rq[i, h]
            k = rk[i, h]
            v = rv[i, h]
            scores = (
                lax.dot_general(q, k, (((1,), (1,)), ((), ())), preferred_element_type=f32)
                * within[h]
            )
            raw[i, h] = jnp.dot(scores.astype(bf16), v, preferred_element_type=f32)
            scaled = (k.astype(f32) * kdec[h]).astype(bf16)
            update[i, h] = lax.dot_general(
                scaled, v, (((0,), (0,)), ((), ())), preferred_element_type=f32
            )

    def project(i):
        x = xall[i].reshape(tok, xall.shape[3])
        start = jnp.full((1, half_head), z * (group * tok) + near(i) * tok, jnp.int32)
        turn = start.astype(f32) * inverse_freq
        cos_turn, sin_turn = jnp.cos(turn), jnp.sin(turn)
        for m in (4, 5, 3, 1, 2, 0):
            cut = w_ret if m < 3 else w_fox
            y = jnp.dot(x, cut[m % 3], preferred_element_type=f32).astype(bf16)
            if m < 2:
                cosine = ctab[...] * cos_turn - stab[...] * sin_turn
                sine = stab[...] * cos_turn + ctab[...] * sin_turn
            for h in range(hret if m < 3 else hfox):
                if m < 2:
                    lo = h * RET_DIM
                    a = y[:, lo : lo + half_head].astype(f32)
                    b = y[:, lo + half_head : lo + RET_DIM].astype(f32)
                    to = rq if m == 0 else rk
                    by = 1.0 if m == 0 else RET_DIM ** (-0.5)
                    to[i, h, :, :half_head] = ((a * cosine - b * sine) * by).astype(bf16)
                    to[i, h, :, half_head:] = ((a * sine + b * cosine) * by).astype(bf16)
                elif m == 2:
                    rv[i, h] = y[:, h * RET_DIM : (h + 1) * RET_DIM]
                elif m == 3:
                    fq[i, h] = y[:, h * FOX_DIM : (h + 1) * FOX_DIM]
                else:
                    kv[z, i, m - 4, h] = y[:, h * FOX_DIM : (h + 1) * FOX_DIM]
            if m == 5:

                @pl.when(z < last)
                def _():
                    kv_hop(z, i).start()

            if m == 3:

                @pl.when(z == last)
                def _():
                    query_hop(i).start()

    def take(step, i):
        block = z - step
        wanted = block >= 0
        if step > 1:
            wanted = wanted & (z < last)

        @pl.when(wanted)
        def _():
            kv_hop(block, i).wait_recv()

            @pl.when(z < host)
            def _():
                kv_hop(block, i).start()

    for copy in loads:
        copy.wait()
    pair_copy(0).wait_recv()
    project(0)
    line(0, 1)
    line(1, 1)
    take(1, 0)
    retain(0)
    for step in range(2, depth):
        line(0, step)
        line(1, step)
    for i in (1, 2):
        token_copy(i).wait_recv()
        token_relay(i).start()
        pair_copy(i).start()
    for i in range(1, group):
        rows_copy(i).wait_recv()
    pair_copy(1).wait_recv()
    project(1)
    pair_copy(2).wait_recv()
    project(2)
    begin_line(2)
    for i in (1, 2):
        plane_copy(i).start()
    retain(1)
    retain(2)
    line(2, 1)
    take(1, 1)
    take(1, 2)
    for i in (1, 2):
        token_relay(i).wait_recv()
    pair_copy(3).start()
    pair_copy(3).wait_recv()
    project(3)
    retain(3)

    run_decay = [jnp.exp(-rates[h] * float(group * tok)) for h in range(hret)]
    tok_decay = [jnp.exp(-rates[h] * float(tok)) for h in range(hret)]
    for h in range(hret):
        held = update[g, h]
        for p in range(1, group):
            held = held * tok_decay[h] + update[near(p), h]
        carry_state[h] = held

    @pl.when(z == 0)
    def _():
        state_out[...] = carry_state[...].astype(bf16)
        state_hop().start()

    take(1, 3)
    for step in range(2, depth):
        line(2, step)

    @pl.when(z > 0)
    def _():
        state_hop().wait_recv()

        @pl.when(z < last)
        def _():
            for h in range(hret):
                state_out[h] = (state_in[h].astype(f32) * run_decay[h] + carry_state[h]).astype(
                    bf16
                )
            state_hop().start()

        carry_state[...] = state_in[...].astype(f32)

    @pl.when(z == 0)
    def _():
        carry_state[...] = jnp.zeros(carry_state.shape, f32)

    for i in range(1, n_sp):
        gate_copy(i).wait_recv()

    def gate_row(plane, i, h):
        return gall[plane * group + near(i), pl.ds(g * hfox + h, 1), :]

    def spread_columns(line_row, to, i, h):
        for c in range(tok // 128):
            piece = line_row[:, c * 128 : (c + 1) * 128]
            to[i, h, c * 128 : (c + 1) * 128, :] = jnp.broadcast_to(piece, (128, 128)).T

    for h in range(hfox):
        for i in range(group):
            spread_columns(gate_row(z, i, h), gcol, i, h)

    @pl.when(z == host)
    def _():
        for h in range(hfox):
            for i in range(group):
                spread_columns(gate_row(last, i, h), guest_col, i, h)

    inverse = FOX_DIM ** (-0.5)

    def weigh(q, column_gates, keys, key_gates, mask=None):
        scores = (
            lax.dot_general(q, keys, (((1,), (1,)), ((), ())), preferred_element_type=f32)
            * inverse
        )
        count = keys.shape[0] // 128
        scores = scores + jnp.concatenate([column_gates] * count, axis=1) - key_gates
        if mask is not None:
            scores = jnp.where(mask, scores, -jnp.inf)
        return jnp.exp(scores).astype(bf16)

    def widen(v):
        return jnp.concatenate([v, jnp.ones(v.shape, bf16)], axis=1)

    def own_attention():
        mask = row >= column
        for h in range(hfox):
            for t in range(group):
                it = near(t)
                weights, vals = [], []
                for s in range(t + 1):
                    js = near(s)
                    weights.append(
                        weigh(
                            fq[it, h],
                            gcol[it, h],
                            kv[z, js, 0, h],
                            gall[z * group + s, pl.ds(g * hfox + h, 1), :],
                            mask if s == t else None,
                        )
                    )
                    vals.append(kv[z, js, 1, h])
                w = weights[0] if t == 0 else jnp.concatenate(weights, axis=1)
                v = vals[0] if t == 0 else jnp.concatenate(vals, axis=0)
                numer[it, h] = jnp.dot(w, widen(v), preferred_element_type=f32)

    def attend(block, queries, columns, to, fresh, done=None):
        for h in range(hfox):
            keys = kv[block, :, 0, h].reshape(group * tok, FOX_DIM)
            vals = widen(kv[block, :, 1, h].reshape(group * tok, FOX_DIM))
            key_gates = jnp.concatenate([gate_row(block, i, h) for i in range(group)], axis=1)

            def query_step(j, carry):
                w = weigh(queries[j, h], columns[j, h], keys, key_gates)
                product = jnp.dot(w, vals, preferred_element_type=f32)
                if fresh:
                    to[j, h] = product
                else:
                    to[j, h] += product
                return carry

            lax.fori_loop(0, group, query_step, 0)

    def hand_back():
        for i in range(group):
            for h in range(hfox):
                num_out[i, h] = guest_numer[i, h, :, :FOX_DIM].astype(bf16)
                for c in range(tok // 128):
                    at = (i * hfox + h) * (tok // 128) + c
                    den = guest_numer[i, h, c * 128 : (c + 1) * 128, FOX_DIM:]
                    den_out[at : at + 1, :] = den.T[0:1]
            num_hop(i).start()
        den_hop().start()

    def take_back():
        den_hop().wait_recv()
        for i in range(group):
            num_hop(i).wait_recv()
            for h in range(hfox):
                numer[i, h, :, :FOX_DIM] += num_in[i, h].astype(f32)
                for c in range(tok // 128):
                    at = (i * hfox + h) * (tok // 128) + c
                    den = jnp.broadcast_to(den_in[at : at + 1, :], (128, 128)).T
                    numer[i, h, c * 128 : (c + 1) * 128, FOX_DIM:] += den

    def earlier(step):
        wanted = z - step >= 0
        if step > 1:
            wanted = wanted & (z < last)

        @pl.when(wanted)
        def _():
            block = z - step

            @pl.when(z == host)
            def _():
                attend(block, guest, guest_col, guest_numer, step == 1)
                if step == host:
                    hand_back()

            attend(block, fq, gcol, numer, False)

    def retention_out():
        for h in range(hret):
            held = carry_state[h]
            for p in range(group):
                ip = near(p)
                cross = jnp.dot(rq[ip, h], held.astype(bf16), preferred_element_type=f32)
                full = raw[ip, h] + cross * qdec[h]
                rq[ip, h] = normalize(full)
                if p < group - 1:
                    held = held * tok_decay[h] + update[ip, h]
        for i in range(group):
            left = jnp.concatenate([rq[i, h] for h in range(hret)], axis=1)

            def column_step(p, carry, left=left, i=i):
                right = jnp.concatenate(
                    [wret[p // 2, near(2 * lax.rem(p, 2) + e)] for e in range(2)], axis=1
                )
                product = jnp.dot(left, right, preferred_element_type=f32).astype(bf16)
                at = pl.ds(pl.multiple_of(p * 256, 256), 256)
                part[i, 0, :, at] = product[:rows]
                part[i, 1, :, at] = product[rows:]
                return carry

            lax.fori_loop(0, n_sp // 2, column_step, 0)
            part_copy(i).start()

    own_attention()
    retention_out()
    for i in (1, 2):
        plane_copy(i).wait_recv()
        plane_relay(i).start()

    @pl.when(z == host)
    def _():
        for i in range(group):
            query_hop(i).wait_recv()

    earlier(1)
    for i in range(group):
        part_copy(i).wait_recv()
        rsum[i] = (part[i, tp].astype(f32) + part_in[i].astype(f32)).astype(bf16)
    for k in range(2):
        scatter_x(k).start()
        scatter_y(k).start()
    for step in range(2, depth):
        for i in range(group):
            take(step, i)
        earlier(step)

    for k in range(2):
        scatter_x(k).wait_recv()
        scatter_y(k).wait_recv()
    second_out[0] = (rsum[2, :, :half].astype(f32) + xa[1].astype(f32)).astype(bf16)
    second_out[1] = (rsum[1, :, half:].astype(f32) + yb[1].astype(f32)).astype(bf16)
    for k in range(2):
        scatter_second(k).start()

    @pl.when(z == last)
    def _():
        take_back()

    for i in range(group):
        for h in range(hfox):
            fox_buf[i, :, h * FOX_DIM : (h + 1) * FOX_DIM] = normalize(
                numer[i, h, :, :FOX_DIM] / numer[i, h, :, FOX_DIM:]
            )
        if i > 0:
            mixed_copy(i).start()
    mixed[:, my_cols] = fox_buf[0]
    for i in (1, 2):
        plane_relay(i).wait_recv()
    for i in range(1, group):
        mixed_copy(i).wait_recv()

    def fox_column(p, carry):
        right = jnp.concatenate(
            [wfox[near(2 * lax.rem(p, 2) + e), p // 2] for e in range(2)], axis=1
        )
        product = jnp.dot(mixed[...], right, preferred_element_type=f32).astype(bf16)
        at = pl.ds(pl.multiple_of(p * 256, 256), 256)
        fpart[0, :, at] = product[:rows]
        fpart[1, :, at] = product[rows:]
        return carry

    lax.fori_loop(0, n_sp // 2, fox_column, 0)
    final_copy().start()
    for k in range(2):
        scatter_second(k).wait_recv()
    final_copy().wait_recv()
    mine = fpart[tp].astype(f32) + fgot[...].astype(f32)
    ret_low = rsum[0, :, :half].astype(f32) + xa[0].astype(f32) + second_in[0].astype(f32)
    ret_high = rsum[0, :, half:].astype(f32) + yb[0].astype(f32) + second_in[1].astype(f32)
    out[:, :half] = (mine[:, :half] + ret_low).astype(bf16)
    out[:, half:] = (mine[:, half:] + ret_high).astype(bf16)

    for i in (1, 2):
        token_copy(i).wait_send()
        token_relay(i).wait_send()
        plane_copy(i).wait_send()
        plane_relay(i).wait_send()
    for i in range(group):
        pair_copy(i).wait_send()
        part_copy(i).wait_send()
    for i in range(1, group):
        rows_copy(i).wait_send()
        mixed_copy(i).wait_send()
    for i in range(1, n_sp):
        gate_copy(i).wait_send()
    for kind in range(3):
        settle_line(kind)
    for k in range(2):
        scatter_x(k).wait_send()
        scatter_y(k).wait_send()
        scatter_second(k).wait_send()
    final_copy().wait_send()

    @pl.when(z < last)
    def _():
        state_hop().wait_send()
        for i in range(group):
            kv_hop(z, i).wait_send()

    for step in range(1, depth):

        @pl.when((z - step >= 0) & (z < host))
        def _():
            for i in range(group):
                kv_hop(z - step, i).wait_send()

    @pl.when(z == last)
    def _():
        for i in range(group):
            query_hop(i).wait_send()

    @pl.when(z == host)
    def _():
        for i in range(group):
            num_hop(i).wait_send()
        den_hop().wait_send()


def fused(tokens, gain, gates, inverse, w_ret, w_fox, w_in, hret, hfox, n_sp):
    rows, width = tokens.shape
    group = 4
    tok = 2 * rows
    depth = n_sp // group
    out_cols = n_sp * w_ret.shape[1]
    half = out_cols // 2
    ret_rows = hret * RET_DIM
    fox_rows = group * hfox * FOX_DIM
    vmem = pl.BlockSpec(memory_space=pltpu.VMEM)
    hbm = pl.BlockSpec(memory_space=pl.ANY)
    dma = pltpu.SemaphoreType.DMA
    f32 = jnp.float32
    bf16 = jnp.bfloat16
    square = (hret, RET_DIM, RET_DIM)
    heads = (group, hfox, tok, FOX_DIM)
    dens = group * hfox * (tok // 128)
    total = float(tok * n_sp)

    def body(*refs):
        fused_kernel(n_sp, total, *refs[:6], refs[6:12], *refs[12:])

    V = pltpu.VMEM
    return pl.pallas_call(
        body,
        out_shape=jax.ShapeDtypeStruct((rows, out_cols), bf16),
        in_specs=[vmem] * 4 + [hbm] * 8,
        out_specs=vmem,
        scratch_shapes=[
            V((group, 2, rows, width), bf16),
            V((3, width, ret_rows), bf16),
            V((3, width, hfox * FOX_DIM), bf16),
            V(w_ret.shape, bf16),
            V((depth, group, ret_rows, w_ret.shape[1]), bf16),
            V((group, depth, fox_rows, w_ret.shape[1]), bf16),
            V((n_sp,) + gates.shape, f32),
            V((tok, RET_DIM // 2), f32),
            V((tok, RET_DIM // 2), f32),
            V((hret, tok, tok), f32),
            V((hret, tok, RET_DIM), f32),
            V((hret, tok, RET_DIM), f32),
            V((group, hret, tok, RET_DIM), bf16),
            V((group, hret, tok, RET_DIM), bf16),
            V((group, hret, tok, RET_DIM), bf16),
            V(heads, bf16),
            V(heads, bf16),
            V((depth, group, 2, hfox, tok, FOX_DIM), bf16),
            V((group, hret, tok, RET_DIM), f32),
            V((group,) + square, f32),
            V(square, bf16),
            V(square, bf16),
            V(square, f32),
            V((group, hfox, tok, 128), f32),
            V((group, hfox, tok, 128), f32),
            V((group, hfox, tok, 2 * FOX_DIM), f32),
            V((group, hfox, tok, 2 * FOX_DIM), f32),
            V(heads, bf16),
            V(heads, bf16),
            V((dens, 128), f32),
            V((dens, 128), f32),
            V((group, 2, rows, out_cols), bf16),
            V((group, rows, out_cols), bf16),
            V((group, rows, out_cols), bf16),
            V((2, rows, half), bf16),
            V((2, rows, half), bf16),
            V((2, rows, half), bf16),
            V((2, rows, half), bf16),
            V((group, tok, hfox * FOX_DIM), bf16),
            V((tok, fox_rows), bf16),
            V((2, rows, out_cols), bf16),
            V((rows, out_cols), bf16),
            dma((9,)),
            dma((3,)),
            dma((3,)),
            dma((3,)),
            dma((3,)),
            dma((group,)),
            dma((group,)),
            dma((n_sp,)),
            dma((n_sp,)),
            dma((group,)),
            dma((group,)),
            dma((3, depth)),
            dma((3, depth)),
            dma((3, depth)),
            dma((3, depth)),
            dma((5,)),
            dma((5,)),
            dma((depth, group)),
            dma((depth, group)),
            dma((group,)),
            dma((group,)),
            dma((1,)),
            dma((1,)),
            dma((group + 1,)),
            dma((group + 1,)),
            dma((group,)),
            dma((group,)),
            dma((6,)),
            dma((6,)),
            dma((group,)),
            dma((group,)),
        ],
        compiler_params=pltpu.CompilerParams(
            collective_id=2, has_side_effects=True, vmem_limit_bytes=VMEM_LIMIT
        ),
        name="fused",
    )(tokens, gain, gates, inverse, w_ret, w_fox, *w_in)


def decay_rates(head_ids, total):
    heads_float = head_ids.astype(jnp.float32)
    middle = RET_HEADS // 2
    fast_rate = 1.0 / (32.0 + 16.0 * heads_float)
    slow_rate = jnp.exp2(-(heads_float - middle)) / total
    return jnp.where(head_ids < middle, fast_rate, slow_rate)


def per_device(
    n_sp,
    n_tp,
    tokens,
    gain,
    w_ret_q,
    w_ret_k,
    w_ret_v,
    w_fox_q,
    w_fox_k,
    w_fox_v,
    fox_gates,
    w_out_ret,
    w_out_fox,
):
    f32 = jnp.float32
    rows, width = tokens.shape
    ret_heads = w_ret_q.shape[1] // RET_DIM
    fox_heads = w_fox_q.shape[1] // FOX_DIM
    group = math.gcd(math.gcd(ret_heads, fox_heads), n_sp)
    depth = n_sp // group
    hret = ret_heads // group
    hfox = fox_heads // group
    run = rows * n_tp * group
    half = RET_DIM // 2
    inverse = 10000.0 ** (-jnp.arange(half, dtype=f32) / half)
    if group == 4 and n_tp == 2 and depth > 2:
        return fused(
            tokens,
            gain.reshape(1, width),
            fox_gates.T,
            inverse.reshape(1, half),
            w_out_ret,
            w_out_fox,
            (w_ret_q, w_ret_k, w_ret_v, w_fox_q, w_fox_k, w_fox_v),
            hret,
            hfox,
            n_sp,
        )
    sp = lax.axis_index("sp")
    g = lax.rem(sp, group)
    z = sp // group

    positions = z * run + jnp.arange(run, dtype=jnp.int32)
    angles = positions.astype(f32)[:, None] * inverse[None, :]
    rq, rk, rv, fq, fkv, gall, wz = gather(
        tokens,
        gain.reshape(1, width),
        fox_gates.T,
        w_out_ret,
        w_out_fox,
        jnp.cos(angles),
        jnp.sin(angles),
        (w_ret_q, w_ret_k, w_ret_v, w_fox_q, w_fox_k, w_fox_v),
        hret,
        hfox,
        n_sp,
        n_tp,
        group,
    )

    head_ids = (
        lax.axis_index("tp") * ret_heads + g * hret + jnp.arange(hret, dtype=jnp.int32)
    )
    rates = decay_rates(head_ids, float(run * depth))
    offsets = jnp.arange(BLOCK, dtype=f32)
    spread = offsets[:, None] - offsets[None, :]
    causal = spread >= 0
    within = jnp.where(
        causal[None], jnp.exp(-rates[:, None, None] * jnp.where(causal, spread, 0.0)[None]), 0.0
    )
    steps = jnp.arange(run, dtype=f32)
    qdec = jnp.exp(-rates[:, None] * (steps[None, :] + 1.0))[:, :, None]
    kdec = jnp.exp(-rates[:, None] * (BLOCK - 1.0 - offsets[None, :]))[:, :, None]
    lengths = jnp.array([BLOCK, run], f32)
    bdec = jnp.broadcast_to(
        jnp.exp(-rates[:, None] * lengths[None, :])[:, :, None], (hret, 2, RET_DIM)
    )

    own_gates = lax.dynamic_slice_in_dim(gall, g * hfox, hfox, 1)
    line = own_gates.transpose(1, 0, 2).reshape(hfox, depth, 1, run)
    gq = lax.dynamic_index_in_dim(line, z, 1, False).reshape(hfox, run, 1)
    return mixer(
        rq, rk, rv, fq, fkv, gq, line, within, qdec, kdec, bdec, wz, rows, n_sp, n_tp, group
    )


def solution(mesh):
    in_specs = (
        P(("sp", "tp"), None),
        P(),
        P(None, "tp"),
        P(None, "tp"),
        P(None, "tp"),
        P(None, "tp"),
        P(None, "tp"),
        P(None, "tp"),
        P("sp", "tp"),
        P("tp", "sp"),
        P("tp", "sp"),
    )
    out_specs = P(("sp", "tp"), None)
    return jax.shard_map(
        functools.partial(per_device, mesh.shape["sp"], mesh.shape["tp"]),
        mesh=mesh,
        in_specs=in_specs,
        out_specs=out_specs,
        check_vma=False,
    )
```

```python
import functools
import math

import jax
import jax.numpy as jnp
from jax import lax
from jax.experimental import pallas as pl
from jax.experimental.pallas import tpu as pltpu
from jax.sharding import PartitionSpec as P

RET_HEADS = 8
RET_DIM = 256
FOX_DIM = 128
BLOCK = 128
MESH = pl.DeviceIdType.MESH
VMEM_LIMIT = 60 * 1024 * 1024

eps = 1e-06


def remote(src, dst, send, recv, sp, tp):
    return pltpu.make_async_remote_copy(
        src_ref=src,
        dst_ref=dst,
        send_sem=send,
        recv_sem=recv,
        device_id=(sp, tp),
        device_id_type=MESH,
    )


def gather_kernel(
    n_sp,
    n_tp,
    group,
    tok_ref,
    gain_ref,
    gates_ref,
    wr_ref,
    wf_ref,
    cos_ref,
    sin_ref,
    w_in,
    rq,
    rk,
    rv,
    fq,
    fkv,
    gall,
    wz,
    own,
    xall,
    w_ret,
    w_fox,
    local_sem,
    in_sem,
    tsend,
    trecv,
    dsend,
    drecv,
    psend,
    precv,
    gsend,
    grecv,
    usend,
    urecv,
    nsend,
    nrecv,
):
    sp = lax.axis_index("sp")
    tp = lax.axis_index("tp")
    g = lax.rem(sp, group)
    z = sp // group
    depth = n_sp // group
    rows = tok_ref.shape[0]
    half = rows // 2
    krows = wr_ref.shape[0]

    barrier = pltpu.get_barrier_semaphore()
    for i in range(1, n_sp):
        pl.semaphore_signal(
            barrier, inc=1, device_id=(lax.rem(sp + i, n_sp), tp), device_id_type=MESH
        )
    for i in range(1, n_tp):
        pl.semaphore_signal(
            barrier, inc=1, device_id=(sp, lax.rem(tp + i, n_tp)), device_id_type=MESH
        )

    loads = []
    for i in range(6):
        cut = w_ret if i < 3 else w_fox
        size = cut.shape[2]
        columns = pl.ds(pl.multiple_of(g * size, 128), size)
        loads.append(
            pltpu.make_async_copy(w_in[i].at[:, columns], cut.at[i % 3], in_sem.at[i])
        )

    values = tok_ref[...].astype(jnp.float32)
    scale = lax.rsqrt(jnp.mean(values * values, axis=1, keepdims=True) + eps)
    own[...] = (values * scale * gain_ref[...]).astype(jnp.bfloat16)
    copies = [
        pltpu.make_async_copy(wr_ref, wz.at[z, pl.ds(0, krows)], local_sem.at[0]),
        pltpu.make_async_copy(
            wf_ref, wz.at[z, pl.ds(krows, wf_ref.shape[0])], local_sem.at[1]
        ),
        pltpu.make_async_copy(gates_ref, gall.at[sp], local_sem.at[2]),
    ]
    for copy in copies + loads:
        copy.start()
    pl.semaphore_wait(barrier, n_sp + n_tp - 2)

    def slot(which, core):
        return xall.at[which * n_tp + core]

    mine = pltpu.make_async_copy(own, slot(g, tp), local_sem.at[3])
    mine.start()

    def peer(other):
        return z * group + other

    hyper = group == 4
    direct = []
    for i in range(1, group):
        if hyper and i == 3:
            continue
        other = lax.bitwise_xor(g, i) if hyper else lax.rem(g + i, group)
        direct.append(
            remote(own, slot(g, tp), tsend.at[i], trecv.at[i], peer(other), tp)
        )
    for copy in direct:
        copy.start()
    pair = []
    for i in range(1, n_tp):
        copy = remote(
            own, slot(g, tp), psend.at[0, i], precv.at[0, i], sp, lax.rem(tp + i, n_tp)
        )
        copy.start()
        pair.append(copy)
    gate_copies = []
    for i in range(1, n_sp):
        copy = remote(
            gates_ref, gall.at[sp], gsend.at[i], grecv.at[i], lax.rem(sp + i, n_sp), tp
        )
        copy.start()
        gate_copies.append(copy)

    copies[0].wait()
    copies[1].wait()

    def up(block):
        return remote(
            wz.at[block],
            wz.at[block],
            usend.at[block],
            urecv.at[block],
            lax.rem(sp + group, n_sp),
            tp,
        )

    def down(block):
        return remote(
            wz.at[block],
            wz.at[block],
            nsend.at[block],
            nrecv.at[block],
            lax.rem(sp + n_sp - group, n_sp),
            tp,
        )

    @pl.when(z < depth - 1)
    def _():
        up(z).start()

    @pl.when(z > 0)
    def _():
        down(z).start()

    ready = {0: pair[:]}

    def forward(which, row):
        ready[row] = []
        for i in range(1, n_tp):
            copy = remote(
                slot(which, tp),
                slot(which, tp),
                psend.at[row, i],
                precv.at[row, i],
                sp,
                lax.rem(tp + i, n_tp),
            )
            copy.start()
            pair.append(copy)
            ready[row].append(copy)

    count = n_tp * rows
    half_head = RET_DIM // 2

    def project(which, row):
        for copy in ready[row]:
            copy.wait_recv()
        x = xall[pl.ds(which * n_tp, n_tp)].reshape(count, xall.shape[2])
        span = pl.ds(pl.multiple_of(which * count, count), count)
        for i in range(6):
            cut = w_ret if i < 3 else w_fox
            y = jnp.dot(x, cut[i % 3], preferred_element_type=jnp.float32)
            y = y.astype(jnp.bfloat16)
            if i < 2:
                cosine = cos_ref[span, :]
                sine = sin_ref[span, :]
            for h in range(rq.shape[0] if i < 3 else fq.shape[0]):
                if i < 2:
                    lo = h * RET_DIM
                    a = y[:, lo : lo + half_head].astype(jnp.float32)
                    b = y[:, lo + half_head : lo + RET_DIM].astype(jnp.float32)
                    to = rq if i == 0 else rk
                    by = 1.0 if i == 0 else RET_DIM ** (-0.5)
                    first = (a * cosine - b * sine) * by
                    second = (a * sine + b * cosine) * by
                    to[h, span, :half_head] = first.astype(jnp.bfloat16)
                    to[h, span, half_head:] = second.astype(jnp.bfloat16)
                elif i == 2:
                    rv[h, span, :] = y[:, h * RET_DIM : (h + 1) * RET_DIM]
                elif i == 3:
                    fq[h, span, :] = y[:, h * FOX_DIM : (h + 1) * FOX_DIM]
                else:
                    fkv[i - 4, h, span, :] = y[:, h * FOX_DIM : (h + 1) * FOX_DIM]

    mine.wait()
    for copy in loads:
        copy.wait()
    if not hyper:
        project(g, 0)

    if hyper:
        relays = []
        for i in (1, 2):
            direct[i - 1].wait_recv()
            source = lax.bitwise_xor(g, i)
            target = lax.bitwise_xor(g, 3 - i)
            part = pl.ds((i - 1) * half, half)
            copy = remote(
                slot(source, tp).at[part],
                slot(source, tp).at[part],
                dsend.at[i],
                drecv.at[i],
                peer(target),
                tp,
            )
            copy.start()
            relays.append(copy)
            forward(source, i)
        project(g, 0)
    else:
        for i in range(1, group):
            direct[i - 1].wait_recv()
            forward(lax.rem(g + group - i, group), i)
            project(lax.rem(g + group - i, group), i)

    def line(step, carry):
        below = z - step
        above = z + step

        @pl.when(below >= 0)
        def _():
            up(below).wait_recv()

            @pl.when(z < depth - 1)
            def _():
                up(below).start()

        @pl.when(above <= depth - 1)
        def _():
            down(above).wait_recv()

            @pl.when(z > 0)
            def _():
                down(above).start()

        return carry

    split = depth // 2 if hyper else depth
    lax.fori_loop(1, split, line, 0)
    if hyper:
        project(lax.bitwise_xor(g, 1), 1)
        for copy in relays:
            copy.wait_recv()
        forward(lax.bitwise_xor(g, 3), 3)
    lax.fori_loop(split, depth - 1, line, 0)
    if hyper:
        project(lax.bitwise_xor(g, 2), 2)
        project(lax.bitwise_xor(g, 3), 3)
    lax.fori_loop(max(split, depth - 1), depth, line, 0)

    def settle(step, carry):
        @pl.when((z < depth - 1) & (step <= z))
        def _():
            up(step).wait_send()

        @pl.when((z > 0) & (step >= z))
        def _():
            down(step).wait_send()

        return carry

    lax.fori_loop(0, depth, settle, 0)
    for copy in direct:
        copy.wait_send()
    if hyper:
        for copy in relays:
            copy.wait_send()
    for copy in gate_copies:
        copy.wait()
    for copy in pair:
        copy.wait_send()
    copies[2].wait()


def gather(
    tokens, gain, gates, w_ret, w_fox, cosine, sine, w_in, hret, hfox, n_sp, n_tp, group
):
    rows, width = tokens.shape
    depth = n_sp // group
    out_rows = w_ret.shape[0] + w_fox.shape[0]
    vmem = pl.BlockSpec(memory_space=pltpu.VMEM)
    hbm = pl.BlockSpec(memory_space=pl.ANY)
    dma = pltpu.SemaphoreType.DMA
    run = rows * n_tp * group
    bf16 = jnp.bfloat16

    def body(*refs):
        gather_kernel(n_sp, n_tp, group, *refs[:7], refs[7:13], *refs[13:])

    return pl.pallas_call(
        body,
        out_shape=(
            jax.ShapeDtypeStruct((hret, run, RET_DIM), bf16),
            jax.ShapeDtypeStruct((hret, run, RET_DIM), bf16),
            jax.ShapeDtypeStruct((hret, run, RET_DIM), bf16),
            jax.ShapeDtypeStruct((hfox, run, FOX_DIM), bf16),
            jax.ShapeDtypeStruct((2, hfox, run, FOX_DIM), bf16),
            jax.ShapeDtypeStruct((n_sp,) + gates.shape, jnp.float32),
            jax.ShapeDtypeStruct((depth, out_rows, w_ret.shape[1]), jnp.bfloat16),
        ),
        in_specs=[vmem, vmem, vmem, hbm, hbm, vmem, vmem] + [hbm] * 6,
        out_specs=(vmem,) * 7,
        scratch_shapes=[
            pltpu.VMEM((rows, width), bf16),
            pltpu.VMEM((group * n_tp, rows, width), bf16),
            pltpu.VMEM((3, width, hret * RET_DIM), bf16),
            pltpu.VMEM((3, width, hfox * FOX_DIM), bf16),
            dma((4,)),
            dma((6,)),
            dma((max(group, 2),)),
            dma((max(group, 2),)),
            dma((3,)),
            dma((3,)),
            dma((group, n_tp)),
            dma((group, n_tp)),
            dma((n_sp,)),
            dma((n_sp,)),
            dma((depth,)),
            dma((depth,)),
            dma((depth,)),
            dma((depth,)),
        ],
        compiler_params=pltpu.CompilerParams(
            collective_id=0, has_side_effects=True, vmem_limit_bytes=VMEM_LIMIT
        ),
        name="gather",
    )(tokens, gain, gates, w_ret, w_fox, cosine, sine, *w_in)


def normalize(values):
    return (
        values * lax.rsqrt(jnp.mean(values * values, axis=1, keepdims=True) + eps)
    ).astype(jnp.bfloat16)


def mixer_kernel(
    n_sp,
    n_tp,
    group,
    rq,
    rk,
    rv,
    fq,
    fkv,
    gq,
    gk,
    within,
    qdec,
    kdec,
    bdec,
    wz,
    out,
    w_all,
    slots,
    raw,
    state,
    state_in,
    state_out,
    numer,
    denom,
    ret_buf,
    fox_buf,
    mixed,
    part,
    got,
    local_sem,
    ksend,
    krecv,
    ssend,
    srecv,
    wsend,
    wrecv,
    dsend,
    drecv,
    asend,
    arecv,
    osend,
    orecv,
):
    sp = lax.axis_index("sp")
    tp = lax.axis_index("tp")
    g = lax.rem(sp, group)
    z = sp // group
    depth = n_sp // group
    hret = rq.shape[0]
    hfox = fq.shape[0]
    run = rq.shape[1]
    tok = run // group
    rows = out.shape[0]
    after = lax.rem(sp + group, n_sp)
    before = lax.rem(sp + n_sp - group, n_sp)
    f32 = jnp.float32

    def peer(other):
        return z * group + other

    barrier = pltpu.get_barrier_semaphore()
    for i in range(1, group):
        pl.semaphore_signal(
            barrier, inc=1, device_id=(peer(lax.rem(g + i, group)), tp), device_id_type=MESH
        )
    for i in range(1, n_tp):
        pl.semaphore_signal(
            barrier, inc=1, device_id=(sp, lax.rem(tp + i, n_tp)), device_id_type=MESH
        )
    if depth > 1:

        @pl.when(z < depth - 1)
        def _():
            pl.semaphore_signal(barrier, inc=1, device_id=(after, tp), device_id_type=MESH)

        @pl.when(z > 0)
        def _():
            pl.semaphore_signal(barrier, inc=1, device_id=(before, tp), device_id_type=MESH)

    ends = (z + depth - 1) // depth + (2 * depth - 2 - z) // depth
    pl.semaphore_wait(barrier, group + n_tp - 2 + ends)

    def first_hop():
        return remote(fkv, slots.at[z], ksend.at[z], krecv.at[z], after, tp)

    def hop(block):
        return remote(
            slots.at[block], slots.at[block], ksend.at[block], krecv.at[block], after, tp
        )

    if depth > 1:

        @pl.when(z < depth - 1)
        def _():
            first_hop().start()

    hyper = group == 4
    mine = pltpu.make_async_copy(wz, w_all.at[g], local_sem.at[0])
    mine.start()
    direct = []
    for i in range(1, group):
        if hyper and i == 3:
            continue
        other = lax.bitwise_xor(g, i) if hyper else lax.rem(g + i, group)
        direct.append(
            remote(wz, w_all.at[g], wsend.at[i], wrecv.at[i], peer(other), tp)
        )
    for copy in direct:
        copy.start()

    def relay(i):
        source = lax.bitwise_xor(g, i)
        target = lax.bitwise_xor(g, 3 - i)
        span = pl.ds((i - 1) * (depth // 2), depth // 2)
        return remote(
            w_all.at[source, span],
            w_all.at[source, span],
            dsend.at[i],
            drecv.at[i],
            peer(target),
            tp,
        )

    for h in range(hret):
        state[h] = jnp.zeros(state.shape[1:], f32)

        def ret_step(b, carry):
            span = pl.ds(pl.multiple_of(b * BLOCK, BLOCK), BLOCK)
            q = rq[h, span, :]
            k = rk[h, span, :]
            v = rv[h, span, :]
            scores = (
                lax.dot_general(q, k, (((1,), (1,)), ((), ())), preferred_element_type=f32)
                * within[h]
            )
            inner = jnp.dot(scores.astype(jnp.bfloat16), v, preferred_element_type=f32)
            held = state[h]
            cross = jnp.dot(q, held.astype(jnp.bfloat16), preferred_element_type=f32)
            raw[h, span, :] = inner + cross * qdec[h, pl.ds(0, BLOCK), :]
            scaled = (k.astype(f32) * kdec[h]).astype(jnp.bfloat16)
            update = lax.dot_general(
                scaled, v, (((0,), (0,)), ((), ())), preferred_element_type=f32
            )
            state[h] = held * bdec[h, 0:1, :] + update
            return carry

        lax.fori_loop(0, run // BLOCK, ret_step, 0)

    def state_hop():
        return remote(state_out, state_in, ssend.at[0], srecv.at[0], after, tp)

    if depth > 1:

        @pl.when(z == 0)
        def _():
            state_out[...] = state[...]
            state_hop().start()

    tile = math.gcd(run, 256)
    inverse = FOX_DIM ** (-0.5)

    def attend(h, t, keys, values, key_gates, diagonal, fresh):
        span = pl.ds(pl.multiple_of(t * tile, tile), tile)
        scores = (
            lax.dot_general(
                fq[h, span, :], keys, (((1,), (1,)), ((), ())), preferred_element_type=f32
            )
            * inverse
        )
        scores = scores + gq[h, span, :] - key_gates
        if diagonal:
            row = lax.broadcasted_iota(jnp.int32, scores.shape, 0)
            col = lax.broadcasted_iota(jnp.int32, scores.shape, 1)
            scores = jnp.where(col <= row, scores, -jnp.inf)
        weights = jnp.exp(scores)
        total = jnp.sum(weights, axis=1, keepdims=True)
        product = jnp.dot(weights.astype(jnp.bfloat16), values, preferred_element_type=f32)
        if fresh:
            numer[h, span, :] = product
            denom[h, span, :] = total
        else:
            numer[h, span, :] += product
            denom[h, span, :] += total

    for h in range(hfox):
        for t in range(run // tile):
            for s in range(t, -1, -1):
                span = pl.ds(s * tile, tile)
                attend(
                    h,
                    t,
                    fkv[0, h, span, :],
                    fkv[1, h, span, :],
                    gk[h, z, :, span],
                    s == t,
                    s == t,
                )

    def carried():
        state_hop().wait_recv()

        @pl.when(z < depth - 1)
        def _():
            for h in range(hret):
                state_out[h] = state_in[h] * bdec[h, 1:2, :] + state[h]
            state_hop().start()

        for h in range(hret):
            held = state_in[h].astype(jnp.bfloat16)

            def cross_step(b, carry):
                span = pl.ds(pl.multiple_of(b * tile, tile), tile)
                cross = jnp.dot(rq[h, span, :], held, preferred_element_type=f32)
                raw[h, span, :] += cross * qdec[h, span, :]
                return carry

            lax.fori_loop(0, run // tile, cross_step, 0)

    def earlier(step, carry):
        @pl.when(step <= z)
        def _():
            block = z - step
            hop(block).wait_recv()

            @pl.when(z < depth - 1)
            def _():
                hop(block).start()

            for h in range(hfox):

                def query_step(t, c):
                    attend(
                        h,
                        t,
                        slots[block, 0, h],
                        slots[block, 1, h],
                        gk[h, block],
                        False,
                        False,
                    )
                    return c

                lax.fori_loop(0, run // tile, query_step, 0)

        return carry

    if depth > 1:
        lax.fori_loop(1, 2, earlier, 0)

        @pl.when(z > 0)
        def _():
            carried()

        if hyper:
            direct[0].wait_recv()
            relay(1).start()
            direct[1].wait_recv()
            relay(2).start()
        lax.fori_loop(2, depth, earlier, 0)
    elif hyper:
        direct[0].wait_recv()
        relay(1).start()
        direct[1].wait_recv()
        relay(2).start()

    rw = hret * RET_DIM
    fw = hfox * FOX_DIM
    for t in range(group):
        span = pl.ds(t * tok, tok)
        for h in range(hret):
            ret_buf[t, :, h * RET_DIM : (h + 1) * RET_DIM] = normalize(raw[h, span, :])
        for h in range(hfox):
            fox_buf[t, :, h * FOX_DIM : (h + 1) * FOX_DIM] = normalize(
                numer[h, span, :] / denom[h, span, :]
            )
    ret_cols = pl.ds(pl.multiple_of(g * rw, 128), rw)
    fox_cols = pl.ds(pl.multiple_of(group * rw + g * fw, 128), fw)
    exchange = []
    for i in range(1, group):
        other = lax.rem(g + i, group)
        for kind, (buf, cols) in enumerate(((ret_buf, ret_cols), (fox_buf, fox_cols))):
            copy = remote(
                buf.at[other],
                mixed.at[:, cols],
                asend.at[kind, i],
                arecv.at[kind, i],
                peer(other),
                tp,
            )
            copy.start()
            exchange.append(copy)
    mixed[:, ret_cols] = ret_buf[g]
    mixed[:, fox_cols] = fox_buf[g]
    for copy in exchange:
        copy.wait_recv()
    mine.wait()
    if hyper:
        relay(1).wait_recv()
        relay(2).wait_recv()
    else:
        for copy in direct:
            copy.wait_recv()

    cols = w_all.shape[3]
    pack = max(1, 128 // cols)
    wide = pack * cols
    for t in range(n_tp):
        left = mixed[t * rows : (t + 1) * rows, :]

        def column(p, carry, left=left, t=t):
            blocks = [
                w_all[lax.rem(p * pack + i, group), (p * pack + i) // group]
                for i in range(pack)
            ]
            right = blocks[0] if pack == 1 else jnp.concatenate(blocks, axis=1)
            product = jnp.dot(left, right, preferred_element_type=f32)
            at = pl.ds(pl.multiple_of(p * wide, wide), wide)
            part[t, :, at] = product.astype(jnp.bfloat16)
            return carry

        lax.fori_loop(0, n_sp // pack, column, 0)
    final = []
    for i in range(1, n_tp):
        other = lax.rem(tp + i, n_tp)
        copy = remote(part.at[other], got.at[i], osend.at[i], orecv.at[i], sp, other)
        copy.start()
        final.append(copy)
    total = part[tp].astype(f32)
    for i in range(1, n_tp):
        final[i - 1].wait_recv()
        total = total + got[i].astype(f32)
    out[...] = total.astype(jnp.bfloat16)

    for copy in final + exchange + direct:
        copy.wait_send()
    if hyper:
        relay(1).wait_send()
        relay(2).wait_send()
    if depth > 1:

        @pl.when(z < depth - 1)
        def _():
            first_hop().wait_send()
            state_hop().wait_send()

            def settle(block, carry):
                @pl.when(block < z)
                def _():
                    hop(block).wait_send()

                return carry

            lax.fori_loop(0, depth, settle, 0)


def mixer(rq, rk, rv, fq, fkv, gq, gk, within, qdec, kdec, bdec, wz, rows, n_sp, n_tp, group):
    depth = n_sp // group
    hret, run, _ = rq.shape
    hfox = fq.shape[0]
    tok = run // group
    out_rows, cols = wz.shape[1:]
    width = n_sp * cols
    vmem = pl.BlockSpec(memory_space=pltpu.VMEM)
    dma = pltpu.SemaphoreType.DMA
    f32 = jnp.float32
    bf16 = jnp.bfloat16
    square = (hret, RET_DIM, RET_DIM)
    return pl.pallas_call(
        functools.partial(mixer_kernel, n_sp, n_tp, group),
        out_shape=jax.ShapeDtypeStruct((rows, width), bf16),
        in_specs=[vmem] * 11 + [pl.BlockSpec(memory_space=pl.ANY)],
        out_specs=vmem,
        scratch_shapes=[
            pltpu.VMEM((group,) + wz.shape, bf16),
            pltpu.VMEM((depth,) + fkv.shape, bf16),
            pltpu.VMEM((hret, run, RET_DIM), f32),
            pltpu.VMEM(square, f32),
            pltpu.VMEM(square, f32),
            pltpu.VMEM(square, f32),
            pltpu.VMEM((hfox, run, FOX_DIM), f32),
            pltpu.VMEM((hfox, run, 1), f32),
            pltpu.VMEM((group, tok, hret * RET_DIM), bf16),
            pltpu.VMEM((group, tok, hfox * FOX_DIM), bf16),
            pltpu.VMEM((tok, out_rows), bf16),
            pltpu.VMEM((n_tp, rows, width), bf16),
            pltpu.VMEM((n_tp, rows, width), bf16),
            dma((1,)),
            dma((depth,)),
            dma((depth,)),
            dma((1,)),
            dma((1,)),
            dma((max(group, 2),)),
            dma((max(group, 2),)),
            dma((3,)),
            dma((3,)),
            dma((2, group)),
            dma((2, group)),
            dma((n_tp,)),
            dma((n_tp,)),
        ],
        compiler_params=pltpu.CompilerParams(
            collective_id=1, has_side_effects=True, vmem_limit_bytes=VMEM_LIMIT
        ),
        name="mixer",
    )(rq, rk, rv, fq, fkv, gq, gk, within, qdec, kdec, bdec, wz)


def fused_kernel(
    n_sp,
    total,
    tok_ref,
    gain_ref,
    gates_ref,
    inv_ref,
    wr_ref,
    wf_ref,
    w_in,
    out,
    xall,
    w_ret,
    w_fox,
    wrs,
    wret,
    wfox,
    gall,
    ctab,
    stab,
    within,
    qdec,
    kdec,
    rq,
    rk,
    rv,
    fq,
    guest,
    kv,
    raw,
    update,
    state_in,
    state_out,
    carry_state,
    gcol,
    guest_col,
    numer,
    guest_numer,
    num_out,
    num_in,
    den_out,
    den_in,
    part,
    part_in,
    rsum,
    xa,
    yb,
    second_out,
    second_in,
    fox_buf,
    mixed,
    fpart,
    fgot,
    local_sem,
    tsend,
    trecv,
    dsend,
    drecv,
    psend,
    precv,
    gsend,
    grecv,
    asend,
    arecv,
    usend,
    urecv,
    nsend,
    nrecv,
    fsend,
    frecv,
    ksend,
    krecv,
    qsend,
    qrecv,
    ssend,
    srecv,
    osend,
    orecv,
    psum_send,
    psum_recv,
    rsend,
    rrecv,
    esend,
    erecv,
):
    f32 = jnp.float32
    bf16 = jnp.bfloat16
    group = 4
    sp = lax.axis_index("sp")
    tp = lax.axis_index("tp")
    other_core = 1 - tp
    g = lax.rem(sp, group)
    z = sp // group
    depth = n_sp // group
    last = depth - 1
    host = depth - 2
    rows = tok_ref.shape[0]
    tok = 2 * rows
    hret = rq.shape[1]
    hfox = fq.shape[1]
    ret_rows = hret * RET_DIM
    after = lax.rem(sp + group, n_sp)
    before = lax.rem(sp + n_sp - group, n_sp)

    def near(i):
        return lax.bitwise_xor(g, i)

    def peer(i):
        return z * group + near(i)

    barrier = pltpu.get_barrier_semaphore()
    for i in range(1, n_sp):
        pl.semaphore_signal(
            barrier, inc=1, device_id=(lax.rem(sp + i, n_sp), tp), device_id_type=MESH
        )
    pl.semaphore_signal(barrier, inc=1, device_id=(sp, other_core), device_id_type=MESH)

    locals_ = [
        pltpu.make_async_copy(wr_ref, wrs, local_sem.at[0]),
        pltpu.make_async_copy(
            wr_ref.at[pl.ds(pl.multiple_of(g * ret_rows, ret_rows), ret_rows)],
            wret.at[z, 0],
            local_sem.at[1],
        ),
        pltpu.make_async_copy(wf_ref, wfox.at[0, z], local_sem.at[2]),
    ]
    loads = []
    for i in range(6):
        cut = w_ret if i < 3 else w_fox
        size = cut.shape[2]
        columns = pl.ds(pl.multiple_of(g * size, 128), size)
        loads.append(
            pltpu.make_async_copy(
                w_in[i].at[:, columns], cut.at[i % 3], local_sem.at[3 + i]
            )
        )
    for copy in locals_ + loads:
        copy.start()

    values = tok_ref[...].astype(f32)
    scale = lax.rsqrt(jnp.mean(values * values, axis=1, keepdims=True) + eps)
    xall[0, tp] = (values * scale * gain_ref[...]).astype(bf16)
    gall[sp] = gates_ref[...]
    with jax.named_scope("barrier"):
        pl.semaphore_wait(barrier, n_sp)

    def token_copy(i):
        return remote(xall.at[0, tp], xall.at[i, tp], tsend.at[i], trecv.at[i], peer(i), tp)

    def token_relay(i):
        span = pl.ds((i - 1) * (rows // 2), rows // 2)
        return remote(
            xall.at[i, tp, span],
            xall.at[3, tp, span],
            dsend.at[i],
            drecv.at[i],
            peer(3 - i),
            tp,
        )

    def pair_copy(i):
        return remote(
            xall.at[i, tp], xall.at[i, tp], psend.at[i], precv.at[i], sp, other_core
        )

    def gate_copy(i):
        return remote(
            gates_ref, gall.at[sp], gsend.at[i], grecv.at[i], lax.rem(sp + i, n_sp), tp
        )

    def rows_copy(i):
        span = pl.ds(pl.multiple_of(near(i) * ret_rows, ret_rows), ret_rows)
        return remote(wrs.at[span], wret.at[z, i], asend.at[i], arecv.at[i], peer(i), tp)

    def cut_of(kind, block):
        if kind == 0:
            return wfox.at[0, block]
        if kind == 1:
            return wret.at[block, 0]
        return wret.at[block, pl.ds(1, group - 1)]

    def up(kind, block):
        ref = cut_of(kind, block)
        return remote(ref, ref, usend.at[kind, block], urecv.at[kind, block], after, tp)

    def down(kind, block):
        ref = cut_of(kind, block)
        return remote(ref, ref, nsend.at[kind, block], nrecv.at[kind, block], before, tp)

    def begin_line(kind):
        @pl.when(z < last)
        def _():
            up(kind, z).start()

        @pl.when(z > 0)
        def _():
            down(kind, z).start()

    def line(kind, step):
        below = z - step
        above = z + step

        @pl.when(below >= 0)
        def _():
            up(kind, below).wait_recv()

            @pl.when(z < last)
            def _():
                up(kind, below).start()

        @pl.when(above <= last)
        def _():
            down(kind, above).wait_recv()

            @pl.when(z > 0)
            def _():
                down(kind, above).start()

    def settle_line(kind):
        for block in range(depth):

            @pl.when((z < last) & (block <= z))
            def _():
                up(kind, block).wait_send()

            @pl.when((z > 0) & (block >= z))
            def _():
                down(kind, block).wait_send()

    def plane_copy(i):
        return remote(wfox.at[0], wfox.at[i], fsend.at[i], frecv.at[i], peer(i), tp)

    def plane_relay(i):
        span = pl.ds(0, depth // 2) if i == 1 else pl.ds(depth // 2, depth - depth // 2)
        return remote(
            wfox.at[i, span],
            wfox.at[3, span],
            fsend.at[2 + i],
            frecv.at[2 + i],
            peer(3 - i),
            tp,
        )

    def kv_hop(block, i):
        ref = kv.at[block, i]
        return remote(ref, ref, ksend.at[block, i], krecv.at[block, i], after, tp)

    def query_hop(i):
        return remote(fq.at[i], guest.at[i], qsend.at[i], qrecv.at[i], before, tp)

    def state_hop():
        return remote(state_out, state_in, ssend.at[0], srecv.at[0], after, tp)

    def num_hop(i):
        return remote(num_out.at[i], num_in.at[i], osend.at[i], orecv.at[i], after, tp)

    def den_hop():
        return remote(den_out, den_in, osend.at[group], orecv.at[group], after, tp)

    def part_copy(i):
        return remote(
            part.at[i, other_core],
            part_in.at[i],
            psum_send.at[i],
            psum_recv.at[i],
            sp,
            other_core,
        )

    width = out.shape[1]
    half = width // 2
    wide = width // depth
    first_cols = pl.ds(0, half)
    last_cols = pl.ds(half, half)

    def scatter_x(k):
        return remote(
            rsum.at[1 + 2 * k, :, first_cols],
            xa.at[k],
            rsend.at[k],
            rrecv.at[k],
            peer(1),
            tp,
        )

    def scatter_y(k):
        return remote(
            rsum.at[2 + k, :, last_cols],
            yb.at[k],
            rsend.at[2 + k],
            rrecv.at[2 + k],
            peer(2),
            tp,
        )

    def scatter_second(k):
        return remote(
            second_out.at[k],
            second_in.at[k],
            rsend.at[4 + k],
            rrecv.at[4 + k],
            peer(2 if k == 0 else 1),
            tp,
        )

    fw = hfox * FOX_DIM
    my_cols = pl.ds(pl.multiple_of(g * fw, 128), fw)

    def mixed_copy(i):
        return remote(
            fox_buf.at[i], mixed.at[:, my_cols], esend.at[i], erecv.at[i], peer(i), tp
        )

    def final_copy():
        return remote(
            fpart.at[other_core], fgot, esend.at[0], erecv.at[0], sp, other_core
        )

    for i in (1, 2):
        token_copy(i).start()
    pair_copy(0).start()
    with jax.named_scope("first_sends"):
        for i in range(1, n_sp):
            gate_copy(i).start()
        for copy in locals_:
            copy.wait()
        for i in range(1, group):
            rows_copy(i).start()
        begin_line(0)
        begin_line(1)

    head_of = [tp * (group * hret) + g * hret + h for h in range(hret)]
    rates = []
    for h in range(hret):
        ids = jnp.full((1, RET_DIM), head_of[h], jnp.int32)
        heads_float = ids.astype(f32)
        middle = RET_HEADS // 2
        fast_rate = 1.0 / (32.0 + 16.0 * heads_float)
        slow_rate = jnp.exp2(-(heads_float - middle)) / total
        rates.append(jnp.where(ids < middle, fast_rate, slow_rate))
    square = (tok, RET_DIM)
    offset = lax.broadcasted_iota(jnp.int32, square, 0)
    column = lax.broadcasted_iota(jnp.int32, (tok, tok), 1)
    row = lax.broadcasted_iota(jnp.int32, (tok, tok), 0)
    for h in range(hret):
        rate = rates[h]
        spread = jnp.maximum(row - column, 0).astype(f32)
        within[h] = jnp.where(row >= column, jnp.exp(-rate[:, :1] * spread), 0.0)
        steps = offset.astype(f32)
        qdec[h] = jnp.exp(-rate * (steps + 1.0))
        kdec[h] = jnp.exp(-rate * (tok - 1.0 - steps))
    inverse_freq = inv_ref[...]
    unit = 16
    low = lax.broadcasted_iota(jnp.int32, (unit, RET_DIM // 2), 0).astype(f32)
    high = lax.broadcasted_iota(jnp.int32, (tok // unit, RET_DIM // 2), 0).astype(f32)
    cos_low, sin_low = jnp.cos(low * inverse_freq), jnp.sin(low * inverse_freq)
    high = high * float(unit) * inverse_freq
    cos_high, sin_high = jnp.cos(high), jnp.sin(high)
    for a in range(tok // unit):
        ca, sa = cos_high[a : a + 1], sin_high[a : a + 1]
        ctab[a * unit : (a + 1) * unit] = cos_low * ca - sin_low * sa
        stab[a * unit : (a + 1) * unit] = sin_low * ca + cos_low * sa

    half_head = RET_DIM // 2

    run_decay = [jnp.exp(-rates[h] * float(group * tok)) for h in range(hret)]
    tok_decay = [jnp.exp(-rates[h] * float(tok)) for h in range(hret)]

    def sum_state():
        for h in range(hret):
            held = update[g, h]
            for p in range(1, group):
                held = held * tok_decay[h] + update[near(p), h]
            carry_state[h] = held

        @pl.when(z == 0)
        def _():
            state_out[...] = carry_state[...].astype(bf16)
            state_hop().start()

    def retain(i):
        for h in range(hret):
            q = rq[i, h]
            k = rk[i, h]
            v = rv[i, h]
            scores = (
                lax.dot_general(q, k, (((1,), (1,)), ((), ())), preferred_element_type=f32)
                * within[h]
            )
            raw[i, h] = jnp.dot(scores.astype(bf16), v, preferred_element_type=f32)

    def gather_state(i):
        for h in range(hret):
            scaled = (rk[i, h].astype(f32) * kdec[h]).astype(bf16)
            update[i, h] = lax.dot_general(
                scaled, rv[i, h], (((0,), (0,)), ((), ())), preferred_element_type=f32
            )

    def project(i):
        x = xall[i].reshape(tok, xall.shape[3])
        start = jnp.full((1, half_head), z * (group * tok) + near(i) * tok, jnp.int32)
        turn = start.astype(f32) * inverse_freq
        cos_turn, sin_turn = jnp.cos(turn), jnp.sin(turn)
        for m in (4, 5, 3, 1, 2, 0) if i < 3 else (1, 2, 4, 5, 3, 0):
            cut = w_ret if m < 3 else w_fox
            y = jnp.dot(x, cut[m % 3], preferred_element_type=f32).astype(bf16)
            if m < 2:
                cosine = ctab[...] * cos_turn - stab[...] * sin_turn
                sine = stab[...] * cos_turn + ctab[...] * sin_turn
            for h in range(hret if m < 3 else hfox):
                if m < 2:
                    lo = h * RET_DIM
                    a = y[:, lo : lo + half_head].astype(f32)
                    b = y[:, lo + half_head : lo + RET_DIM].astype(f32)
                    to = rq if m == 0 else rk
                    by = 1.0 if m == 0 else RET_DIM ** (-0.5)
                    to[i, h, :, :half_head] = ((a * cosine - b * sine) * by).astype(bf16)
                    to[i, h, :, half_head:] = ((a * sine + b * cosine) * by).astype(bf16)
                elif m == 2:
                    rv[i, h] = y[:, h * RET_DIM : (h + 1) * RET_DIM]
                elif m == 3:
                    fq[i, h] = y[:, h * FOX_DIM : (h + 1) * FOX_DIM]
                else:
                    kv[z, i, m - 4, h] = y[:, h * FOX_DIM : (h + 1) * FOX_DIM]
            if m == 2:
                gather_state(i)
                if i == 3:
                    sum_state()
            if m == 5:

                @pl.when(z < last)
                def _():
                    kv_hop(z, i).start()

            if m == 3:

                @pl.when(z == last)
                def _():
                    query_hop(i).start()

    def take(step, i):
        block = z - step
        wanted = block >= 0
        if step > 1:
            wanted = wanted & (z < last)

        @pl.when(wanted)
        def _():
            kv_hop(block, i).wait_recv()

            @pl.when(z < host)
            def _():
                kv_hop(block, i).start()

    def phase(name, *steps):
        with jax.named_scope(name):
            for step in steps:
                step[0](*step[1:])

    def wait_loads():
        for copy in loads:
            copy.wait()
        pair_copy(0).wait_recv()

    def tokens_on(i):
        token_copy(i).wait_recv()
        token_relay(i).start()
        pair_copy(i).start()

    def wait_rows():
        for i in range(1, group):
            rows_copy(i).wait_recv()

    def wait_pair(i):
        pair_copy(i).wait_recv()

    def tokens_last():
        for i in (1, 2):
            token_relay(i).wait_recv()
        pair_copy(3).start()

    def begin_plane():
        for i in (1, 2):
            plane_copy(i).start()

    def pass_state():
        @pl.when(z > 0)
        def _():
            state_hop().wait_recv()

            @pl.when(z < last)
            def _():
                for h in range(hret):
                    held = state_in[h].astype(f32) * run_decay[h] + carry_state[h]
                    state_out[h] = held.astype(bf16)
                state_hop().start()

            carry_state[...] = state_in[...].astype(f32)

        @pl.when(z == 0)
        def _():
            carry_state[...] = jnp.zeros(carry_state.shape, f32)

    def gate_row(plane, i, h):
        return gall[plane * group + near(i), pl.ds(g * hfox + h, 1), :]

    def spread_columns(line_row, to, i, h):
        for c in range(tok // 128):
            piece = line_row[:, c * 128 : (c + 1) * 128]
            to[i, h, c * 128 : (c + 1) * 128, :] = jnp.broadcast_to(piece, (128, 128)).T

    def gate_columns():
        for i in range(1, n_sp):
            gate_copy(i).wait_recv()
        for h in range(hfox):
            for i in range(group):
                spread_columns(gate_row(z, i, h), gcol, i, h)

        @pl.when(z == host)
        def _():
            for h in range(hfox):
                for i in range(group):
                    spread_columns(gate_row(last, i, h), guest_col, i, h)

    inverse = FOX_DIM ** (-0.5)

    def weigh(q, column_gates, keys, key_gates, mask=None):
        scores = (
            lax.dot_general(q, keys, (((1,), (1,)), ((), ())), preferred_element_type=f32)
            * inverse
        )
        count = keys.shape[0] // 128
        scores = scores + jnp.concatenate([column_gates] * count, axis=1) - key_gates
        if mask is not None:
            scores = jnp.where(mask, scores, -jnp.inf)
        return jnp.exp(scores).astype(bf16)

    def widen(v):
        return jnp.concatenate([v, jnp.ones(v.shape, bf16)], axis=1)

    def own_attention():
        mask = row >= column
        for h in range(hfox):
            for t in range(group):
                it = near(t)
                weights, vals = [], []
                for s in range(t + 1):
                    js = near(s)
                    weights.append(
                        weigh(
                            fq[it, h],
                            gcol[it, h],
                            kv[z, js, 0, h],
                            gall[z * group + s, pl.ds(g * hfox + h, 1), :],
                            mask if s == t else None,
                        )
                    )
                    vals.append(kv[z, js, 1, h])
                w = weights[0] if t == 0 else jnp.concatenate(weights, axis=1)
                v = vals[0] if t == 0 else jnp.concatenate(vals, axis=0)
                numer[it, h] = jnp.dot(w, widen(v), preferred_element_type=f32)

    def attend(block, queries, columns, to, fresh, done=None):
        for h in range(hfox):
            keys = kv[block, :, 0, h].reshape(group * tok, FOX_DIM)
            vals = widen(kv[block, :, 1, h].reshape(group * tok, FOX_DIM))
            key_gates = jnp.concatenate([gate_row(block, i, h) for i in range(group)], axis=1)

            def query_step(j, carry):
                w = weigh(queries[j, h], columns[j, h], keys, key_gates)
                product = jnp.dot(w, vals, preferred_element_type=f32)
                if fresh:
                    to[j, h] = product
                else:
                    to[j, h] += product
                return carry

            lax.fori_loop(0, group, query_step, 0)

    def hand_back():
        for i in range(group):
            for h in range(hfox):
                num_out[i, h] = guest_numer[i, h, :, :FOX_DIM].astype(bf16)
                for c in range(tok // 128):
                    at = (i * hfox + h) * (tok // 128) + c
                    den = guest_numer[i, h, c * 128 : (c + 1) * 128, FOX_DIM:]
                    den_out[at : at + 1, :] = den.T[0:1]
            num_hop(i).start()
        den_hop().start()

    def take_back():
        den_hop().wait_recv()
        for i in range(group):
            num_hop(i).wait_recv()
            for h in range(hfox):
                numer[i, h, :, :FOX_DIM] += num_in[i, h].astype(f32)
                for c in range(tok // 128):
                    at = (i * hfox + h) * (tok // 128) + c
                    den = jnp.broadcast_to(den_in[at : at + 1, :], (128, 128)).T
                    numer[i, h, c * 128 : (c + 1) * 128, FOX_DIM:] += den

    def earlier(step):
        wanted = z - step >= 0
        if step > 1:
            wanted = wanted & (z < last)

        @pl.when(wanted)
        def _():
            block = z - step

            @pl.when(z == host)
            def _():
                attend(block, guest, guest_col, guest_numer, step == 1)
                if step == host:
                    hand_back()

            attend(block, fq, gcol, numer, False)

    def retention_out():
        for h in range(hret):
            held = carry_state[h]
            for p in range(group):
                ip = near(p)
                cross = jnp.dot(rq[ip, h], held.astype(bf16), preferred_element_type=f32)
                full = raw[ip, h] + cross * qdec[h]
                rq[ip, h] = normalize(full)
                if p < group - 1:
                    held = held * tok_decay[h] + update[ip, h]
        for order in ((3, 1), (2, 0)):
            left = jnp.concatenate(
                [
                    jnp.concatenate([rq[i, h] for i in order], axis=0)
                    for h in range(hret)
                ],
                axis=1,
            )

            def column_step(p, carry, left=left, order=order):
                right = jnp.concatenate([wret[p, near(e)] for e in range(group)], axis=1)
                product = jnp.dot(left, right, preferred_element_type=f32).astype(bf16)
                at = pl.ds(pl.multiple_of(p * wide, wide), wide)
                for e in range(4):
                    part[order[e // 2], e % 2, :, at] = product[e * rows : (e + 1) * rows]
                return carry

            lax.fori_loop(0, depth, column_step, 0)
            for i in order:
                part_copy(i).start()

    def plane_on():
        for i in (1, 2):
            plane_copy(i).wait_recv()
            plane_relay(i).start()

    def wait_guest():
        @pl.when(z == host)
        def _():
            for i in range(group):
                query_hop(i).wait_recv()

    def scatter_first():
        for i in (3, 1, 2, 0):
            part_copy(i).wait_recv()
            rsum[i] = (part[i, tp].astype(f32) + part_in[i].astype(f32)).astype(bf16)
            if i == 3:
                scatter_x(1).start()
                scatter_y(1).start()
            elif i == 1:
                scatter_x(0).start()
            elif i == 2:
                scatter_y(0).start()

    def scatter_next():
        for k in range(2):
            scatter_x(k).wait_recv()
            scatter_y(k).wait_recv()
        second_out[0] = (rsum[2, :, :half].astype(f32) + xa[1].astype(f32)).astype(bf16)
        second_out[1] = (rsum[1, :, half:].astype(f32) + yb[1].astype(f32)).astype(bf16)
        for k in range(2):
            scatter_second(k).start()

    def guest_sums():
        @pl.when(z == last)
        def _():
            take_back()

    def send_fox():
        for i in range(group):
            for h in range(hfox):
                fox_buf[i, :, h * FOX_DIM : (h + 1) * FOX_DIM] = normalize(
                    numer[i, h, :, :FOX_DIM] / numer[i, h, :, FOX_DIM:]
                )
            if i > 0:
                mixed_copy(i).start()
        mixed[:, my_cols] = fox_buf[0]

    def wait_fox():
        for i in (1, 2):
            plane_relay(i).wait_recv()
        for i in range(1, group):
            mixed_copy(i).wait_recv()

    def fox_out():
        def fox_column(p, carry):
            right = jnp.concatenate([wfox[near(e), p] for e in range(group)], axis=1)
            product = jnp.dot(mixed[...], right, preferred_element_type=f32).astype(bf16)
            at = pl.ds(pl.multiple_of(p * wide, wide), wide)
            fpart[0, :, at] = product[:rows]
            fpart[1, :, at] = product[rows:]
            return carry

        lax.fori_loop(0, depth, fox_column, 0)
        final_copy().start()

    def wait_final():
        for k in range(2):
            scatter_second(k).wait_recv()
        final_copy().wait_recv()

    def finish():
        mine = fpart[tp].astype(f32) + fgot[...].astype(f32)
        ret_low = rsum[0, :, :half].astype(f32) + xa[0].astype(f32) + second_in[0].astype(f32)
        ret_high = rsum[0, :, half:].astype(f32) + yb[0].astype(f32) + second_in[1].astype(f32)
        out[:, :half] = (mine[:, :half] + ret_low).astype(bf16)
        out[:, half:] = (mine[:, half:] + ret_high).astype(bf16)

    phase("w_loads", (wait_loads,))
    phase("project0", (project, 0))
    phase("line01", (line, 0, 1), (line, 1, 1))
    phase("take10", (take, 1, 0))
    phase("retain0", (retain, 0))
    phase("tokens1", (tokens_on, 1))
    phase("tokens2", (tokens_on, 2))
    phase("line02", (line, 0, 2), (line, 1, 2))
    phase("w_pair1", (wait_pair, 1))
    phase("project1", (project, 1))
    phase("w_rows", (wait_rows,), (begin_line, 2))
    phase("w_pair2", (wait_pair, 2))
    phase("project2", (project, 2))
    for step in range(3, depth):
        phase("line0" + str(step), (line, 0, step), (line, 1, step))
    phase("begin_plane", (begin_plane,))
    phase("retain1", (retain, 1))
    phase("line21", (line, 2, 1))
    phase("tokens3", (tokens_last,))
    phase("retain2", (retain, 2))
    phase("w_pair3", (wait_pair, 3))
    phase("project3", (project, 3))
    phase("retain3", (retain, 3))
    phase("gates", (gate_columns,))
    phase("line22", (line, 2, 2))
    phase("pass_state", (pass_state,))
    phase("take11", (take, 1, 1))
    phase("take12", (take, 1, 2))
    phase("take13", (take, 1, 3))
    phase("own_attention", (own_attention,))
    phase("plane_on", (plane_on,))
    for step in range(3, depth):
        phase("line2" + str(step), (line, 2, step))
    phase("retention_out", (retention_out,))
    phase("w_guest", (wait_guest,))
    phase("earlier1", (earlier, 1))
    phase("scatter1", (scatter_first,))
    for step in range(2, depth):
        for i in range(group):
            phase("take" + str(step) + str(i), (take, step, i))
        phase("earlier" + str(step), (earlier, step))
    phase("guest_sums", (guest_sums,))
    phase("send_fox", (send_fox,))
    phase("scatter2", (scatter_next,))
    phase("w_fox", (wait_fox,))
    phase("fox_out", (fox_out,))
    phase("w_final", (wait_final,))
    phase("finish", (finish,))

    for i in (1, 2):
        token_copy(i).wait_send()
        token_relay(i).wait_send()
        plane_copy(i).wait_send()
        plane_relay(i).wait_send()
    for i in range(group):
        pair_copy(i).wait_send()
        part_copy(i).wait_send()
    for i in range(1, group):
        rows_copy(i).wait_send()
        mixed_copy(i).wait_send()
    for i in range(1, n_sp):
        gate_copy(i).wait_send()
    for kind in range(3):
        settle_line(kind)
    for k in range(2):
        scatter_x(k).wait_send()
        scatter_y(k).wait_send()
        scatter_second(k).wait_send()
    final_copy().wait_send()

    @pl.when(z < last)
    def _():
        state_hop().wait_send()
        for i in range(group):
            kv_hop(z, i).wait_send()

    for step in range(1, depth):

        @pl.when((z - step >= 0) & (z < host))
        def _():
            for i in range(group):
                kv_hop(z - step, i).wait_send()

    @pl.when(z == last)
    def _():
        for i in range(group):
            query_hop(i).wait_send()

    @pl.when(z == host)
    def _():
        for i in range(group):
            num_hop(i).wait_send()
        den_hop().wait_send()


def fused(tokens, gain, gates, inverse, w_ret, w_fox, w_in, hret, hfox, n_sp):
    rows, width = tokens.shape
    group = 4
    tok = 2 * rows
    depth = n_sp // group
    out_cols = n_sp * w_ret.shape[1]
    half = out_cols // 2
    ret_rows = hret * RET_DIM
    fox_rows = group * hfox * FOX_DIM
    vmem = pl.BlockSpec(memory_space=pltpu.VMEM)
    hbm = pl.BlockSpec(memory_space=pl.ANY)
    dma = pltpu.SemaphoreType.DMA
    f32 = jnp.float32
    bf16 = jnp.bfloat16
    square = (hret, RET_DIM, RET_DIM)
    heads = (group, hfox, tok, FOX_DIM)
    dens = group * hfox * (tok // 128)
    total = float(tok * n_sp)

    def body(*refs):
        fused_kernel(n_sp, total, *refs[:6], refs[6:12], *refs[12:])

    V = pltpu.VMEM
    return pl.pallas_call(
        body,
        out_shape=jax.ShapeDtypeStruct((rows, out_cols), bf16),
        in_specs=[vmem] * 4 + [hbm] * 8,
        out_specs=vmem,
        scratch_shapes=[
            V((group, 2, rows, width), bf16),
            V((3, width, ret_rows), bf16),
            V((3, width, hfox * FOX_DIM), bf16),
            V(w_ret.shape, bf16),
            V((depth, group, ret_rows, w_ret.shape[1]), bf16),
            V((group, depth, fox_rows, w_ret.shape[1]), bf16),
            V((n_sp,) + gates.shape, f32),
            V((tok, RET_DIM // 2), f32),
            V((tok, RET_DIM // 2), f32),
            V((hret, tok, tok), f32),
            V((hret, tok, RET_DIM), f32),
            V((hret, tok, RET_DIM), f32),
            V((group, hret, tok, RET_DIM), bf16),
            V((group, hret, tok, RET_DIM), bf16),
            V((group, hret, tok, RET_DIM), bf16),
            V(heads, bf16),
            V(heads, bf16),
            V((depth, group, 2, hfox, tok, FOX_DIM), bf16),
            V((group, hret, tok, RET_DIM), f32),
            V((group,) + square, f32),
            V(square, bf16),
            V(square, bf16),
            V(square, f32),
            V((group, hfox, tok, 128), f32),
            V((group, hfox, tok, 128), f32),
            V((group, hfox, tok, 2 * FOX_DIM), f32),
            V((group, hfox, tok, 2 * FOX_DIM), f32),
            V(heads, bf16),
            V(heads, bf16),
            V((dens, 128), f32),
            V((dens, 128), f32),
            V((group, 2, rows, out_cols), bf16),
            V((group, rows, out_cols), bf16),
            V((group, rows, out_cols), bf16),
            V((2, rows, half), bf16),
            V((2, rows, half), bf16),
            V((2, rows, half), bf16),
            V((2, rows, half), bf16),
            V((group, tok, hfox * FOX_DIM), bf16),
            V((tok, fox_rows), bf16),
            V((2, rows, out_cols), bf16),
            V((rows, out_cols), bf16),
            dma((9,)),
            dma((3,)),
            dma((3,)),
            dma((3,)),
            dma((3,)),
            dma((group,)),
            dma((group,)),
            dma((n_sp,)),
            dma((n_sp,)),
            dma((group,)),
            dma((group,)),
            dma((3, depth)),
            dma((3, depth)),
            dma((3, depth)),
            dma((3, depth)),
            dma((5,)),
            dma((5,)),
            dma((depth, group)),
            dma((depth, group)),
            dma((group,)),
            dma((group,)),
            dma((1,)),
            dma((1,)),
            dma((group + 1,)),
            dma((group + 1,)),
            dma((group,)),
            dma((group,)),
            dma((6,)),
            dma((6,)),
            dma((group,)),
            dma((group,)),
        ],
        compiler_params=pltpu.CompilerParams(
            collective_id=2, has_side_effects=True, vmem_limit_bytes=VMEM_LIMIT
        ),
        name="fused",
    )(tokens, gain, gates, inverse, w_ret, w_fox, *w_in)


def decay_rates(head_ids, total):
    heads_float = head_ids.astype(jnp.float32)
    middle = RET_HEADS // 2
    fast_rate = 1.0 / (32.0 + 16.0 * heads_float)
    slow_rate = jnp.exp2(-(heads_float - middle)) / total
    return jnp.where(head_ids < middle, fast_rate, slow_rate)


def per_device(
    n_sp,
    n_tp,
    tokens,
    gain,
    w_ret_q,
    w_ret_k,
    w_ret_v,
    w_fox_q,
    w_fox_k,
    w_fox_v,
    fox_gates,
    w_out_ret,
    w_out_fox,
):
    f32 = jnp.float32
    rows, width = tokens.shape
    ret_heads = w_ret_q.shape[1] // RET_DIM
    fox_heads = w_fox_q.shape[1] // FOX_DIM
    group = math.gcd(math.gcd(ret_heads, fox_heads), n_sp)
    depth = n_sp // group
    hret = ret_heads // group
    hfox = fox_heads // group
    run = rows * n_tp * group
    half = RET_DIM // 2
    inverse = 10000.0 ** (-jnp.arange(half, dtype=f32) / half)
    if group == 4 and n_tp == 2 and depth > 2:
        return fused(
            tokens,
            gain.reshape(1, width),
            fox_gates.T,
            inverse.reshape(1, half),
            w_out_ret,
            w_out_fox,
            (w_ret_q, w_ret_k, w_ret_v, w_fox_q, w_fox_k, w_fox_v),
            hret,
            hfox,
            n_sp,
        )
    sp = lax.axis_index("sp")
    g = lax.rem(sp, group)
    z = sp // group

    positions = z * run + jnp.arange(run, dtype=jnp.int32)
    angles = positions.astype(f32)[:, None] * inverse[None, :]
    rq, rk, rv, fq, fkv, gall, wz = gather(
        tokens,
        gain.reshape(1, width),
        fox_gates.T,
        w_out_ret,
        w_out_fox,
        jnp.cos(angles),
        jnp.sin(angles),
        (w_ret_q, w_ret_k, w_ret_v, w_fox_q, w_fox_k, w_fox_v),
        hret,
        hfox,
        n_sp,
        n_tp,
        group,
    )

    head_ids = (
        lax.axis_index("tp") * ret_heads + g * hret + jnp.arange(hret, dtype=jnp.int32)
    )
    rates = decay_rates(head_ids, float(run * depth))
    offsets = jnp.arange(BLOCK, dtype=f32)
    spread = offsets[:, None] - offsets[None, :]
    causal = spread >= 0
    within = jnp.where(
        causal[None], jnp.exp(-rates[:, None, None] * jnp.where(causal, spread, 0.0)[None]), 0.0
    )
    steps = jnp.arange(run, dtype=f32)
    qdec = jnp.exp(-rates[:, None] * (steps[None, :] + 1.0))[:, :, None]
    kdec = jnp.exp(-rates[:, None] * (BLOCK - 1.0 - offsets[None, :]))[:, :, None]
    lengths = jnp.array([BLOCK, run], f32)
    bdec = jnp.broadcast_to(
        jnp.exp(-rates[:, None] * lengths[None, :])[:, :, None], (hret, 2, RET_DIM)
    )

    own_gates = lax.dynamic_slice_in_dim(gall, g * hfox, hfox, 1)
    line = own_gates.transpose(1, 0, 2).reshape(hfox, depth, 1, run)
    gq = lax.dynamic_index_in_dim(line, z, 1, False).reshape(hfox, run, 1)
    return mixer(
        rq, rk, rv, fq, fkv, gq, line, within, qdec, kdec, bdec, wz, rows, n_sp, n_tp, group
    )


def solution(mesh):
    in_specs = (
        P(("sp", "tp"), None),
        P(),
        P(None, "tp"),
        P(None, "tp"),
        P(None, "tp"),
        P(None, "tp"),
        P(None, "tp"),
        P(None, "tp"),
        P("sp", "tp"),
        P("tp", "sp"),
        P("tp", "sp"),
    )
    out_specs = P(("sp", "tp"), None)
    return jax.shard_map(
        functools.partial(per_device, mesh.shape["sp"], mesh.shape["tp"]),
        mesh=mesh,
        in_specs=in_specs,
        out_specs=out_specs,
        check_vma=False,
    )
```

```python
import functools
import math

import jax
import jax.numpy as jnp
from jax import lax
from jax.experimental import pallas as pl
from jax.experimental.pallas import tpu as pltpu
from jax.sharding import PartitionSpec as P

RET_HEADS = 8
RET_DIM = 256
FOX_DIM = 128
BLOCK = 128
MESH = pl.DeviceIdType.MESH
VMEM_LIMIT = 60 * 1024 * 1024

eps = 1e-06


def remote(src, dst, send, recv, sp, tp):
    return pltpu.make_async_remote_copy(
        src_ref=src,
        dst_ref=dst,
        send_sem=send,
        recv_sem=recv,
        device_id=(sp, tp),
        device_id_type=MESH,
    )


def gather_kernel(
    n_sp,
    n_tp,
    group,
    tok_ref,
    gain_ref,
    gates_ref,
    wr_ref,
    wf_ref,
    cos_ref,
    sin_ref,
    w_in,
    rq,
    rk,
    rv,
    fq,
    fkv,
    gall,
    wz,
    own,
    xall,
    w_ret,
    w_fox,
    local_sem,
    in_sem,
    tsend,
    trecv,
    dsend,
    drecv,
    psend,
    precv,
    gsend,
    grecv,
    usend,
    urecv,
    nsend,
    nrecv,
):
    sp = lax.axis_index("sp")
    tp = lax.axis_index("tp")
    g = lax.rem(sp, group)
    z = sp // group
    depth = n_sp // group
    rows = tok_ref.shape[0]
    half = rows // 2
    krows = wr_ref.shape[0]

    barrier = pltpu.get_barrier_semaphore()
    for i in range(1, n_sp):
        pl.semaphore_signal(
            barrier, inc=1, device_id=(lax.rem(sp + i, n_sp), tp), device_id_type=MESH
        )
    for i in range(1, n_tp):
        pl.semaphore_signal(
            barrier, inc=1, device_id=(sp, lax.rem(tp + i, n_tp)), device_id_type=MESH
        )

    loads = []
    for i in range(6):
        cut = w_ret if i < 3 else w_fox
        size = cut.shape[2]
        columns = pl.ds(pl.multiple_of(g * size, 128), size)
        loads.append(
            pltpu.make_async_copy(w_in[i].at[:, columns], cut.at[i % 3], in_sem.at[i])
        )

    values = tok_ref[...].astype(jnp.float32)
    scale = lax.rsqrt(jnp.mean(values * values, axis=1, keepdims=True) + eps)
    own[...] = (values * scale * gain_ref[...]).astype(jnp.bfloat16)
    copies = [
        pltpu.make_async_copy(wr_ref, wz.at[z, pl.ds(0, krows)], local_sem.at[0]),
        pltpu.make_async_copy(
            wf_ref, wz.at[z, pl.ds(krows, wf_ref.shape[0])], local_sem.at[1]
        ),
        pltpu.make_async_copy(gates_ref, gall.at[sp], local_sem.at[2]),
    ]
    for copy in copies + loads:
        copy.start()
    pl.semaphore_wait(barrier, n_sp + n_tp - 2)

    def slot(which, core):
        return xall.at[which * n_tp + core]

    mine = pltpu.make_async_copy(own, slot(g, tp), local_sem.at[3])
    mine.start()

    def peer(other):
        return z * group + other

    hyper = group == 4
    direct = []
    for i in range(1, group):
        if hyper and i == 3:
            continue
        other = lax.bitwise_xor(g, i) if hyper else lax.rem(g + i, group)
        direct.append(
            remote(own, slot(g, tp), tsend.at[i], trecv.at[i], peer(other), tp)
        )
    for copy in direct:
        copy.start()
    pair = []
    for i in range(1, n_tp):
        copy = remote(
            own, slot(g, tp), psend.at[0, i], precv.at[0, i], sp, lax.rem(tp + i, n_tp)
        )
        copy.start()
        pair.append(copy)
    gate_copies = []
    for i in range(1, n_sp):
        copy = remote(
            gates_ref, gall.at[sp], gsend.at[i], grecv.at[i], lax.rem(sp + i, n_sp), tp
        )
        copy.start()
        gate_copies.append(copy)

    copies[0].wait()
    copies[1].wait()

    def up(block):
        return remote(
            wz.at[block],
            wz.at[block],
            usend.at[block],
            urecv.at[block],
            lax.rem(sp + group, n_sp),
            tp,
        )

    def down(block):
        return remote(
            wz.at[block],
            wz.at[block],
            nsend.at[block],
            nrecv.at[block],
            lax.rem(sp + n_sp - group, n_sp),
            tp,
        )

    @pl.when(z < depth - 1)
    def _():
        up(z).start()

    @pl.when(z > 0)
    def _():
        down(z).start()

    ready = {0: pair[:]}

    def forward(which, row):
        ready[row] = []
        for i in range(1, n_tp):
            copy = remote(
                slot(which, tp),
                slot(which, tp),
                psend.at[row, i],
                precv.at[row, i],
                sp,
                lax.rem(tp + i, n_tp),
            )
            copy.start()
            pair.append(copy)
            ready[row].append(copy)

    count = n_tp * rows
    half_head = RET_DIM // 2

    def project(which, row):
        for copy in ready[row]:
            copy.wait_recv()
        x = xall[pl.ds(which * n_tp, n_tp)].reshape(count, xall.shape[2])
        span = pl.ds(pl.multiple_of(which * count, count), count)
        for i in range(6):
            cut = w_ret if i < 3 else w_fox
            y = jnp.dot(x, cut[i % 3], preferred_element_type=jnp.float32)
            y = y.astype(jnp.bfloat16)
            if i < 2:
                cosine = cos_ref[span, :]
                sine = sin_ref[span, :]
            for h in range(rq.shape[0] if i < 3 else fq.shape[0]):
                if i < 2:
                    lo = h * RET_DIM
                    a = y[:, lo : lo + half_head].astype(jnp.float32)
                    b = y[:, lo + half_head : lo + RET_DIM].astype(jnp.float32)
                    to = rq if i == 0 else rk
                    by = 1.0 if i == 0 else RET_DIM ** (-0.5)
                    first = (a * cosine - b * sine) * by
                    second = (a * sine + b * cosine) * by
                    to[h, span, :half_head] = first.astype(jnp.bfloat16)
                    to[h, span, half_head:] = second.astype(jnp.bfloat16)
                elif i == 2:
                    rv[h, span, :] = y[:, h * RET_DIM : (h + 1) * RET_DIM]
                elif i == 3:
                    fq[h, span, :] = y[:, h * FOX_DIM : (h + 1) * FOX_DIM]
                else:
                    fkv[i - 4, h, span, :] = y[:, h * FOX_DIM : (h + 1) * FOX_DIM]

    mine.wait()
    for copy in loads:
        copy.wait()
    if not hyper:
        project(g, 0)

    if hyper:
        relays = []
        for i in (1, 2):
            direct[i - 1].wait_recv()
            source = lax.bitwise_xor(g, i)
            target = lax.bitwise_xor(g, 3 - i)
            part = pl.ds((i - 1) * half, half)
            copy = remote(
                slot(source, tp).at[part],
                slot(source, tp).at[part],
                dsend.at[i],
                drecv.at[i],
                peer(target),
                tp,
            )
            copy.start()
            relays.append(copy)
            forward(source, i)
        project(g, 0)
    else:
        for i in range(1, group):
            direct[i - 1].wait_recv()
            forward(lax.rem(g + group - i, group), i)
            project(lax.rem(g + group - i, group), i)

    def line(step, carry):
        below = z - step
        above = z + step

        @pl.when(below >= 0)
        def _():
            up(below).wait_recv()

            @pl.when(z < depth - 1)
            def _():
                up(below).start()

        @pl.when(above <= depth - 1)
        def _():
            down(above).wait_recv()

            @pl.when(z > 0)
            def _():
                down(above).start()

        return carry

    split = depth // 2 if hyper else depth
    lax.fori_loop(1, split, line, 0)
    if hyper:
        project(lax.bitwise_xor(g, 1), 1)
        for copy in relays:
            copy.wait_recv()
        forward(lax.bitwise_xor(g, 3), 3)
    lax.fori_loop(split, depth - 1, line, 0)
    if hyper:
        project(lax.bitwise_xor(g, 2), 2)
        project(lax.bitwise_xor(g, 3), 3)
    lax.fori_loop(max(split, depth - 1), depth, line, 0)

    def settle(step, carry):
        @pl.when((z < depth - 1) & (step <= z))
        def _():
            up(step).wait_send()

        @pl.when((z > 0) & (step >= z))
        def _():
            down(step).wait_send()

        return carry

    lax.fori_loop(0, depth, settle, 0)
    for copy in direct:
        copy.wait_send()
    if hyper:
        for copy in relays:
            copy.wait_send()
    for copy in gate_copies:
        copy.wait()
    for copy in pair:
        copy.wait_send()
    copies[2].wait()


def gather(
    tokens, gain, gates, w_ret, w_fox, cosine, sine, w_in, hret, hfox, n_sp, n_tp, group
):
    rows, width = tokens.shape
    depth = n_sp // group
    out_rows = w_ret.shape[0] + w_fox.shape[0]
    vmem = pl.BlockSpec(memory_space=pltpu.VMEM)
    hbm = pl.BlockSpec(memory_space=pl.ANY)
    dma = pltpu.SemaphoreType.DMA
    run = rows * n_tp * group
    bf16 = jnp.bfloat16

    def body(*refs):
        gather_kernel(n_sp, n_tp, group, *refs[:7], refs[7:13], *refs[13:])

    return pl.pallas_call(
        body,
        out_shape=(
            jax.ShapeDtypeStruct((hret, run, RET_DIM), bf16),
            jax.ShapeDtypeStruct((hret, run, RET_DIM), bf16),
            jax.ShapeDtypeStruct((hret, run, RET_DIM), bf16),
            jax.ShapeDtypeStruct((hfox, run, FOX_DIM), bf16),
            jax.ShapeDtypeStruct((2, hfox, run, FOX_DIM), bf16),
            jax.ShapeDtypeStruct((n_sp,) + gates.shape, jnp.float32),
            jax.ShapeDtypeStruct((depth, out_rows, w_ret.shape[1]), jnp.bfloat16),
        ),
        in_specs=[vmem, vmem, vmem, hbm, hbm, vmem, vmem] + [hbm] * 6,
        out_specs=(vmem,) * 7,
        scratch_shapes=[
            pltpu.VMEM((rows, width), bf16),
            pltpu.VMEM((group * n_tp, rows, width), bf16),
            pltpu.VMEM((3, width, hret * RET_DIM), bf16),
            pltpu.VMEM((3, width, hfox * FOX_DIM), bf16),
            dma((4,)),
            dma((6,)),
            dma((max(group, 2),)),
            dma((max(group, 2),)),
            dma((3,)),
            dma((3,)),
            dma((group, n_tp)),
            dma((group, n_tp)),
            dma((n_sp,)),
            dma((n_sp,)),
            dma((depth,)),
            dma((depth,)),
            dma((depth,)),
            dma((depth,)),
        ],
        compiler_params=pltpu.CompilerParams(
            collective_id=0, has_side_effects=True, vmem_limit_bytes=VMEM_LIMIT
        ),
        name="gather",
    )(tokens, gain, gates, w_ret, w_fox, cosine, sine, *w_in)


def normalize(values):
    return (
        values * lax.rsqrt(jnp.mean(values * values, axis=1, keepdims=True) + eps)
    ).astype(jnp.bfloat16)


def mixer_kernel(
    n_sp,
    n_tp,
    group,
    rq,
    rk,
    rv,
    fq,
    fkv,
    gq,
    gk,
    within,
    qdec,
    kdec,
    bdec,
    wz,
    out,
    w_all,
    slots,
    raw,
    state,
    state_in,
    state_out,
    numer,
    denom,
    ret_buf,
    fox_buf,
    mixed,
    part,
    got,
    local_sem,
    ksend,
    krecv,
    ssend,
    srecv,
    wsend,
    wrecv,
    dsend,
    drecv,
    asend,
    arecv,
    osend,
    orecv,
):
    sp = lax.axis_index("sp")
    tp = lax.axis_index("tp")
    g = lax.rem(sp, group)
    z = sp // group
    depth = n_sp // group
    hret = rq.shape[0]
    hfox = fq.shape[0]
    run = rq.shape[1]
    tok = run // group
    rows = out.shape[0]
    after = lax.rem(sp + group, n_sp)
    before = lax.rem(sp + n_sp - group, n_sp)
    f32 = jnp.float32

    def peer(other):
        return z * group + other

    barrier = pltpu.get_barrier_semaphore()
    for i in range(1, group):
        pl.semaphore_signal(
            barrier, inc=1, device_id=(peer(lax.rem(g + i, group)), tp), device_id_type=MESH
        )
    for i in range(1, n_tp):
        pl.semaphore_signal(
            barrier, inc=1, device_id=(sp, lax.rem(tp + i, n_tp)), device_id_type=MESH
        )
    if depth > 1:

        @pl.when(z < depth - 1)
        def _():
            pl.semaphore_signal(barrier, inc=1, device_id=(after, tp), device_id_type=MESH)

        @pl.when(z > 0)
        def _():
            pl.semaphore_signal(barrier, inc=1, device_id=(before, tp), device_id_type=MESH)

    ends = (z + depth - 1) // depth + (2 * depth - 2 - z) // depth
    pl.semaphore_wait(barrier, group + n_tp - 2 + ends)

    def first_hop():
        return remote(fkv, slots.at[z], ksend.at[z], krecv.at[z], after, tp)

    def hop(block):
        return remote(
            slots.at[block], slots.at[block], ksend.at[block], krecv.at[block], after, tp
        )

    if depth > 1:

        @pl.when(z < depth - 1)
        def _():
            first_hop().start()

    hyper = group == 4
    mine = pltpu.make_async_copy(wz, w_all.at[g], local_sem.at[0])
    mine.start()
    direct = []
    for i in range(1, group):
        if hyper and i == 3:
            continue
        other = lax.bitwise_xor(g, i) if hyper else lax.rem(g + i, group)
        direct.append(
            remote(wz, w_all.at[g], wsend.at[i], wrecv.at[i], peer(other), tp)
        )
    for copy in direct:
        copy.start()

    def relay(i):
        source = lax.bitwise_xor(g, i)
        target = lax.bitwise_xor(g, 3 - i)
        span = pl.ds((i - 1) * (depth // 2), depth // 2)
        return remote(
            w_all.at[source, span],
            w_all.at[source, span],
            dsend.at[i],
            drecv.at[i],
            peer(target),
            tp,
        )

    for h in range(hret):
        state[h] = jnp.zeros(state.shape[1:], f32)

        def ret_step(b, carry):
            span = pl.ds(pl.multiple_of(b * BLOCK, BLOCK), BLOCK)
            q = rq[h, span, :]
            k = rk[h, span, :]
            v = rv[h, span, :]
            scores = (
                lax.dot_general(q, k, (((1,), (1,)), ((), ())), preferred_element_type=f32)
                * within[h]
            )
            inner = jnp.dot(scores.astype(jnp.bfloat16), v, preferred_element_type=f32)
            held = state[h]
            cross = jnp.dot(q, held.astype(jnp.bfloat16), preferred_element_type=f32)
            raw[h, span, :] = inner + cross * qdec[h, pl.ds(0, BLOCK), :]
            scaled = (k.astype(f32) * kdec[h]).astype(jnp.bfloat16)
            update = lax.dot_general(
                scaled, v, (((0,), (0,)), ((), ())), preferred_element_type=f32
            )
            state[h] = held * bdec[h, 0:1, :] + update
            return carry

        lax.fori_loop(0, run // BLOCK, ret_step, 0)

    def state_hop():
        return remote(state_out, state_in, ssend.at[0], srecv.at[0], after, tp)

    if depth > 1:

        @pl.when(z == 0)
        def _():
            state_out[...] = state[...]
            state_hop().start()

    tile = math.gcd(run, 256)
    inverse = FOX_DIM ** (-0.5)

    def attend(h, t, keys, values, key_gates, diagonal, fresh):
        span = pl.ds(pl.multiple_of(t * tile, tile), tile)
        scores = (
            lax.dot_general(
                fq[h, span, :], keys, (((1,), (1,)), ((), ())), preferred_element_type=f32
            )
            * inverse
        )
        scores = scores + gq[h, span, :] - key_gates
        if diagonal:
            row = lax.broadcasted_iota(jnp.int32, scores.shape, 0)
            col = lax.broadcasted_iota(jnp.int32, scores.shape, 1)
            scores = jnp.where(col <= row, scores, -jnp.inf)
        weights = jnp.exp(scores)
        total = jnp.sum(weights, axis=1, keepdims=True)
        product = jnp.dot(weights.astype(jnp.bfloat16), values, preferred_element_type=f32)
        if fresh:
            numer[h, span, :] = product
            denom[h, span, :] = total
        else:
            numer[h, span, :] += product
            denom[h, span, :] += total

    for h in range(hfox):
        for t in range(run // tile):
            for s in range(t, -1, -1):
                span = pl.ds(s * tile, tile)
                attend(
                    h,
                    t,
                    fkv[0, h, span, :],
                    fkv[1, h, span, :],
                    gk[h, z, :, span],
                    s == t,
                    s == t,
                )

    def carried():
        state_hop().wait_recv()

        @pl.when(z < depth - 1)
        def _():
            for h in range(hret):
                state_out[h] = state_in[h] * bdec[h, 1:2, :] + state[h]
            state_hop().start()

        for h in range(hret):
            held = state_in[h].astype(jnp.bfloat16)

            def cross_step(b, carry):
                span = pl.ds(pl.multiple_of(b * tile, tile), tile)
                cross = jnp.dot(rq[h, span, :], held, preferred_element_type=f32)
                raw[h, span, :] += cross * qdec[h, span, :]
                return carry

            lax.fori_loop(0, run // tile, cross_step, 0)

    def earlier(step, carry):
        @pl.when(step <= z)
        def _():
            block = z - step
            hop(block).wait_recv()

            @pl.when(z < depth - 1)
            def _():
                hop(block).start()

            for h in range(hfox):

                def query_step(t, c):
                    attend(
                        h,
                        t,
                        slots[block, 0, h],
                        slots[block, 1, h],
                        gk[h, block],
                        False,
                        False,
                    )
                    return c

                lax.fori_loop(0, run // tile, query_step, 0)

        return carry

    if depth > 1:
        lax.fori_loop(1, 2, earlier, 0)

        @pl.when(z > 0)
        def _():
            carried()

        if hyper:
            direct[0].wait_recv()
            relay(1).start()
            direct[1].wait_recv()
            relay(2).start()
        lax.fori_loop(2, depth, earlier, 0)
    elif hyper:
        direct[0].wait_recv()
        relay(1).start()
        direct[1].wait_recv()
        relay(2).start()

    rw = hret * RET_DIM
    fw = hfox * FOX_DIM
    for t in range(group):
        span = pl.ds(t * tok, tok)
        for h in range(hret):
            ret_buf[t, :, h * RET_DIM : (h + 1) * RET_DIM] = normalize(raw[h, span, :])
        for h in range(hfox):
            fox_buf[t, :, h * FOX_DIM : (h + 1) * FOX_DIM] = normalize(
                numer[h, span, :] / denom[h, span, :]
            )
    ret_cols = pl.ds(pl.multiple_of(g * rw, 128), rw)
    fox_cols = pl.ds(pl.multiple_of(group * rw + g * fw, 128), fw)
    exchange = []
    for i in range(1, group):
        other = lax.rem(g + i, group)
        for kind, (buf, cols) in enumerate(((ret_buf, ret_cols), (fox_buf, fox_cols))):
            copy = remote(
                buf.at[other],
                mixed.at[:, cols],
                asend.at[kind, i],
                arecv.at[kind, i],
                peer(other),
                tp,
            )
            copy.start()
            exchange.append(copy)
    mixed[:, ret_cols] = ret_buf[g]
    mixed[:, fox_cols] = fox_buf[g]
    for copy in exchange:
        copy.wait_recv()
    mine.wait()
    if hyper:
        relay(1).wait_recv()
        relay(2).wait_recv()
    else:
        for copy in direct:
            copy.wait_recv()

    cols = w_all.shape[3]
    pack = max(1, 128 // cols)
    wide = pack * cols
    for t in range(n_tp):
        left = mixed[t * rows : (t + 1) * rows, :]

        def column(p, carry, left=left, t=t):
            blocks = [
                w_all[lax.rem(p * pack + i, group), (p * pack + i) // group]
                for i in range(pack)
            ]
            right = blocks[0] if pack == 1 else jnp.concatenate(blocks, axis=1)
            product = jnp.dot(left, right, preferred_element_type=f32)
            at = pl.ds(pl.multiple_of(p * wide, wide), wide)
            part[t, :, at] = product.astype(jnp.bfloat16)
            return carry

        lax.fori_loop(0, n_sp // pack, column, 0)
    final = []
    for i in range(1, n_tp):
        other = lax.rem(tp + i, n_tp)
        copy = remote(part.at[other], got.at[i], osend.at[i], orecv.at[i], sp, other)
        copy.start()
        final.append(copy)
    total = part[tp].astype(f32)
    for i in range(1, n_tp):
        final[i - 1].wait_recv()
        total = total + got[i].astype(f32)
    out[...] = total.astype(jnp.bfloat16)

    for copy in final + exchange + direct:
        copy.wait_send()
    if hyper:
        relay(1).wait_send()
        relay(2).wait_send()
    if depth > 1:

        @pl.when(z < depth - 1)
        def _():
            first_hop().wait_send()
            state_hop().wait_send()

            def settle(block, carry):
                @pl.when(block < z)
                def _():
                    hop(block).wait_send()

                return carry

            lax.fori_loop(0, depth, settle, 0)


def mixer(rq, rk, rv, fq, fkv, gq, gk, within, qdec, kdec, bdec, wz, rows, n_sp, n_tp, group):
    depth = n_sp // group
    hret, run, _ = rq.shape
    hfox = fq.shape[0]
    tok = run // group
    out_rows, cols = wz.shape[1:]
    width = n_sp * cols
    vmem = pl.BlockSpec(memory_space=pltpu.VMEM)
    dma = pltpu.SemaphoreType.DMA
    f32 = jnp.float32
    bf16 = jnp.bfloat16
    square = (hret, RET_DIM, RET_DIM)
    return pl.pallas_call(
        functools.partial(mixer_kernel, n_sp, n_tp, group),
        out_shape=jax.ShapeDtypeStruct((rows, width), bf16),
        in_specs=[vmem] * 11 + [pl.BlockSpec(memory_space=pl.ANY)],
        out_specs=vmem,
        scratch_shapes=[
            pltpu.VMEM((group,) + wz.shape, bf16),
            pltpu.VMEM((depth,) + fkv.shape, bf16),
            pltpu.VMEM((hret, run, RET_DIM), f32),
            pltpu.VMEM(square, f32),
            pltpu.VMEM(square, f32),
            pltpu.VMEM(square, f32),
            pltpu.VMEM((hfox, run, FOX_DIM), f32),
            pltpu.VMEM((hfox, run, 1), f32),
            pltpu.VMEM((group, tok, hret * RET_DIM), bf16),
            pltpu.VMEM((group, tok, hfox * FOX_DIM), bf16),
            pltpu.VMEM((tok, out_rows), bf16),
            pltpu.VMEM((n_tp, rows, width), bf16),
            pltpu.VMEM((n_tp, rows, width), bf16),
            dma((1,)),
            dma((depth,)),
            dma((depth,)),
            dma((1,)),
            dma((1,)),
            dma((max(group, 2),)),
            dma((max(group, 2),)),
            dma((3,)),
            dma((3,)),
            dma((2, group)),
            dma((2, group)),
            dma((n_tp,)),
            dma((n_tp,)),
        ],
        compiler_params=pltpu.CompilerParams(
            collective_id=1, has_side_effects=True, vmem_limit_bytes=VMEM_LIMIT
        ),
        name="mixer",
    )(rq, rk, rv, fq, fkv, gq, gk, within, qdec, kdec, bdec, wz)


def fused_kernel(
    n_sp,
    total,
    tok_ref,
    gain_ref,
    gates_ref,
    inv_ref,
    wr_ref,
    wf_ref,
    w_in,
    out,
    xall,
    w_ret,
    w_fox,
    wrs,
    wret,
    wfox,
    gall,
    ctab,
    stab,
    within,
    qdec,
    kdec,
    rq,
    rk,
    rv,
    fq,
    guest,
    kv,
    raw,
    update,
    state_in,
    state_out,
    carry_state,
    gcol,
    guest_col,
    numer,
    guest_numer,
    num_out,
    num_in,
    den_out,
    den_in,
    part,
    part_in,
    rsum,
    xa,
    yb,
    second_out,
    second_in,
    fox_buf,
    mixed,
    fpart,
    fgot,
    local_sem,
    tsend,
    trecv,
    dsend,
    drecv,
    psend,
    precv,
    gsend,
    grecv,
    asend,
    arecv,
    usend,
    urecv,
    nsend,
    nrecv,
    fsend,
    frecv,
    ksend,
    krecv,
    qsend,
    qrecv,
    ssend,
    srecv,
    osend,
    orecv,
    psum_send,
    psum_recv,
    rsend,
    rrecv,
    esend,
    erecv,
):
    f32 = jnp.float32
    bf16 = jnp.bfloat16
    group = 4
    sp = lax.axis_index("sp")
    tp = lax.axis_index("tp")
    other_core = 1 - tp
    g = lax.rem(sp, group)
    z = sp // group
    depth = n_sp // group
    last = depth - 1
    host = 1
    rows = tok_ref.shape[0]
    tok = 2 * rows
    hret = rq.shape[1]
    hfox = fq.shape[1]
    ret_rows = hret * RET_DIM
    after = lax.rem(sp + group, n_sp)
    before = lax.rem(sp + n_sp - group, n_sp)

    def near(i):
        return lax.bitwise_xor(g, i)

    def peer(i):
        return z * group + near(i)

    barrier = pltpu.get_barrier_semaphore()
    for i in range(1, n_sp):
        pl.semaphore_signal(
            barrier, inc=1, device_id=(lax.rem(sp + i, n_sp), tp), device_id_type=MESH
        )
    pl.semaphore_signal(barrier, inc=1, device_id=(sp, other_core), device_id_type=MESH)

    locals_ = [
        pltpu.make_async_copy(wr_ref, wrs, local_sem.at[0]),
        pltpu.make_async_copy(
            wr_ref.at[pl.ds(pl.multiple_of(g * ret_rows, ret_rows), ret_rows)],
            wret.at[z, 0],
            local_sem.at[1],
        ),
        pltpu.make_async_copy(wf_ref, wfox.at[0, z], local_sem.at[2]),
    ]
    loads = []
    for i in range(6):
        cut = w_ret if i < 3 else w_fox
        size = cut.shape[2]
        columns = pl.ds(pl.multiple_of(g * size, 128), size)
        loads.append(
            pltpu.make_async_copy(
                w_in[i].at[:, columns], cut.at[i % 3], local_sem.at[3 + i]
            )
        )
    for copy in locals_ + loads:
        copy.start()

    values = tok_ref[...].astype(f32)
    scale = lax.rsqrt(jnp.mean(values * values, axis=1, keepdims=True) + eps)
    xall[0, tp] = (values * scale * gain_ref[...]).astype(bf16)
    gall[sp] = gates_ref[...]
    with jax.named_scope("barrier"):
        pl.semaphore_wait(barrier, n_sp)

    def token_copy(i):
        return remote(xall.at[0, tp], xall.at[i, tp], tsend.at[i], trecv.at[i], peer(i), tp)

    def token_relay(i):
        span = pl.ds((i - 1) * (rows // 2), rows // 2)
        return remote(
            xall.at[i, tp, span],
            xall.at[3, tp, span],
            dsend.at[i],
            drecv.at[i],
            peer(3 - i),
            tp,
        )

    def pair_copy(i):
        return remote(
            xall.at[i, tp], xall.at[i, tp], psend.at[i], precv.at[i], sp, other_core
        )

    def gate_copy(i):
        return remote(
            gates_ref, gall.at[sp], gsend.at[i], grecv.at[i], lax.rem(sp + i, n_sp), tp
        )

    def rows_copy(i):
        span = pl.ds(pl.multiple_of(near(i) * ret_rows, ret_rows), ret_rows)
        return remote(wrs.at[span], wret.at[z, i], asend.at[i], arecv.at[i], peer(i), tp)

    def cut_of(kind, block):
        if kind == 0:
            return wfox.at[0, block]
        if kind == 1:
            return wret.at[block, 0]
        return wret.at[block, pl.ds(1, group - 1)]

    def up(kind, block):
        ref = cut_of(kind, block)
        return remote(ref, ref, usend.at[kind, block], urecv.at[kind, block], after, tp)

    def down(kind, block):
        ref = cut_of(kind, block)
        return remote(ref, ref, nsend.at[kind, block], nrecv.at[kind, block], before, tp)

    def begin_line(kind):
        @pl.when(z < last)
        def _():
            up(kind, z).start()

        @pl.when(z > 0)
        def _():
            down(kind, z).start()

    def line_up(kind, step):
        below = z - step

        @pl.when(below >= 0)
        def _():
            up(kind, below).wait_recv()

            @pl.when(z < last)
            def _():
                up(kind, below).start()

    def line_down(kind, step):
        above = z + step

        @pl.when(above <= last)
        def _():
            down(kind, above).wait_recv()

            @pl.when(z > 0)
            def _():
                down(kind, above).start()

    def line(kind, step):
        line_up(kind, step)
        line_down(kind, step)

    def settle_line(kind):
        for block in range(depth):

            @pl.when((z < last) & (block <= z))
            def _():
                up(kind, block).wait_send()

            @pl.when((z > 0) & (block >= z))
            def _():
                down(kind, block).wait_send()

    def plane_copy(i):
        return remote(wfox.at[0], wfox.at[i], fsend.at[i], frecv.at[i], peer(i), tp)

    def plane_relay(i):
        span = pl.ds(0, depth // 2) if i == 1 else pl.ds(depth // 2, depth - depth // 2)
        return remote(
            wfox.at[i, span],
            wfox.at[3, span],
            fsend.at[2 + i],
            frecv.at[2 + i],
            peer(3 - i),
            tp,
        )

    def kv_hop(block, i):
        ref = kv.at[block, i]
        return remote(ref, ref, ksend.at[block, i], krecv.at[block, i], after, tp)

    def query_hop(k, i):
        there = lax.rem(sp + n_sp - (k + 1) * group, n_sp)
        return remote(fq.at[i], guest.at[k, i], qsend.at[k, i], qrecv.at[k, i], there, tp)

    slices = 4
    slice_rows = RET_DIM // slices

    def state_hop(c):
        span = pl.ds(c * slice_rows, slice_rows)
        return remote(
            state_out.at[:, span], state_in.at[:, span], ssend.at[c], srecv.at[c], after, tp
        )

    guests = depth - 1 - host

    def num_hop(k, i):
        there = lax.rem(sp + (k + 1) * group, n_sp)
        return remote(
            num_out.at[k, i], num_in.at[i], osend.at[k, i], orecv.at[i], there, tp
        )

    def den_hop(k):
        there = lax.rem(sp + (k + 1) * group, n_sp)
        return remote(
            den_out.at[k], den_in, osend.at[k, group], orecv.at[group], there, tp
        )

    def part_copy(i):
        return remote(
            part.at[i, other_core],
            part_in.at[i],
            psum_send.at[i],
            psum_recv.at[i],
            sp,
            other_core,
        )

    width = out.shape[1]
    half = width // 2
    wide = width // depth
    first_cols = pl.ds(0, half)
    last_cols = pl.ds(half, half)

    def scatter_x(k):
        return remote(
            rsum.at[1 + 2 * k, :, first_cols],
            xa.at[k],
            rsend.at[k],
            rrecv.at[k],
            peer(1),
            tp,
        )

    def scatter_y(k):
        return remote(
            rsum.at[2 + k, :, last_cols],
            yb.at[k],
            rsend.at[2 + k],
            rrecv.at[2 + k],
            peer(2),
            tp,
        )

    def scatter_second(k):
        return remote(
            second_out.at[k],
            second_in.at[k],
            rsend.at[4 + k],
            rrecv.at[4 + k],
            peer(2 if k == 0 else 1),
            tp,
        )

    fw = hfox * FOX_DIM
    my_cols = pl.ds(pl.multiple_of(g * fw, 128), fw)

    def mixed_copy(i):
        return remote(
            fox_buf.at[i], mixed.at[:, my_cols], esend.at[i], erecv.at[i], peer(i), tp
        )

    def final_copy():
        return remote(
            fpart.at[other_core], fgot, esend.at[0], erecv.at[0], sp, other_core
        )

    for i in (1, 2):
        token_copy(i).start()
    pair_copy(0).start()
    with jax.named_scope("first_sends"):
        for i in range(1, n_sp):
            gate_copy(i).start()
        for copy in locals_:
            copy.wait()
        for i in range(1, group):
            rows_copy(i).start()
        begin_line(0)
        begin_line(1)

    head_of = [tp * (group * hret) + g * hret + h for h in range(hret)]
    rates = []
    for h in range(hret):
        ids = jnp.full((1, RET_DIM), head_of[h], jnp.int32)
        heads_float = ids.astype(f32)
        middle = RET_HEADS // 2
        fast_rate = 1.0 / (32.0 + 16.0 * heads_float)
        slow_rate = jnp.exp2(-(heads_float - middle)) / total
        rates.append(jnp.where(ids < middle, fast_rate, slow_rate))
    square = (tok, RET_DIM)
    offset = lax.broadcasted_iota(jnp.int32, square, 0)
    column = lax.broadcasted_iota(jnp.int32, (tok, tok), 1)
    row = lax.broadcasted_iota(jnp.int32, (tok, tok), 0)
    for h in range(hret):
        rate = rates[h]
        spread = jnp.maximum(row - column, 0).astype(f32)
        within[h] = jnp.where(row >= column, jnp.exp(-rate[:, :1] * spread), 0.0)
        steps = offset.astype(f32)
        qdec[h] = jnp.exp(-rate * (steps + 1.0))
        kdec[h] = jnp.exp(-rate * (tok - 1.0 - steps))
    inverse_freq = inv_ref[...]
    unit = 16
    low = lax.broadcasted_iota(jnp.int32, (unit, RET_DIM // 2), 0).astype(f32)
    high = lax.broadcasted_iota(jnp.int32, (tok // unit, RET_DIM // 2), 0).astype(f32)
    cos_low, sin_low = jnp.cos(low * inverse_freq), jnp.sin(low * inverse_freq)
    high = high * float(unit) * inverse_freq
    cos_high, sin_high = jnp.cos(high), jnp.sin(high)
    for a in range(tok // unit):
        ca, sa = cos_high[a : a + 1], sin_high[a : a + 1]
        ctab[a * unit : (a + 1) * unit] = cos_low * ca - sin_low * sa
        stab[a * unit : (a + 1) * unit] = sin_low * ca + cos_low * sa

    half_head = RET_DIM // 2

    run_decay = [jnp.exp(-rates[h] * float(group * tok)) for h in range(hret)]
    tok_decay = [jnp.exp(-rates[h] * float(tok)) for h in range(hret)]

    def sum_state():
        for h in range(hret):
            held = update[g, h]
            for p in range(1, group):
                held = held * tok_decay[h] + update[near(p), h]
            carry_state[h] = held

        @pl.when(z == 0)
        def _():
            state_out[...] = carry_state[...].astype(bf16)
            for c in range(slices):
                state_hop(c).start()

    def retain(i):
        for h in range(hret):
            q = rq[i, h]
            k = rk[i, h]
            v = rv[i, h]
            scores = (
                lax.dot_general(q, k, (((1,), (1,)), ((), ())), preferred_element_type=f32)
                * within[h]
            )
            raw[i, h] = jnp.dot(scores.astype(bf16), v, preferred_element_type=f32)

    def gather_state(i):
        for h in range(hret):
            scaled = (rk[i, h].astype(f32) * kdec[h]).astype(bf16)
            update[i, h] = lax.dot_general(
                scaled, rv[i, h], (((0,), (0,)), ((), ())), preferred_element_type=f32
            )

    def queries_of(k):
        @pl.when(z == host + 1 + k)
        def _():
            for i in range(1, group):
                query_hop(k, i).start()

    def project(i):
        x = xall[i].reshape(tok, xall.shape[3])
        start = jnp.full((1, half_head), z * (group * tok) + near(i) * tok, jnp.int32)
        turn = start.astype(f32) * inverse_freq
        cos_turn, sin_turn = jnp.cos(turn), jnp.sin(turn)
        for m in (4, 5, 3, 1, 2, 0) if i < 3 else (1, 2, 4, 5, 3, 0):
            cut = w_ret if m < 3 else w_fox
            y = jnp.dot(x, cut[m % 3], preferred_element_type=f32).astype(bf16)
            if m < 2:
                cosine = ctab[...] * cos_turn - stab[...] * sin_turn
                sine = stab[...] * cos_turn + ctab[...] * sin_turn
            for h in range(hret if m < 3 else hfox):
                if m < 2:
                    lo = h * RET_DIM
                    a = y[:, lo : lo + half_head].astype(f32)
                    b = y[:, lo + half_head : lo + RET_DIM].astype(f32)
                    to = rq if m == 0 else rk
                    by = 1.0 if m == 0 else RET_DIM ** (-0.5)
                    to[i, h, :, :half_head] = ((a * cosine - b * sine) * by).astype(bf16)
                    to[i, h, :, half_head:] = ((a * sine + b * cosine) * by).astype(bf16)
                elif m == 2:
                    rv[i, h] = y[:, h * RET_DIM : (h + 1) * RET_DIM]
                elif m == 3:
                    fq[i, h] = y[:, h * FOX_DIM : (h + 1) * FOX_DIM]
                else:
                    kv[z, i, m - 4, h] = y[:, h * FOX_DIM : (h + 1) * FOX_DIM]
            if m == 2:
                gather_state(i)
                if i == 3:
                    sum_state()
            if m == 5:
                ready = z < (last, 0, 1, 1)[i]

                @pl.when(ready)
                def _():
                    kv_hop(z, i).start()

            if m == 3 and i == 0:
                for k in range(guests):

                    @pl.when(z == host + 1 + k)
                    def _(k=k):
                        query_hop(k, 0).start()

    def second_piece():
        @pl.when(z < last - 1)
        def _():
            kv_hop(z, 1).start()

    def late_pieces():
        @pl.when(z < last)
        def _():
            for c in range(slices):
                state_hop(c).wait_send()

        for i in range(1, group):

            @pl.when((z >= (last - 1 if i == 1 else 1)) & (z < last))
            def _():
                kv_hop(z, i).start()

    def phase(name, *steps):
        with jax.named_scope(name):
            for step in steps:
                step[0](*step[1:])

    def wait_loads():
        for copy in loads:
            copy.wait()
        pair_copy(0).wait_recv()

    def tokens_on(i):
        token_copy(i).wait_recv()
        token_relay(i).start()
        pair_copy(i).start()

    def wait_rows():
        for i in range(1, group):
            rows_copy(i).wait_recv()

    def wait_pair(i):
        pair_copy(i).wait_recv()

    def tokens_last():
        for i in (1, 2):
            token_relay(i).wait_recv()
        pair_copy(3).start()

    def begin_plane():
        for i in (1, 2):
            plane_copy(i).start()

    def pass_state():
        @pl.when(z > 0)
        def _():
            for c in range(slices):
                span = slice(c * slice_rows, (c + 1) * slice_rows)
                state_hop(c).wait_recv()

                @pl.when(z < last)
                def _():
                    for h in range(hret):
                        held = state_in[h, span].astype(f32) * run_decay[h] + carry_state[h, span]
                        state_out[h, span] = held.astype(bf16)
                    state_hop(c).start()

            carry_state[...] = state_in[...].astype(f32)

        @pl.when(z == 0)
        def _():
            carry_state[...] = jnp.zeros(carry_state.shape, f32)

    def gate_row(plane, i, h):
        return gall[plane * group + near(i), pl.ds(g * hfox + h, 1), :]

    def spread_columns(line_row, to, i, h):
        for c in range(tok // 128):
            piece = line_row[:, c * 128 : (c + 1) * 128]
            to[i, h, c * 128 : (c + 1) * 128, :] = jnp.broadcast_to(piece, (128, 128)).T

    def gate_columns():
        for i in range(1, n_sp):
            gate_copy(i).wait_recv()
        for h in range(hfox):
            for i in range(group):
                spread_columns(gate_row(z, i, h), gcol, i, h)

        @pl.when(z == host)
        def _():
            for k in range(guests):
                for h in range(hfox):
                    for i in range(group):
                        spread_columns(gate_row(host + 1 + k, i, h), guest_col.at[k], i, h)

    inverse = FOX_DIM ** (-0.5)

    def weigh(q, column_gates, keys, key_gates, mask=None):
        scores = (
            lax.dot_general(q, keys, (((1,), (1,)), ((), ())), preferred_element_type=f32)
            * inverse
        )
        count = keys.shape[0] // 128
        scores = scores + jnp.concatenate([column_gates] * count, axis=1) - key_gates
        if mask is not None:
            scores = jnp.where(mask, scores, -jnp.inf)
        return jnp.exp(scores).astype(bf16)

    def widen(v):
        return jnp.concatenate([v, jnp.ones(v.shape, bf16)], axis=1)

    def own_attention():
        mask = row >= column
        for h in range(hfox):
            for t in range(group):
                it = near(t)
                weights, vals = [], []
                for s in range(t + 1):
                    js = near(s)
                    weights.append(
                        weigh(
                            fq[it, h],
                            gcol[it, h],
                            kv[z, js, 0, h],
                            gall[z * group + s, pl.ds(g * hfox + h, 1), :],
                            mask if s == t else None,
                        )
                    )
                    vals.append(kv[z, js, 1, h])
                w = weights[0] if t == 0 else jnp.concatenate(weights, axis=1)
                v = vals[0] if t == 0 else jnp.concatenate(vals, axis=0)
                numer[it, h] = jnp.dot(w, widen(v), preferred_element_type=f32)

    def attend(block, queries, columns, to, fresh, done=None):
        for h in range(hfox):
            keys = kv[block, :, 0, h].reshape(group * tok, FOX_DIM)
            vals = widen(kv[block, :, 1, h].reshape(group * tok, FOX_DIM))
            key_gates = jnp.concatenate([gate_row(block, i, h) for i in range(group)], axis=1)

            def query_step(p, carry):
                for j in (2 * p, 2 * p + 1):
                    w = weigh(queries[j, h], columns[j, h], keys, key_gates)
                    product = jnp.dot(w, vals, preferred_element_type=f32)
                    if fresh:
                        to[j, h] = product
                    else:
                        to[j, h] += product
                if done is not None and h == hfox - 1:
                    done(2 * p)
                    done(2 * p + 1)
                return carry

            lax.fori_loop(0, group // 2, query_step, 0)

    lines = tok // 128

    def serve(k):
        def hand_back(j):
            for h in range(hfox):
                num_out[k, j, h] = guest_numer[k, j, h, :, :FOX_DIM].astype(bf16)
                for c in range(lines):
                    at = (j * hfox + h) * lines + c
                    den = guest_numer[k, j, h, c * 128 : (c + 1) * 128, FOX_DIM:]
                    den_out[k, pl.ds(at, 1), :] = den.T[0:1]
            num_hop(k, j).start()

        @pl.when(z == host)
        def _():
            for i in range(group):
                query_hop(k, i).wait_recv()
            for block in range(k + 1):
                attend(
                    block,
                    guest.at[k],
                    guest_col.at[k],
                    guest_numer.at[k],
                    block == 0,
                    hand_back if block == k else None,
                )
            den_hop(k).start()

    def take_back():
        den_hop(0).wait_recv()
        for i in range(group):
            num_hop(0, i).wait_recv()
            for h in range(hfox):
                numer[i, h, :, :FOX_DIM] += num_in[i, h].astype(f32)
                for c in range(lines):
                    at = (i * hfox + h) * lines + c
                    den = jnp.broadcast_to(den_in[at : at + 1, :], (128, 128)).T
                    numer[i, h, c * 128 : (c + 1) * 128, FOX_DIM:] += den

    def earlier():
        @pl.when(z > 0)
        def _():
            attend(z - 1, fq, gcol, numer, False)

    def retention_out():
        for h in range(hret):
            held = carry_state[h]
            for p in range(group):
                ip = near(p)
                cross = jnp.dot(rq[ip, h], held.astype(bf16), preferred_element_type=f32)
                full = raw[ip, h] + cross * qdec[h]
                rq[ip, h] = normalize(full)
                if p < group - 1:
                    held = held * tok_decay[h] + update[ip, h]

    def ret_product(*order):
        left = jnp.concatenate(
            [jnp.concatenate([rq[i, h] for i in order], axis=0) for h in range(hret)], axis=1
        )

        def column_step(p, carry):
            right = jnp.concatenate([wret[p, near(e)] for e in range(group)], axis=1)
            product = jnp.dot(left, right, preferred_element_type=f32).astype(bf16)
            at = pl.ds(pl.multiple_of(p * wide, wide), wide)
            for e in range(2 * len(order)):
                part[order[e // 2], e % 2, :, at] = product[e * rows : (e + 1) * rows]
            return carry

        lax.fori_loop(0, depth, column_step, 0)
        for i in order:
            part_copy(i).start()

    def plane_on():
        for i in (1, 2):
            plane_copy(i).wait_recv()
            plane_relay(i).start()

    def take_all():
        @pl.when((z > 0) & (z != host))
        def _():
            for i in range(group):
                kv_hop(z - 1, i).wait_recv()

    def serve_first():
        @pl.when(z == host)
        def _():
            for i in range(group):
                kv_hop(z - 1, i).wait_recv()

        serve(0)

    def serve_rest():
        for k in range(1, guests):
            serve(k)

    def scatter_first(*order):
        for i in order:
            part_copy(i).wait_recv()
            rsum[i] = (part[i, tp].astype(f32) + part_in[i].astype(f32)).astype(bf16)
            if i == 3:
                scatter_x(1).start()
                scatter_y(1).start()
            elif i == 1:
                scatter_x(0).start()
            elif i == 2:
                scatter_y(0).start()

    def scatter_next():
        scatter_x(1).wait_recv()
        scatter_y(1).wait_recv()
        second_out[0] = (rsum[2, :, :half].astype(f32) + xa[1].astype(f32)).astype(bf16)
        second_out[1] = (rsum[1, :, half:].astype(f32) + yb[1].astype(f32)).astype(bf16)
        for k in range(2):
            scatter_second(k).start()

    def guest_sums():
        @pl.when(z > host)
        def _():
            take_back()

    def send_fox():
        for i in range(group):
            for h in range(hfox):
                fox_buf[i, :, h * FOX_DIM : (h + 1) * FOX_DIM] = normalize(
                    numer[i, h, :, :FOX_DIM] / numer[i, h, :, FOX_DIM:]
                )
            if i > 0:
                mixed_copy(i).start()
        mixed[:, my_cols] = fox_buf[0]

    def wait_fox():
        for i in (1, 2):
            plane_relay(i).wait_recv()
        for i in range(1, group):
            mixed_copy(i).wait_recv()

    def fox_out():
        def fox_column(p, carry):
            right = jnp.concatenate([wfox[near(e), p] for e in range(group)], axis=1)
            product = jnp.dot(mixed[...], right, preferred_element_type=f32).astype(bf16)
            at = pl.ds(pl.multiple_of(p * wide, wide), wide)
            fpart[0, :, at] = product[:rows]
            fpart[1, :, at] = product[rows:]
            return carry

        lax.fori_loop(0, depth, fox_column, 0)
        final_copy().start()

    def wait_final():
        scatter_x(0).wait_recv()
        scatter_y(0).wait_recv()
        for k in range(2):
            scatter_second(k).wait_recv()
        final_copy().wait_recv()

    def finish():
        mine = fpart[tp].astype(f32) + fgot[...].astype(f32)
        ret_low = rsum[0, :, :half].astype(f32) + xa[0].astype(f32) + second_in[0].astype(f32)
        ret_high = rsum[0, :, half:].astype(f32) + yb[0].astype(f32) + second_in[1].astype(f32)
        out[:, :half] = (mine[:, :half] + ret_low).astype(bf16)
        out[:, half:] = (mine[:, half:] + ret_high).astype(bf16)

    phase("w_loads", (wait_loads,))
    phase("project0", (project, 0))
    phase("line01", (line, 0, 1), (line, 1, 1))
    phase("retain0", (retain, 0))
    phase("tokens1", (tokens_on, 1))
    phase("tokens2", (tokens_on, 2))
    phase("line02", (line, 0, 2), (line, 1, 2))
    phase("w_pair1", (wait_pair, 1))
    phase("project1", (project, 1))
    phase("w_rows", (wait_rows,), (begin_line, 2), (second_piece,))
    phase("w_pair2", (wait_pair, 2))
    phase("project2", (project, 2))
    for step in range(3, depth):
        phase("line0" + str(step), (line, 0, step), (line, 1, step))
    phase("begin_plane", (begin_plane,))
    phase("retain1", (retain, 1))
    phase("retain2", (retain, 2))
    phase("tokens3", (tokens_last,))
    phase("w_pair3", (wait_pair, 3))
    phase("up21", (line_up, 2, 1))
    phase("down21", (line_down, 2, 1))
    phase("project3", (project, 3))
    upper = z > host

    @pl.when(upper)
    def _():
        phase("retain3", (retain, 3))
        phase("gates", (gate_columns,))
        phase("query0", (queries_of, 0))
        phase("up22", (line_up, 2, 2))

    @pl.when(z == last)
    def _():
        phase("plane_on", (plane_on,), (queries_of, 1))

    phase("pass_state", (pass_state,))

    @pl.when(upper & (z < last))
    def _():
        phase("plane_on", (plane_on,))

    @pl.when(z <= host)
    def _():
        phase("down22", (line_down, 2, 2))
        phase("retain3", (retain, 3))
        phase("gates", (gate_columns,))
        phase("plane_on", (plane_on,))

    phase("own_attention", (own_attention,))
    for step in range(3, depth):
        phase("line2" + str(step), (line, 2, step))
    phase("late_pieces", (late_pieces,))
    phase("retention_out", (retention_out,))
    phase("ret_product1", (ret_product, 3, 1))
    phase("ret_product2", (ret_product, 2, 0))
    phase("serve0", (serve_first,))
    phase("scatter1a", (scatter_first, 3, 1))
    phase("scatter1b", (scatter_first, 2, 0))
    phase("serve1", (serve_rest,))
    phase("takes", (take_all,))
    phase("earlier", (earlier,))
    phase("guest_sums", (guest_sums,))
    phase("send_fox", (send_fox,))
    phase("scatter2", (scatter_next,))
    phase("w_fox", (wait_fox,))
    phase("fox_out", (fox_out,))
    phase("w_final", (wait_final,))
    phase("finish", (finish,))

    def settle_all():
        for i in (1, 2):
            token_copy(i).wait_send()
            token_relay(i).wait_send()
            plane_copy(i).wait_send()
            plane_relay(i).wait_send()
        for i in range(group):
            pair_copy(i).wait_send()
            part_copy(i).wait_send()
        for i in range(1, group):
            rows_copy(i).wait_send()
            mixed_copy(i).wait_send()
        for i in range(1, n_sp):
            gate_copy(i).wait_send()
        for kind in range(3):
            settle_line(kind)
        for k in range(2):
            scatter_x(k).wait_send()
            scatter_y(k).wait_send()
            scatter_second(k).wait_send()
        final_copy().wait_send()

        @pl.when(z < last)
        def _():
            for i in range(group):
                kv_hop(z, i).wait_send()

        for k in range(guests):

            @pl.when(z == host + 1 + k)
            def _(k=k):
                for i in range(group):
                    query_hop(k, i).wait_send()

        @pl.when(z == host)
        def _():
            for k in range(guests):
                for i in range(group):
                    num_hop(k, i).wait_send()
                den_hop(k).wait_send()

    phase("settle", (settle_all,))


def fused(tokens, gain, gates, inverse, w_ret, w_fox, w_in, hret, hfox, n_sp):
    rows, width = tokens.shape
    group = 4
    tok = 2 * rows
    depth = n_sp // group
    out_cols = n_sp * w_ret.shape[1]
    half = out_cols // 2
    ret_rows = hret * RET_DIM
    fox_rows = group * hfox * FOX_DIM
    vmem = pl.BlockSpec(memory_space=pltpu.VMEM)
    hbm = pl.BlockSpec(memory_space=pl.ANY)
    dma = pltpu.SemaphoreType.DMA
    f32 = jnp.float32
    bf16 = jnp.bfloat16
    square = (hret, RET_DIM, RET_DIM)
    heads = (group, hfox, tok, FOX_DIM)
    dens = group * hfox * (tok // 128)
    guests = depth - 2
    total = float(tok * n_sp)

    def body(*refs):
        fused_kernel(n_sp, total, *refs[:6], refs[6:12], *refs[12:])

    V = pltpu.VMEM
    return pl.pallas_call(
        body,
        out_shape=jax.ShapeDtypeStruct((rows, out_cols), bf16),
        in_specs=[vmem] * 4 + [hbm] * 8,
        out_specs=vmem,
        scratch_shapes=[
            V((group, 2, rows, width), bf16),
            V((3, width, ret_rows), bf16),
            V((3, width, hfox * FOX_DIM), bf16),
            V(w_ret.shape, bf16),
            V((depth, group, ret_rows, w_ret.shape[1]), bf16),
            V((group, depth, fox_rows, w_ret.shape[1]), bf16),
            V((n_sp,) + gates.shape, f32),
            V((tok, RET_DIM // 2), f32),
            V((tok, RET_DIM // 2), f32),
            V((hret, tok, tok), f32),
            V((hret, tok, RET_DIM), f32),
            V((hret, tok, RET_DIM), f32),
            V((group, hret, tok, RET_DIM), bf16),
            V((group, hret, tok, RET_DIM), bf16),
            V((group, hret, tok, RET_DIM), bf16),
            V(heads, bf16),
            V((guests,) + heads, bf16),
            V((depth, group, 2, hfox, tok, FOX_DIM), bf16),
            V((group, hret, tok, RET_DIM), f32),
            V((group,) + square, f32),
            V(square, bf16),
            V(square, bf16),
            V(square, f32),
            V((group, hfox, tok, 128), f32),
            V((guests, group, hfox, tok, 128), f32),
            V((group, hfox, tok, 2 * FOX_DIM), f32),
            V((guests, group, hfox, tok, 2 * FOX_DIM), f32),
            V((guests,) + heads, bf16),
            V(heads, bf16),
            V((guests, dens, 128), f32),
            V((dens, 128), f32),
            V((group, 2, rows, out_cols), bf16),
            V((group, rows, out_cols), bf16),
            V((group, rows, out_cols), bf16),
            V((2, rows, half), bf16),
            V((2, rows, half), bf16),
            V((2, rows, half), bf16),
            V((2, rows, half), bf16),
            V((group, tok, hfox * FOX_DIM), bf16),
            V((tok, fox_rows), bf16),
            V((2, rows, out_cols), bf16),
            V((rows, out_cols), bf16),
            dma((9,)),
            dma((3,)),
            dma((3,)),
            dma((3,)),
            dma((3,)),
            dma((group,)),
            dma((group,)),
            dma((n_sp,)),
            dma((n_sp,)),
            dma((group,)),
            dma((group,)),
            dma((3, depth)),
            dma((3, depth)),
            dma((3, depth)),
            dma((3, depth)),
            dma((5,)),
            dma((5,)),
            dma((depth, group)),
            dma((depth, group)),
            dma((guests, group)),
            dma((guests, group)),
            dma((4,)),
            dma((4,)),
            dma((guests, group + 1)),
            dma((group + 1,)),
            dma((group,)),
            dma((group,)),
            dma((6,)),
            dma((6,)),
            dma((group,)),
            dma((group,)),
        ],
        compiler_params=pltpu.CompilerParams(
            collective_id=2, has_side_effects=True, vmem_limit_bytes=VMEM_LIMIT
        ),
        name="fused",
    )(tokens, gain, gates, inverse, w_ret, w_fox, *w_in)


def decay_rates(head_ids, total):
    heads_float = head_ids.astype(jnp.float32)
    middle = RET_HEADS // 2
    fast_rate = 1.0 / (32.0 + 16.0 * heads_float)
    slow_rate = jnp.exp2(-(heads_float - middle)) / total
    return jnp.where(head_ids < middle, fast_rate, slow_rate)


def per_device(
    n_sp,
    n_tp,
    tokens,
    gain,
    w_ret_q,
    w_ret_k,
    w_ret_v,
    w_fox_q,
    w_fox_k,
    w_fox_v,
    fox_gates,
    w_out_ret,
    w_out_fox,
):
    f32 = jnp.float32
    rows, width = tokens.shape
    ret_heads = w_ret_q.shape[1] // RET_DIM
    fox_heads = w_fox_q.shape[1] // FOX_DIM
    group = math.gcd(math.gcd(ret_heads, fox_heads), n_sp)
    depth = n_sp // group
    hret = ret_heads // group
    hfox = fox_heads // group
    run = rows * n_tp * group
    half = RET_DIM // 2
    inverse = 10000.0 ** (-jnp.arange(half, dtype=f32) / half)
    if group == 4 and n_tp == 2 and depth == 4:
        return fused(
            tokens,
            gain.reshape(1, width),
            fox_gates.T,
            inverse.reshape(1, half),
            w_out_ret,
            w_out_fox,
            (w_ret_q, w_ret_k, w_ret_v, w_fox_q, w_fox_k, w_fox_v),
            hret,
            hfox,
            n_sp,
        )
    sp = lax.axis_index("sp")
    g = lax.rem(sp, group)
    z = sp // group

    positions = z * run + jnp.arange(run, dtype=jnp.int32)
    angles = positions.astype(f32)[:, None] * inverse[None, :]
    rq, rk, rv, fq, fkv, gall, wz = gather(
        tokens,
        gain.reshape(1, width),
        fox_gates.T,
        w_out_ret,
        w_out_fox,
        jnp.cos(angles),
        jnp.sin(angles),
        (w_ret_q, w_ret_k, w_ret_v, w_fox_q, w_fox_k, w_fox_v),
        hret,
        hfox,
        n_sp,
        n_tp,
        group,
    )

    head_ids = (
        lax.axis_index("tp") * ret_heads + g * hret + jnp.arange(hret, dtype=jnp.int32)
    )
    rates = decay_rates(head_ids, float(run * depth))
    offsets = jnp.arange(BLOCK, dtype=f32)
    spread = offsets[:, None] - offsets[None, :]
    causal = spread >= 0
    within = jnp.where(
        causal[None], jnp.exp(-rates[:, None, None] * jnp.where(causal, spread, 0.0)[None]), 0.0
    )
    steps = jnp.arange(run, dtype=f32)
    qdec = jnp.exp(-rates[:, None] * (steps[None, :] + 1.0))[:, :, None]
    kdec = jnp.exp(-rates[:, None] * (BLOCK - 1.0 - offsets[None, :]))[:, :, None]
    lengths = jnp.array([BLOCK, run], f32)
    bdec = jnp.broadcast_to(
        jnp.exp(-rates[:, None] * lengths[None, :])[:, :, None], (hret, 2, RET_DIM)
    )

    own_gates = lax.dynamic_slice_in_dim(gall, g * hfox, hfox, 1)
    line = own_gates.transpose(1, 0, 2).reshape(hfox, depth, 1, run)
    gq = lax.dynamic_index_in_dim(line, z, 1, False).reshape(hfox, run, 1)
    return mixer(
        rq, rk, rv, fq, fkv, gq, line, within, qdec, kdec, bdec, wz, rows, n_sp, n_tp, group
    )


def solution(mesh):
    in_specs = (
        P(("sp", "tp"), None),
        P(),
        P(None, "tp"),
        P(None, "tp"),
        P(None, "tp"),
        P(None, "tp"),
        P(None, "tp"),
        P(None, "tp"),
        P("sp", "tp"),
        P("tp", "sp"),
        P("tp", "sp"),
    )
    out_specs = P(("sp", "tp"), None)
    return jax.shard_map(
        functools.partial(per_device, mesh.shape["sp"], mesh.shape["tp"]),
        mesh=mesh,
        in_specs=in_specs,
        out_specs=out_specs,
        check_vma=False,
    )
```

```python
import functools
import math

import jax
import jax.numpy as jnp
from jax import lax
from jax.experimental import pallas as pl
from jax.experimental.pallas import tpu as pltpu
from jax.sharding import PartitionSpec as P

RET_HEADS = 8
RET_DIM = 256
FOX_DIM = 128
BLOCK = 128
MESH = pl.DeviceIdType.MESH
VMEM_LIMIT = 60 * 1024 * 1024
FUSED_LIMIT = 52 * 1024 * 1024

eps = 1e-06


def remote(src, dst, send, recv, sp, tp):
    return pltpu.make_async_remote_copy(
        src_ref=src,
        dst_ref=dst,
        send_sem=send,
        recv_sem=recv,
        device_id=(sp, tp),
        device_id_type=MESH,
    )


def gather_kernel(
    n_sp,
    n_tp,
    group,
    tok_ref,
    gain_ref,
    gates_ref,
    wr_ref,
    wf_ref,
    cos_ref,
    sin_ref,
    w_in,
    rq,
    rk,
    rv,
    fq,
    fkv,
    gall,
    wz,
    own,
    xall,
    w_ret,
    w_fox,
    local_sem,
    in_sem,
    tsend,
    trecv,
    dsend,
    drecv,
    psend,
    precv,
    gsend,
    grecv,
    usend,
    urecv,
    nsend,
    nrecv,
):
    sp = lax.axis_index("sp")
    tp = lax.axis_index("tp")
    g = lax.rem(sp, group)
    z = sp // group
    depth = n_sp // group
    rows = tok_ref.shape[0]
    half = rows // 2
    krows = wr_ref.shape[0]

    barrier = pltpu.get_barrier_semaphore()
    for i in range(1, n_sp):
        pl.semaphore_signal(
            barrier, inc=1, device_id=(lax.rem(sp + i, n_sp), tp), device_id_type=MESH
        )
    for i in range(1, n_tp):
        pl.semaphore_signal(
            barrier, inc=1, device_id=(sp, lax.rem(tp + i, n_tp)), device_id_type=MESH
        )

    loads = []
    for i in range(6):
        cut = w_ret if i < 3 else w_fox
        size = cut.shape[2]
        columns = pl.ds(pl.multiple_of(g * size, 128), size)
        loads.append(
            pltpu.make_async_copy(w_in[i].at[:, columns], cut.at[i % 3], in_sem.at[i])
        )

    values = tok_ref[...].astype(jnp.float32)
    scale = lax.rsqrt(jnp.mean(values * values, axis=1, keepdims=True) + eps)
    own[...] = (values * scale * gain_ref[...]).astype(jnp.bfloat16)
    copies = [
        pltpu.make_async_copy(wr_ref, wz.at[z, pl.ds(0, krows)], local_sem.at[0]),
        pltpu.make_async_copy(
            wf_ref, wz.at[z, pl.ds(krows, wf_ref.shape[0])], local_sem.at[1]
        ),
        pltpu.make_async_copy(gates_ref, gall.at[sp], local_sem.at[2]),
    ]
    for copy in copies + loads:
        copy.start()
    pl.semaphore_wait(barrier, n_sp + n_tp - 2)

    def slot(which, core):
        return xall.at[which * n_tp + core]

    mine = pltpu.make_async_copy(own, slot(g, tp), local_sem.at[3])
    mine.start()

    def peer(other):
        return z * group + other

    hyper = group == 4
    direct = []
    for i in range(1, group):
        if hyper and i == 3:
            continue
        other = lax.bitwise_xor(g, i) if hyper else lax.rem(g + i, group)
        direct.append(
            remote(own, slot(g, tp), tsend.at[i], trecv.at[i], peer(other), tp)
        )
    for copy in direct:
        copy.start()
    pair = []
    for i in range(1, n_tp):
        copy = remote(
            own, slot(g, tp), psend.at[0, i], precv.at[0, i], sp, lax.rem(tp + i, n_tp)
        )
        copy.start()
        pair.append(copy)
    gate_copies = []
    for i in range(1, n_sp):
        copy = remote(
            gates_ref, gall.at[sp], gsend.at[i], grecv.at[i], lax.rem(sp + i, n_sp), tp
        )
        copy.start()
        gate_copies.append(copy)

    copies[0].wait()
    copies[1].wait()

    def up(block):
        return remote(
            wz.at[block],
            wz.at[block],
            usend.at[block],
            urecv.at[block],
            lax.rem(sp + group, n_sp),
            tp,
        )

    def down(block):
        return remote(
            wz.at[block],
            wz.at[block],
            nsend.at[block],
            nrecv.at[block],
            lax.rem(sp + n_sp - group, n_sp),
            tp,
        )

    @pl.when(z < depth - 1)
    def _():
        up(z).start()

    @pl.when(z > 0)
    def _():
        down(z).start()

    ready = {0: pair[:]}

    def forward(which, row):
        ready[row] = []
        for i in range(1, n_tp):
            copy = remote(
                slot(which, tp),
                slot(which, tp),
                psend.at[row, i],
                precv.at[row, i],
                sp,
                lax.rem(tp + i, n_tp),
            )
            copy.start()
            pair.append(copy)
            ready[row].append(copy)

    count = n_tp * rows
    half_head = RET_DIM // 2

    def project(which, row):
        for copy in ready[row]:
            copy.wait_recv()
        x = xall[pl.ds(which * n_tp, n_tp)].reshape(count, xall.shape[2])
        span = pl.ds(pl.multiple_of(which * count, count), count)
        for i in range(6):
            cut = w_ret if i < 3 else w_fox
            y = jnp.dot(x, cut[i % 3], preferred_element_type=jnp.float32)
            y = y.astype(jnp.bfloat16)
            if i < 2:
                cosine = cos_ref[span, :]
                sine = sin_ref[span, :]
            for h in range(rq.shape[0] if i < 3 else fq.shape[0]):
                if i < 2:
                    lo = h * RET_DIM
                    a = y[:, lo : lo + half_head].astype(jnp.float32)
                    b = y[:, lo + half_head : lo + RET_DIM].astype(jnp.float32)
                    to = rq if i == 0 else rk
                    by = 1.0 if i == 0 else RET_DIM ** (-0.5)
                    first = (a * cosine - b * sine) * by
                    second = (a * sine + b * cosine) * by
                    to[h, span, :half_head] = first.astype(jnp.bfloat16)
                    to[h, span, half_head:] = second.astype(jnp.bfloat16)
                elif i == 2:
                    rv[h, span, :] = y[:, h * RET_DIM : (h + 1) * RET_DIM]
                elif i == 3:
                    fq[h, span, :] = y[:, h * FOX_DIM : (h + 1) * FOX_DIM]
                else:
                    fkv[i - 4, h, span, :] = y[:, h * FOX_DIM : (h + 1) * FOX_DIM]

    mine.wait()
    for copy in loads:
        copy.wait()
    if not hyper:
        project(g, 0)

    if hyper:
        relays = []
        for i in (1, 2):
            direct[i - 1].wait_recv()
            source = lax.bitwise_xor(g, i)
            target = lax.bitwise_xor(g, 3 - i)
            part = pl.ds((i - 1) * half, half)
            copy = remote(
                slot(source, tp).at[part],
                slot(source, tp).at[part],
                dsend.at[i],
                drecv.at[i],
                peer(target),
                tp,
            )
            copy.start()
            relays.append(copy)
            forward(source, i)
        project(g, 0)
    else:
        for i in range(1, group):
            direct[i - 1].wait_recv()
            forward(lax.rem(g + group - i, group), i)
            project(lax.rem(g + group - i, group), i)

    def line(step, carry):
        below = z - step
        above = z + step

        @pl.when(below >= 0)
        def _():
            up(below).wait_recv()

            @pl.when(z < depth - 1)
            def _():
                up(below).start()

        @pl.when(above <= depth - 1)
        def _():
            down(above).wait_recv()

            @pl.when(z > 0)
            def _():
                down(above).start()

        return carry

    split = depth // 2 if hyper else depth
    lax.fori_loop(1, split, line, 0)
    if hyper:
        project(lax.bitwise_xor(g, 1), 1)
        for copy in relays:
            copy.wait_recv()
        forward(lax.bitwise_xor(g, 3), 3)
    lax.fori_loop(split, depth - 1, line, 0)
    if hyper:
        project(lax.bitwise_xor(g, 2), 2)
        project(lax.bitwise_xor(g, 3), 3)
    lax.fori_loop(max(split, depth - 1), depth, line, 0)

    def settle(step, carry):
        @pl.when((z < depth - 1) & (step <= z))
        def _():
            up(step).wait_send()

        @pl.when((z > 0) & (step >= z))
        def _():
            down(step).wait_send()

        return carry

    lax.fori_loop(0, depth, settle, 0)
    for copy in direct:
        copy.wait_send()
    if hyper:
        for copy in relays:
            copy.wait_send()
    for copy in gate_copies:
        copy.wait()
    for copy in pair:
        copy.wait_send()
    copies[2].wait()


def gather(
    tokens, gain, gates, w_ret, w_fox, cosine, sine, w_in, hret, hfox, n_sp, n_tp, group
):
    rows, width = tokens.shape
    depth = n_sp // group
    out_rows = w_ret.shape[0] + w_fox.shape[0]
    vmem = pl.BlockSpec(memory_space=pltpu.VMEM)
    hbm = pl.BlockSpec(memory_space=pl.ANY)
    dma = pltpu.SemaphoreType.DMA
    run = rows * n_tp * group
    bf16 = jnp.bfloat16

    def body(*refs):
        gather_kernel(n_sp, n_tp, group, *refs[:7], refs[7:13], *refs[13:])

    return pl.pallas_call(
        body,
        out_shape=(
            jax.ShapeDtypeStruct((hret, run, RET_DIM), bf16),
            jax.ShapeDtypeStruct((hret, run, RET_DIM), bf16),
            jax.ShapeDtypeStruct((hret, run, RET_DIM), bf16),
            jax.ShapeDtypeStruct((hfox, run, FOX_DIM), bf16),
            jax.ShapeDtypeStruct((2, hfox, run, FOX_DIM), bf16),
            jax.ShapeDtypeStruct((n_sp,) + gates.shape, jnp.float32),
            jax.ShapeDtypeStruct((depth, out_rows, w_ret.shape[1]), jnp.bfloat16),
        ),
        in_specs=[vmem, vmem, vmem, hbm, hbm, vmem, vmem] + [hbm] * 6,
        out_specs=(vmem,) * 7,
        scratch_shapes=[
            pltpu.VMEM((rows, width), bf16),
            pltpu.VMEM((group * n_tp, rows, width), bf16),
            pltpu.VMEM((3, width, hret * RET_DIM), bf16),
            pltpu.VMEM((3, width, hfox * FOX_DIM), bf16),
            dma((4,)),
            dma((6,)),
            dma((max(group, 2),)),
            dma((max(group, 2),)),
            dma((3,)),
            dma((3,)),
            dma((group, n_tp)),
            dma((group, n_tp)),
            dma((n_sp,)),
            dma((n_sp,)),
            dma((depth,)),
            dma((depth,)),
            dma((depth,)),
            dma((depth,)),
        ],
        compiler_params=pltpu.CompilerParams(
            collective_id=0, has_side_effects=True, vmem_limit_bytes=VMEM_LIMIT
        ),
        name="gather",
    )(tokens, gain, gates, w_ret, w_fox, cosine, sine, *w_in)


def normalize(values):
    return (
        values * lax.rsqrt(jnp.mean(values * values, axis=1, keepdims=True) + eps)
    ).astype(jnp.bfloat16)


def mixer_kernel(
    n_sp,
    n_tp,
    group,
    rq,
    rk,
    rv,
    fq,
    fkv,
    gq,
    gk,
    within,
    qdec,
    kdec,
    bdec,
    wz,
    out,
    w_all,
    slots,
    raw,
    state,
    state_in,
    state_out,
    numer,
    denom,
    ret_buf,
    fox_buf,
    mixed,
    part,
    got,
    local_sem,
    ksend,
    krecv,
    ssend,
    srecv,
    wsend,
    wrecv,
    dsend,
    drecv,
    asend,
    arecv,
    osend,
    orecv,
):
    sp = lax.axis_index("sp")
    tp = lax.axis_index("tp")
    g = lax.rem(sp, group)
    z = sp // group
    depth = n_sp // group
    hret = rq.shape[0]
    hfox = fq.shape[0]
    run = rq.shape[1]
    tok = run // group
    rows = out.shape[0]
    after = lax.rem(sp + group, n_sp)
    before = lax.rem(sp + n_sp - group, n_sp)
    f32 = jnp.float32

    def peer(other):
        return z * group + other

    barrier = pltpu.get_barrier_semaphore()
    for i in range(1, group):
        pl.semaphore_signal(
            barrier, inc=1, device_id=(peer(lax.rem(g + i, group)), tp), device_id_type=MESH
        )
    for i in range(1, n_tp):
        pl.semaphore_signal(
            barrier, inc=1, device_id=(sp, lax.rem(tp + i, n_tp)), device_id_type=MESH
        )
    if depth > 1:

        @pl.when(z < depth - 1)
        def _():
            pl.semaphore_signal(barrier, inc=1, device_id=(after, tp), device_id_type=MESH)

        @pl.when(z > 0)
        def _():
            pl.semaphore_signal(barrier, inc=1, device_id=(before, tp), device_id_type=MESH)

    ends = (z + depth - 1) // depth + (2 * depth - 2 - z) // depth
    pl.semaphore_wait(barrier, group + n_tp - 2 + ends)

    def first_hop():
        return remote(fkv, slots.at[z], ksend.at[z], krecv.at[z], after, tp)

    def hop(block):
        return remote(
            slots.at[block], slots.at[block], ksend.at[block], krecv.at[block], after, tp
        )

    if depth > 1:

        @pl.when(z < depth - 1)
        def _():
            first_hop().start()

    hyper = group == 4
    mine = pltpu.make_async_copy(wz, w_all.at[g], local_sem.at[0])
    mine.start()
    direct = []
    for i in range(1, group):
        if hyper and i == 3:
            continue
        other = lax.bitwise_xor(g, i) if hyper else lax.rem(g + i, group)
        direct.append(
            remote(wz, w_all.at[g], wsend.at[i], wrecv.at[i], peer(other), tp)
        )
    for copy in direct:
        copy.start()

    def relay(i):
        source = lax.bitwise_xor(g, i)
        target = lax.bitwise_xor(g, 3 - i)
        span = pl.ds((i - 1) * (depth // 2), depth // 2)
        return remote(
            w_all.at[source, span],
            w_all.at[source, span],
            dsend.at[i],
            drecv.at[i],
            peer(target),
            tp,
        )

    for h in range(hret):
        state[h] = jnp.zeros(state.shape[1:], f32)

        def ret_step(b, carry):
            span = pl.ds(pl.multiple_of(b * BLOCK, BLOCK), BLOCK)
            q = rq[h, span, :]
            k = rk[h, span, :]
            v = rv[h, span, :]
            scores = (
                lax.dot_general(q, k, (((1,), (1,)), ((), ())), preferred_element_type=f32)
                * within[h]
            )
            inner = jnp.dot(scores.astype(jnp.bfloat16), v, preferred_element_type=f32)
            held = state[h]
            cross = jnp.dot(q, held.astype(jnp.bfloat16), preferred_element_type=f32)
            raw[h, span, :] = inner + cross * qdec[h, pl.ds(0, BLOCK), :]
            scaled = (k.astype(f32) * kdec[h]).astype(jnp.bfloat16)
            update = lax.dot_general(
                scaled, v, (((0,), (0,)), ((), ())), preferred_element_type=f32
            )
            state[h] = held * bdec[h, 0:1, :] + update
            return carry

        lax.fori_loop(0, run // BLOCK, ret_step, 0)

    def state_hop():
        return remote(state_out, state_in, ssend.at[0], srecv.at[0], after, tp)

    if depth > 1:

        @pl.when(z == 0)
        def _():
            state_out[...] = state[...]
            state_hop().start()

    tile = math.gcd(run, 256)
    inverse = FOX_DIM ** (-0.5)

    def attend(h, t, keys, values, key_gates, diagonal, fresh):
        span = pl.ds(pl.multiple_of(t * tile, tile), tile)
        scores = (
            lax.dot_general(
                fq[h, span, :], keys, (((1,), (1,)), ((), ())), preferred_element_type=f32
            )
            * inverse
        )
        scores = scores + gq[h, span, :] - key_gates
        if diagonal:
            row = lax.broadcasted_iota(jnp.int32, scores.shape, 0)
            col = lax.broadcasted_iota(jnp.int32, scores.shape, 1)
            scores = jnp.where(col <= row, scores, -jnp.inf)
        weights = jnp.exp(scores)
        total = jnp.sum(weights, axis=1, keepdims=True)
        product = jnp.dot(weights.astype(jnp.bfloat16), values, preferred_element_type=f32)
        if fresh:
            numer[h, span, :] = product
            denom[h, span, :] = total
        else:
            numer[h, span, :] += product
            denom[h, span, :] += total

    for h in range(hfox):
        for t in range(run // tile):
            for s in range(t, -1, -1):
                span = pl.ds(s * tile, tile)
                attend(
                    h,
                    t,
                    fkv[0, h, span, :],
                    fkv[1, h, span, :],
                    gk[h, z, :, span],
                    s == t,
                    s == t,
                )

    def carried():
        state_hop().wait_recv()

        @pl.when(z < depth - 1)
        def _():
            for h in range(hret):
                state_out[h] = state_in[h] * bdec[h, 1:2, :] + state[h]
            state_hop().start()

        for h in range(hret):
            held = state_in[h].astype(jnp.bfloat16)

            def cross_step(b, carry):
                span = pl.ds(pl.multiple_of(b * tile, tile), tile)
                cross = jnp.dot(rq[h, span, :], held, preferred_element_type=f32)
                raw[h, span, :] += cross * qdec[h, span, :]
                return carry

            lax.fori_loop(0, run // tile, cross_step, 0)

    def earlier(step, carry):
        @pl.when(step <= z)
        def _():
            block = z - step
            hop(block).wait_recv()

            @pl.when(z < depth - 1)
            def _():
                hop(block).start()

            for h in range(hfox):

                def query_step(t, c):
                    attend(
                        h,
                        t,
                        slots[block, 0, h],
                        slots[block, 1, h],
                        gk[h, block],
                        False,
                        False,
                    )
                    return c

                lax.fori_loop(0, run // tile, query_step, 0)

        return carry

    if depth > 1:
        lax.fori_loop(1, 2, earlier, 0)

        @pl.when(z > 0)
        def _():
            carried()

        if hyper:
            direct[0].wait_recv()
            relay(1).start()
            direct[1].wait_recv()
            relay(2).start()
        lax.fori_loop(2, depth, earlier, 0)
    elif hyper:
        direct[0].wait_recv()
        relay(1).start()
        direct[1].wait_recv()
        relay(2).start()

    rw = hret * RET_DIM
    fw = hfox * FOX_DIM
    for t in range(group):
        span = pl.ds(t * tok, tok)
        for h in range(hret):
            ret_buf[t, :, h * RET_DIM : (h + 1) * RET_DIM] = normalize(raw[h, span, :])
        for h in range(hfox):
            fox_buf[t, :, h * FOX_DIM : (h + 1) * FOX_DIM] = normalize(
                numer[h, span, :] / denom[h, span, :]
            )
    ret_cols = pl.ds(pl.multiple_of(g * rw, 128), rw)
    fox_cols = pl.ds(pl.multiple_of(group * rw + g * fw, 128), fw)
    exchange = []
    for i in range(1, group):
        other = lax.rem(g + i, group)
        for kind, (buf, cols) in enumerate(((ret_buf, ret_cols), (fox_buf, fox_cols))):
            copy = remote(
                buf.at[other],
                mixed.at[:, cols],
                asend.at[kind, i],
                arecv.at[kind, i],
                peer(other),
                tp,
            )
            copy.start()
            exchange.append(copy)
    mixed[:, ret_cols] = ret_buf[g]
    mixed[:, fox_cols] = fox_buf[g]
    for copy in exchange:
        copy.wait_recv()
    mine.wait()
    if hyper:
        relay(1).wait_recv()
        relay(2).wait_recv()
    else:
        for copy in direct:
            copy.wait_recv()

    cols = w_all.shape[3]
    pack = max(1, 128 // cols)
    wide = pack * cols
    for t in range(n_tp):
        left = mixed[t * rows : (t + 1) * rows, :]

        def column(p, carry, left=left, t=t):
            blocks = [
                w_all[lax.rem(p * pack + i, group), (p * pack + i) // group]
                for i in range(pack)
            ]
            right = blocks[0] if pack == 1 else jnp.concatenate(blocks, axis=1)
            product = jnp.dot(left, right, preferred_element_type=f32)
            at = pl.ds(pl.multiple_of(p * wide, wide), wide)
            part[t, :, at] = product.astype(jnp.bfloat16)
            return carry

        lax.fori_loop(0, n_sp // pack, column, 0)
    final = []
    for i in range(1, n_tp):
        other = lax.rem(tp + i, n_tp)
        copy = remote(part.at[other], got.at[i], osend.at[i], orecv.at[i], sp, other)
        copy.start()
        final.append(copy)
    total = part[tp].astype(f32)
    for i in range(1, n_tp):
        final[i - 1].wait_recv()
        total = total + got[i].astype(f32)
    out[...] = total.astype(jnp.bfloat16)

    for copy in final + exchange + direct:
        copy.wait_send()
    if hyper:
        relay(1).wait_send()
        relay(2).wait_send()
    if depth > 1:

        @pl.when(z < depth - 1)
        def _():
            first_hop().wait_send()
            state_hop().wait_send()

            def settle(block, carry):
                @pl.when(block < z)
                def _():
                    hop(block).wait_send()

                return carry

            lax.fori_loop(0, depth, settle, 0)


def mixer(rq, rk, rv, fq, fkv, gq, gk, within, qdec, kdec, bdec, wz, rows, n_sp, n_tp, group):
    depth = n_sp // group
    hret, run, _ = rq.shape
    hfox = fq.shape[0]
    tok = run // group
    out_rows, cols = wz.shape[1:]
    width = n_sp * cols
    vmem = pl.BlockSpec(memory_space=pltpu.VMEM)
    dma = pltpu.SemaphoreType.DMA
    f32 = jnp.float32
    bf16 = jnp.bfloat16
    square = (hret, RET_DIM, RET_DIM)
    return pl.pallas_call(
        functools.partial(mixer_kernel, n_sp, n_tp, group),
        out_shape=jax.ShapeDtypeStruct((rows, width), bf16),
        in_specs=[vmem] * 11 + [pl.BlockSpec(memory_space=pl.ANY)],
        out_specs=vmem,
        scratch_shapes=[
            pltpu.VMEM((group,) + wz.shape, bf16),
            pltpu.VMEM((depth,) + fkv.shape, bf16),
            pltpu.VMEM((hret, run, RET_DIM), f32),
            pltpu.VMEM(square, f32),
            pltpu.VMEM(square, f32),
            pltpu.VMEM(square, f32),
            pltpu.VMEM((hfox, run, FOX_DIM), f32),
            pltpu.VMEM((hfox, run, 1), f32),
            pltpu.VMEM((group, tok, hret * RET_DIM), bf16),
            pltpu.VMEM((group, tok, hfox * FOX_DIM), bf16),
            pltpu.VMEM((tok, out_rows), bf16),
            pltpu.VMEM((n_tp, rows, width), bf16),
            pltpu.VMEM((n_tp, rows, width), bf16),
            dma((1,)),
            dma((depth,)),
            dma((depth,)),
            dma((1,)),
            dma((1,)),
            dma((max(group, 2),)),
            dma((max(group, 2),)),
            dma((3,)),
            dma((3,)),
            dma((2, group)),
            dma((2, group)),
            dma((n_tp,)),
            dma((n_tp,)),
        ],
        compiler_params=pltpu.CompilerParams(
            collective_id=1, has_side_effects=True, vmem_limit_bytes=VMEM_LIMIT
        ),
        name="mixer",
    )(rq, rk, rv, fq, fkv, gq, gk, within, qdec, kdec, bdec, wz)


def fused_kernel(
    n_sp,
    total,
    tok_in,
    gain_in,
    gates_in,
    wr_ref,
    wf_ref,
    w_in,
    out,
    tok_ref,
    gain_ref,
    gates_ref,
    xall,
    w_ret,
    w_fox,
    wrs,
    wret,
    wfox,
    gall,
    ctab,
    stab,
    within,
    qdec,
    kdec,
    rq,
    rk,
    rv,
    fq,
    guest,
    kv,
    raw,
    update,
    state_in,
    state_out,
    carry_state,
    gcol,
    guest_col,
    numer,
    guest_numer,
    num_out,
    num_in,
    den_out,
    den_in,
    part,
    part_in,
    rsum,
    xa,
    yb,
    second_out,
    second_in,
    fox_buf,
    mixed,
    fpart,
    fgot,
    local_sem,
    tsend,
    trecv,
    dsend,
    drecv,
    psend,
    precv,
    gsend,
    grecv,
    asend,
    arecv,
    usend,
    urecv,
    nsend,
    nrecv,
    fsend,
    frecv,
    ksend,
    krecv,
    qsend,
    qrecv,
    ssend,
    srecv,
    osend,
    orecv,
    psum_send,
    psum_recv,
    rsend,
    rrecv,
    esend,
    erecv,
):
    f32 = jnp.float32
    bf16 = jnp.bfloat16
    group = 4
    sp = lax.axis_index("sp")
    tp = lax.axis_index("tp")
    other_core = 1 - tp
    g = lax.rem(sp, group)
    z = sp // group
    depth = n_sp // group
    last = depth - 1
    host = 1
    rows = tok_ref.shape[0]
    tok = 2 * rows
    hret = rq.shape[1]
    hfox = fq.shape[1]
    ret_rows = hret * RET_DIM
    after = lax.rem(sp + group, n_sp)
    before = lax.rem(sp + n_sp - group, n_sp)

    def near(i):
        return lax.bitwise_xor(g, i)

    def peer(i):
        return z * group + near(i)

    barrier = pltpu.get_barrier_semaphore()
    for i in range(1, n_sp):
        pl.semaphore_signal(
            barrier, inc=1, device_id=(lax.rem(sp + i, n_sp), tp), device_id_type=MESH
        )
    pl.semaphore_signal(barrier, inc=1, device_id=(sp, other_core), device_id_type=MESH)

    first = [
        pltpu.make_async_copy(tok_in, tok_ref, local_sem.at[9]),
        pltpu.make_async_copy(gain_in, gain_ref, local_sem.at[10]),
        pltpu.make_async_copy(gates_in, gates_ref, local_sem.at[11]),
    ]
    for copy in first:
        copy.start()
    locals_ = [
        pltpu.make_async_copy(wr_ref, wrs, local_sem.at[0]),
        pltpu.make_async_copy(
            wr_ref.at[pl.ds(pl.multiple_of(g * ret_rows, ret_rows), ret_rows)],
            wret.at[z, 0],
            local_sem.at[1],
        ),
        pltpu.make_async_copy(wf_ref, wfox.at[0, z], local_sem.at[2]),
    ]
    loads = []
    for i in range(6):
        cut = w_ret if i < 3 else w_fox
        size = cut.shape[2]
        columns = pl.ds(pl.multiple_of(g * size, 128), size)
        loads.append(
            pltpu.make_async_copy(
                w_in[i].at[:, columns], cut.at[i % 3], local_sem.at[3 + i]
            )
        )
    for copy in locals_ + loads:
        copy.start()

    for copy in first:
        copy.wait()
    values = tok_ref[...].astype(f32)
    scale = lax.rsqrt(jnp.mean(values * values, axis=1, keepdims=True) + eps)
    xall[0, tp] = (values * scale * gain_ref[...]).astype(bf16)
    gall[sp] = gates_ref[...]
    with jax.named_scope("barrier"):
        pl.semaphore_wait(barrier, n_sp)

    def token_copy(i):
        return remote(xall.at[0, tp], xall.at[i, tp], tsend.at[i], trecv.at[i], peer(i), tp)

    def token_relay(i):
        span = pl.ds((i - 1) * (rows // 2), rows // 2)
        return remote(
            xall.at[i, tp, span],
            xall.at[3, tp, span],
            dsend.at[i],
            drecv.at[i],
            peer(3 - i),
            tp,
        )

    def pair_copy(i):
        return remote(
            xall.at[i, tp], xall.at[i, tp], psend.at[i], precv.at[i], sp, other_core
        )

    def gate_copy(i):
        return remote(
            gates_ref, gall.at[sp], gsend.at[i], grecv.at[i], lax.rem(sp + i, n_sp), tp
        )

    def rows_copy(i):
        span = pl.ds(pl.multiple_of(near(i) * ret_rows, ret_rows), ret_rows)
        return remote(wrs.at[span], wret.at[z, i], asend.at[i], arecv.at[i], peer(i), tp)

    def cut_of(kind, block):
        if kind == 0:
            return wfox.at[0, block]
        if kind == 1:
            return wret.at[block, 0]
        return wret.at[block, pl.ds(1, group - 1)]

    def up(kind, block):
        ref = cut_of(kind, block)
        return remote(ref, ref, usend.at[kind, block], urecv.at[kind, block], after, tp)

    def down(kind, block):
        ref = cut_of(kind, block)
        return remote(ref, ref, nsend.at[kind, block], nrecv.at[kind, block], before, tp)

    def begin_line(kind):
        @pl.when(z < last)
        def _():
            up(kind, z).start()

        @pl.when(z > 0)
        def _():
            down(kind, z).start()

    def line_up(kind, step):
        below = z - step

        @pl.when(below >= 0)
        def _():
            up(kind, below).wait_recv()

            @pl.when(z < last)
            def _():
                up(kind, below).start()

    def line_down(kind, step):
        above = z + step

        @pl.when(above <= last)
        def _():
            down(kind, above).wait_recv()

            @pl.when(z > 0)
            def _():
                down(kind, above).start()

    def line(kind, step):
        line_up(kind, step)
        line_down(kind, step)

    def settle_line(kind):
        for block in range(depth):

            @pl.when((z < last) & (block <= z))
            def _():
                up(kind, block).wait_send()

            @pl.when((z > 0) & (block >= z))
            def _():
                down(kind, block).wait_send()

    def plane_copy(i):
        return remote(wfox.at[0], wfox.at[i], fsend.at[i], frecv.at[i], peer(i), tp)

    def plane_relay(i):
        span = pl.ds(0, depth // 2) if i == 1 else pl.ds(depth // 2, depth - depth // 2)
        return remote(
            wfox.at[i, span],
            wfox.at[3, span],
            fsend.at[2 + i],
            frecv.at[2 + i],
            peer(3 - i),
            tp,
        )

    def kv_hop(block, i):
        ref = kv.at[block, i]
        return remote(ref, ref, ksend.at[block, i], krecv.at[block, i], after, tp)

    def query_hop(k, i):
        there = lax.rem(sp + n_sp - (k + 1) * group, n_sp)
        return remote(fq.at[i], guest.at[k, i], qsend.at[k, i], qrecv.at[k, i], there, tp)

    slices = 4
    slice_rows = RET_DIM // slices

    def state_hop(c):
        span = pl.ds(c * slice_rows, slice_rows)
        return remote(
            state_out.at[:, span], state_in.at[:, span], ssend.at[c], srecv.at[c], after, tp
        )

    guests = depth - 1 - host

    def num_hop(k, i):
        there = lax.rem(sp + (k + 1) * group, n_sp)
        return remote(
            num_out.at[k, i], num_in.at[i], osend.at[k, i], orecv.at[i], there, tp
        )

    def den_hop(k):
        there = lax.rem(sp + (k + 1) * group, n_sp)
        return remote(
            den_out.at[k], den_in, osend.at[k, group], orecv.at[group], there, tp
        )

    def part_copy(i):
        return remote(
            part.at[i, other_core],
            part_in.at[i],
            psum_send.at[i],
            psum_recv.at[i],
            sp,
            other_core,
        )

    width = out.shape[1]
    half = width // 2
    wide = width // depth
    first_cols = pl.ds(0, half)
    last_cols = pl.ds(half, half)

    def scatter_x(k):
        return remote(
            rsum.at[1 + 2 * k, :, first_cols],
            xa.at[k],
            rsend.at[k],
            rrecv.at[k],
            peer(1),
            tp,
        )

    def scatter_y(k):
        return remote(
            rsum.at[2 + k, :, last_cols],
            yb.at[k],
            rsend.at[2 + k],
            rrecv.at[2 + k],
            peer(2),
            tp,
        )

    def scatter_second(k):
        return remote(
            second_out.at[k],
            second_in.at[k],
            rsend.at[4 + k],
            rrecv.at[4 + k],
            peer(2 if k == 0 else 1),
            tp,
        )

    fw = hfox * FOX_DIM
    my_cols = pl.ds(pl.multiple_of(g * fw, 128), fw)

    def mixed_copy(i):
        return remote(
            fox_buf.at[i], mixed.at[:, my_cols], esend.at[i], erecv.at[i], peer(i), tp
        )

    def final_copy():
        return remote(
            fpart.at[other_core], fgot, esend.at[0], erecv.at[0], sp, other_core
        )

    for i in (1, 2):
        token_copy(i).start()
    pair_copy(0).start()
    with jax.named_scope("first_sends"):
        for i in range(1, n_sp):
            gate_copy(i).start()
        for copy in locals_:
            copy.wait()
        for i in range(1, group):
            rows_copy(i).start()
        begin_line(0)
        begin_line(1)

    head_of = [tp * (group * hret) + g * hret + h for h in range(hret)]
    rates = []
    for h in range(hret):
        ids = jnp.full((1, RET_DIM), head_of[h], jnp.int32)
        heads_float = ids.astype(f32)
        middle = RET_HEADS // 2
        fast_rate = 1.0 / (32.0 + 16.0 * heads_float)
        slow_rate = jnp.exp2(-(heads_float - middle)) / total
        rates.append(jnp.where(ids < middle, fast_rate, slow_rate))
    square = (tok, RET_DIM)
    offset = lax.broadcasted_iota(jnp.int32, square, 0)
    column = lax.broadcasted_iota(jnp.int32, (tok, tok), 1)
    row = lax.broadcasted_iota(jnp.int32, (tok, tok), 0)
    for h in range(hret):
        rate = rates[h]
        spread = jnp.maximum(row - column, 0).astype(f32)
        within[h] = jnp.where(row >= column, jnp.exp(-rate[:, :1] * spread), 0.0)
        steps = offset.astype(f32)
        qdec[h] = jnp.exp(-rate * (steps + 1.0))
        kdec[h] = jnp.exp(-rate * (tok - 1.0 - steps))
    half_head = RET_DIM // 2
    index = lax.broadcasted_iota(jnp.int32, (1, half_head), 1).astype(f32)
    inverse_freq = jnp.exp(index * (-math.log(10000.0) / half_head))
    unit = 16
    low = lax.broadcasted_iota(jnp.int32, (unit, RET_DIM // 2), 0).astype(f32)
    high = lax.broadcasted_iota(jnp.int32, (tok // unit, RET_DIM // 2), 0).astype(f32)
    cos_low, sin_low = jnp.cos(low * inverse_freq), jnp.sin(low * inverse_freq)
    high = high * float(unit) * inverse_freq
    cos_high, sin_high = jnp.cos(high), jnp.sin(high)
    for a in range(tok // unit):
        ca, sa = cos_high[a : a + 1], sin_high[a : a + 1]
        ctab[a * unit : (a + 1) * unit] = cos_low * ca - sin_low * sa
        stab[a * unit : (a + 1) * unit] = sin_low * ca + cos_low * sa

    run_decay = [jnp.exp(-rates[h] * float(group * tok)) for h in range(hret)]
    tok_decay = [jnp.exp(-rates[h] * float(tok)) for h in range(hret)]

    def sum_state():
        for h in range(hret):
            held = update[g, h]
            for p in range(1, group):
                held = held * tok_decay[h] + update[near(p), h]
            carry_state[h] = held

        @pl.when(z == 0)
        def _():
            state_out[...] = carry_state[...].astype(bf16)
            for c in range(slices):
                state_hop(c).start()

    def retain(i):
        for h in range(hret):
            q = rq[i, h]
            k = rk[i, h]
            v = rv[i, h]
            scores = (
                lax.dot_general(q, k, (((1,), (1,)), ((), ())), preferred_element_type=f32)
                * within[h]
            )
            raw[i, h] = jnp.dot(scores.astype(bf16), v, preferred_element_type=f32)

    def gather_state(i):
        for h in range(hret):
            scaled = (rk[i, h].astype(f32) * kdec[h]).astype(bf16)
            update[i, h] = lax.dot_general(
                scaled, rv[i, h], (((0,), (0,)), ((), ())), preferred_element_type=f32
            )

    def queries_of(k):
        @pl.when(z == host + 1 + k)
        def _():
            for i in range(1, group):
                query_hop(k, i).start()

    def project(i):
        x = xall[i].reshape(tok, xall.shape[3])
        start = jnp.full((1, half_head), z * (group * tok) + near(i) * tok, jnp.int32)
        turn = start.astype(f32) * inverse_freq
        cos_turn, sin_turn = jnp.cos(turn), jnp.sin(turn)
        for m in (4, 5, 3, 1, 2, 0) if i < 3 else (1, 2, 4, 5, 3, 0):
            cut = w_ret if m < 3 else w_fox
            y = jnp.dot(x, cut[m % 3], preferred_element_type=f32).astype(bf16)
            if m < 2:
                cosine = ctab[...] * cos_turn - stab[...] * sin_turn
                sine = stab[...] * cos_turn + ctab[...] * sin_turn
            for h in range(hret if m < 3 else hfox):
                if m < 2:
                    lo = h * RET_DIM
                    a = y[:, lo : lo + half_head].astype(f32)
                    b = y[:, lo + half_head : lo + RET_DIM].astype(f32)
                    to = rq if m == 0 else rk
                    by = 1.0 if m == 0 else RET_DIM ** (-0.5)
                    to[i, h, :, :half_head] = ((a * cosine - b * sine) * by).astype(bf16)
                    to[i, h, :, half_head:] = ((a * sine + b * cosine) * by).astype(bf16)
                elif m == 2:
                    rv[i, h] = y[:, h * RET_DIM : (h + 1) * RET_DIM]
                elif m == 3:
                    fq[i, h] = y[:, h * FOX_DIM : (h + 1) * FOX_DIM]
                else:
                    kv[z, i, m - 4, h] = y[:, h * FOX_DIM : (h + 1) * FOX_DIM]
            if m == 2:
                gather_state(i)
                if i == 3:
                    sum_state()
            if m == 5:
                if i == 0:

                    @pl.when(z < last)
                    def _():
                        kv_hop(z, 0).start()

                elif i == 3:

                    @pl.when(z == 0)
                    def _():
                        kv_hop(z, 2).start()
                        kv_hop(z, 3).start()

            if m == 3 and i == 0:
                for k in range(guests):

                    @pl.when(z == host + 1 + k)
                    def _(k=k):
                        query_hop(k, 0).start()

    def second_piece():
        @pl.when(z < last - 1)
        def _():
            kv_hop(z, 1).start()

    def late_pieces():
        @pl.when(z < last)
        def _():
            for c in range(slices):
                state_hop(c).wait_send()

        for i in range(1, group):

            @pl.when((z >= (last - 1 if i == 1 else 1)) & (z < last))
            def _():
                kv_hop(z, i).start()

    def phase(name, *steps):
        with jax.named_scope(name):
            for step in steps:
                step[0](*step[1:])

    def wait_loads():
        for copy in loads:
            copy.wait()
        pair_copy(0).wait_recv()

    def tokens_on(i):
        token_copy(i).wait_recv()
        token_relay(i).start()
        pair_copy(i).start()

    def wait_rows():
        for i in range(1, group):
            rows_copy(i).wait_recv()

    def wait_pair(i):
        pair_copy(i).wait_recv()

    def tokens_last():
        for i in (1, 2):
            token_relay(i).wait_recv()
        pair_copy(3).start()

    def begin_plane():
        for i in (1, 2):
            plane_copy(i).start()

    def pass_state():
        @pl.when(z > 0)
        def _():
            for c in range(slices):
                span = slice(c * slice_rows, (c + 1) * slice_rows)
                state_hop(c).wait_recv()

                @pl.when(z < last)
                def _():
                    for h in range(hret):
                        held = state_in[h, span].astype(f32) * run_decay[h] + carry_state[h, span]
                        state_out[h, span] = held.astype(bf16)
                    state_hop(c).start()

            carry_state[...] = state_in[...].astype(f32)

        @pl.when(z == 0)
        def _():
            carry_state[...] = jnp.zeros(carry_state.shape, f32)

    def gate_row(plane, i, h):
        return gall[plane * group + near(i), pl.ds(g * hfox + h, 1), :]

    def spread_columns(line_row, to, i, h):
        for c in range(tok // 128):
            piece = line_row[:, c * 128 : (c + 1) * 128]
            to[i, h, c * 128 : (c + 1) * 128, :] = jnp.broadcast_to(piece, (128, 128)).T

    def gate_columns():
        for i in range(1, n_sp):
            gate_copy(i).wait_recv()
        for h in range(hfox):
            for i in range(group):
                spread_columns(gate_row(z, i, h), gcol, i, h)

        @pl.when(z == host)
        def _():
            for k in range(guests):
                for h in range(hfox):
                    for i in range(group):
                        spread_columns(gate_row(host + 1 + k, i, h), guest_col.at[k], i, h)

    inverse = FOX_DIM ** (-0.5)

    def weigh(q, column_gates, keys, key_gates, mask=None):
        scores = (
            lax.dot_general(q, keys, (((1,), (1,)), ((), ())), preferred_element_type=f32)
            * inverse
        )
        count = keys.shape[0] // 128
        scores = scores + jnp.concatenate([column_gates] * count, axis=1) - key_gates
        if mask is not None:
            scores = jnp.where(mask, scores, -jnp.inf)
        return jnp.exp(scores).astype(bf16)

    def widen(v):
        return jnp.concatenate([v, jnp.ones(v.shape, bf16)], axis=1)

    def own_attention():
        mask = row >= column
        for h in range(hfox):
            for t in range(group):
                it = near(t)
                weights, vals = [], []
                for s in range(t + 1):
                    js = near(s)
                    weights.append(
                        weigh(
                            fq[it, h],
                            gcol[it, h],
                            kv[z, js, 0, h],
                            gall[z * group + s, pl.ds(g * hfox + h, 1), :],
                            mask if s == t else None,
                        )
                    )
                    vals.append(kv[z, js, 1, h])
                w = weights[0] if t == 0 else jnp.concatenate(weights, axis=1)
                v = vals[0] if t == 0 else jnp.concatenate(vals, axis=0)
                numer[it, h] = jnp.dot(w, widen(v), preferred_element_type=f32)

    def attend(block, queries, columns, to, fresh, done=None):
        for h in range(hfox):
            keys = kv[block, :, 0, h].reshape(group * tok, FOX_DIM)
            vals = widen(kv[block, :, 1, h].reshape(group * tok, FOX_DIM))
            key_gates = jnp.concatenate([gate_row(block, i, h) for i in range(group)], axis=1)

            def query_step(p, carry):
                for j in (2 * p, 2 * p + 1):
                    w = weigh(queries[j, h], columns[j, h], keys, key_gates)
                    product = jnp.dot(w, vals, preferred_element_type=f32)
                    if fresh:
                        to[j, h] = product
                    else:
                        to[j, h] += product
                if done is not None and h == hfox - 1:
                    done(2 * p)
                    done(2 * p + 1)
                return carry

            lax.fori_loop(0, group // 2, query_step, 0)

    lines = tok // 128

    def serve(k):
        def hand_back(j):
            for h in range(hfox):
                num_out[k, j, h] = guest_numer[k, j, h, :, :FOX_DIM].astype(bf16)
                for c in range(lines):
                    at = (j * hfox + h) * lines + c
                    den = guest_numer[k, j, h, c * 128 : (c + 1) * 128, FOX_DIM:]
                    den_out[k, pl.ds(at, 1), :] = den.T[0:1]
            num_hop(k, j).start()

        @pl.when(z == host)
        def _():
            for i in range(group):
                query_hop(k, i).wait_recv()
            for block in range(k + 1):
                attend(
                    block,
                    guest.at[k],
                    guest_col.at[k],
                    guest_numer.at[k],
                    block == 0,
                    hand_back if block == k else None,
                )
            den_hop(k).start()

    def take_back():
        den_hop(0).wait_recv()
        for i in range(group):
            num_hop(0, i).wait_recv()
            for h in range(hfox):
                numer[i, h, :, :FOX_DIM] += num_in[i, h].astype(f32)
                for c in range(lines):
                    at = (i * hfox + h) * lines + c
                    den = jnp.broadcast_to(den_in[at : at + 1, :], (128, 128)).T
                    numer[i, h, c * 128 : (c + 1) * 128, FOX_DIM:] += den

    def earlier():
        @pl.when(z > 0)
        def _():
            attend(z - 1, fq, gcol, numer, False)

    def retention_out():
        for h in range(hret):
            held = carry_state[h]
            for p in range(group):
                ip = near(p)
                cross = jnp.dot(rq[ip, h], held.astype(bf16), preferred_element_type=f32)
                full = raw[ip, h] + cross * qdec[h]
                rq[ip, h] = normalize(full)
                if p < group - 1:
                    held = held * tok_decay[h] + update[ip, h]

    def ret_product(*order):
        left = jnp.concatenate(
            [jnp.concatenate([rq[i, h] for i in order], axis=0) for h in range(hret)], axis=1
        )

        def column_step(p, carry):
            right = jnp.concatenate([wret[p, near(e)] for e in range(group)], axis=1)
            product = jnp.dot(left, right, preferred_element_type=f32).astype(bf16)
            at = pl.ds(pl.multiple_of(p * wide, wide), wide)
            for e in range(2 * len(order)):
                part[order[e // 2], e % 2, :, at] = product[e * rows : (e + 1) * rows]
            return carry

        lax.fori_loop(0, depth, column_step, 0)
        for i in order:
            part_copy(i).start()

    def plane_on():
        for i in (1, 2):
            plane_copy(i).wait_recv()
            plane_relay(i).start()

    def take_all():
        @pl.when((z > 0) & (z != host))
        def _():
            for i in range(group):
                kv_hop(z - 1, i).wait_recv()

    def serve_first():
        @pl.when(z == host)
        def _():
            for i in range(group):
                kv_hop(z - 1, i).wait_recv()

        serve(0)

    def serve_rest():
        for k in range(1, guests):
            serve(k)

    def scatter_first(*order):
        for i in order:
            part_copy(i).wait_recv()
            rsum[i] = (part[i, tp].astype(f32) + part_in[i].astype(f32)).astype(bf16)
            if i == 3:
                scatter_x(1).start()
                scatter_y(1).start()
            elif i == 1:
                scatter_x(0).start()
            elif i == 2:
                scatter_y(0).start()

    def scatter_next():
        scatter_x(1).wait_recv()
        scatter_y(1).wait_recv()
        second_out[0] = (rsum[2, :, :half].astype(f32) + xa[1].astype(f32)).astype(bf16)
        second_out[1] = (rsum[1, :, half:].astype(f32) + yb[1].astype(f32)).astype(bf16)
        for k in range(2):
            scatter_second(k).start()

    def guest_sums():
        @pl.when(z > host)
        def _():
            take_back()

    def send_fox():
        for i in range(group):
            for h in range(hfox):
                fox_buf[i, :, h * FOX_DIM : (h + 1) * FOX_DIM] = normalize(
                    numer[i, h, :, :FOX_DIM] / numer[i, h, :, FOX_DIM:]
                )
            if i > 0:
                mixed_copy(i).start()
        mixed[:, my_cols] = fox_buf[0]

    def wait_fox():
        for i in (1, 2):
            plane_relay(i).wait_recv()
        for i in range(1, group):
            mixed_copy(i).wait_recv()

    def fox_out():
        def fox_column(p, carry):
            right = jnp.concatenate([wfox[near(e), p] for e in range(group)], axis=1)
            product = jnp.dot(mixed[...], right, preferred_element_type=f32).astype(bf16)
            at = pl.ds(pl.multiple_of(p * wide, wide), wide)
            fpart[0, :, at] = product[:rows]
            fpart[1, :, at] = product[rows:]
            return carry

        lax.fori_loop(0, depth, fox_column, 0)
        final_copy().start()

    def wait_final():
        scatter_x(0).wait_recv()
        scatter_y(0).wait_recv()
        for k in range(2):
            scatter_second(k).wait_recv()
        final_copy().wait_recv()

    def finish():
        mine = fpart[tp].astype(f32) + fgot[...].astype(f32)
        ret_low = rsum[0, :, :half].astype(f32) + xa[0].astype(f32) + second_in[0].astype(f32)
        ret_high = rsum[0, :, half:].astype(f32) + yb[0].astype(f32) + second_in[1].astype(f32)
        out[:, :half] = (mine[:, :half] + ret_low).astype(bf16)
        out[:, half:] = (mine[:, half:] + ret_high).astype(bf16)

    phase("w_loads", (wait_loads,))
    phase("project0", (project, 0))
    phase("line01", (line, 0, 1), (line, 1, 1))
    phase("retain0", (retain, 0))
    phase("tokens1", (tokens_on, 1))
    phase("tokens2", (tokens_on, 2))
    phase("line02", (line, 0, 2), (line, 1, 2))
    phase("w_pair1", (wait_pair, 1))
    phase("project1", (project, 1))
    phase("w_rows", (wait_rows,), (begin_line, 2), (second_piece,))
    phase("w_pair2", (wait_pair, 2))
    phase("project2", (project, 2))
    for step in range(3, depth):
        phase("line0" + str(step), (line, 0, step), (line, 1, step))
    phase("begin_plane", (begin_plane,))
    phase("retain1", (retain, 1))
    phase("retain2", (retain, 2))
    phase("tokens3", (tokens_last,))
    phase("w_pair3", (wait_pair, 3))
    phase("up21", (line_up, 2, 1))
    phase("down21", (line_down, 2, 1))
    phase("project3", (project, 3))
    upper = z > host

    @pl.when(upper)
    def _():
        phase("retain3", (retain, 3))
        phase("gates", (gate_columns,))
        phase("query0", (queries_of, 0))
        phase("own_attention", (own_attention,))
        phase("up22", (line_up, 2, 2))

    @pl.when(z == last)
    def _():
        phase("plane_on", (plane_on,), (queries_of, 1))

    phase("pass_state", (pass_state,))

    @pl.when(upper & (z < last))
    def _():
        phase("plane_on", (plane_on,))

    @pl.when(z <= host)
    def _():
        phase("down22", (line_down, 2, 2))
        phase("retain3", (retain, 3))
        phase("gates", (gate_columns,))
        phase("own_attention", (own_attention,))
        phase("plane_on", (plane_on,))

    phase("retention_out", (retention_out,))
    phase("late_pieces", (late_pieces,))
    for step in range(3, depth):
        phase("line2" + str(step), (line, 2, step))
    phase("ret_product1", (ret_product, 3, 1))
    phase("ret_product2", (ret_product, 2, 0))
    phase("serve0", (serve_first,))
    phase("scatter1a", (scatter_first, 3, 1))
    phase("scatter1b", (scatter_first, 2, 0))
    phase("serve1", (serve_rest,))
    phase("takes", (take_all,))
    phase("earlier", (earlier,))
    phase("guest_sums", (guest_sums,))
    phase("send_fox", (send_fox,))
    phase("scatter2", (scatter_next,))
    phase("w_fox", (wait_fox,))
    phase("fox_out", (fox_out,))
    phase("w_final", (wait_final,))
    phase("finish", (finish,))

    def settle_all():
        for i in (1, 2):
            token_copy(i).wait_send()
            token_relay(i).wait_send()
            plane_copy(i).wait_send()
            plane_relay(i).wait_send()
        for i in range(group):
            pair_copy(i).wait_send()
            part_copy(i).wait_send()
        for i in range(1, group):
            rows_copy(i).wait_send()
            mixed_copy(i).wait_send()
        for i in range(1, n_sp):
            gate_copy(i).wait_send()
        for kind in range(3):
            settle_line(kind)
        for k in range(2):
            scatter_x(k).wait_send()
            scatter_y(k).wait_send()
            scatter_second(k).wait_send()
        final_copy().wait_send()

        @pl.when(z < last)
        def _():
            for i in range(group):
                kv_hop(z, i).wait_send()

        for k in range(guests):

            @pl.when(z == host + 1 + k)
            def _(k=k):
                for i in range(group):
                    query_hop(k, i).wait_send()

        @pl.when(z == host)
        def _():
            for k in range(guests):
                for i in range(group):
                    num_hop(k, i).wait_send()
                den_hop(k).wait_send()

    phase("settle", (settle_all,))


def fused(tokens, gain, gates, w_ret, w_fox, w_in, hret, hfox, n_sp):
    rows, width = tokens.shape
    group = 4
    tok = 2 * rows
    depth = n_sp // group
    out_cols = n_sp * w_ret.shape[1]
    half = out_cols // 2
    ret_rows = hret * RET_DIM
    fox_rows = group * hfox * FOX_DIM
    vmem = pl.BlockSpec(memory_space=pltpu.VMEM)
    hbm = pl.BlockSpec(memory_space=pltpu.HBM)
    dma = pltpu.SemaphoreType.DMA
    f32 = jnp.float32
    bf16 = jnp.bfloat16
    square = (hret, RET_DIM, RET_DIM)
    heads = (group, hfox, tok, FOX_DIM)
    dens = group * hfox * (tok // 128)
    guests = depth - 2
    total = float(tok * n_sp)

    def body(*refs):
        fused_kernel(n_sp, total, *refs[:5], refs[5:11], *refs[11:])

    V = pltpu.VMEM
    return pl.pallas_call(
        body,
        out_shape=jax.ShapeDtypeStruct((rows, out_cols), bf16),
        in_specs=[hbm] * 11,
        out_specs=vmem,
        scratch_shapes=[
            V(tokens.shape, bf16),
            V(gain.shape, f32),
            V(gates.shape, f32),
            V((group, 2, rows, width), bf16),
            V((3, width, ret_rows), bf16),
            V((3, width, hfox * FOX_DIM), bf16),
            V(w_ret.shape, bf16),
            V((depth, group, ret_rows, w_ret.shape[1]), bf16),
            V((group, depth, fox_rows, w_ret.shape[1]), bf16),
            V((n_sp,) + gates.shape, f32),
            V((tok, RET_DIM // 2), f32),
            V((tok, RET_DIM // 2), f32),
            V((hret, tok, tok), f32),
            V((hret, tok, RET_DIM), f32),
            V((hret, tok, RET_DIM), f32),
            V((group, hret, tok, RET_DIM), bf16),
            V((group, hret, tok, RET_DIM), bf16),
            V((group, hret, tok, RET_DIM), bf16),
            V(heads, bf16),
            V((guests,) + heads, bf16),
            V((depth, group, 2, hfox, tok, FOX_DIM), bf16),
            V((group, hret, tok, RET_DIM), f32),
            V((group,) + square, f32),
            V(square, bf16),
            V(square, bf16),
            V(square, f32),
            V((group, hfox, tok, 128), f32),
            V((guests, group, hfox, tok, 128), f32),
            V((group, hfox, tok, 2 * FOX_DIM), f32),
            V((guests, group, hfox, tok, 2 * FOX_DIM), f32),
            V((guests,) + heads, bf16),
            V(heads, bf16),
            V((guests, dens, 128), f32),
            V((dens, 128), f32),
            V((group, 2, rows, out_cols), bf16),
            V((group, rows, out_cols), bf16),
            V((group, rows, out_cols), bf16),
            V((2, rows, half), bf16),
            V((2, rows, half), bf16),
            V((2, rows, half), bf16),
            V((2, rows, half), bf16),
            V((group, tok, hfox * FOX_DIM), bf16),
            V((tok, fox_rows), bf16),
            V((2, rows, out_cols), bf16),
            V((rows, out_cols), bf16),
            dma((12,)),
            dma((3,)),
            dma((3,)),
            dma((3,)),
            dma((3,)),
            dma((group,)),
            dma((group,)),
            dma((n_sp,)),
            dma((n_sp,)),
            dma((group,)),
            dma((group,)),
            dma((3, depth)),
            dma((3, depth)),
            dma((3, depth)),
            dma((3, depth)),
            dma((5,)),
            dma((5,)),
            dma((depth, group)),
            dma((depth, group)),
            dma((guests, group)),
            dma((guests, group)),
            dma((4,)),
            dma((4,)),
            dma((guests, group + 1)),
            dma((group + 1,)),
            dma((group,)),
            dma((group,)),
            dma((6,)),
            dma((6,)),
            dma((group,)),
            dma((group,)),
        ],
        compiler_params=pltpu.CompilerParams(
            collective_id=2, has_side_effects=True, vmem_limit_bytes=FUSED_LIMIT
        ),
        name="fused",
    )(
        *[
            pltpu.with_memory_space_constraint(array, pltpu.HBM)
            for array in (tokens, gain, gates, w_ret, w_fox, *w_in)
        ]
    )


def decay_rates(head_ids, total):
    heads_float = head_ids.astype(jnp.float32)
    middle = RET_HEADS // 2
    fast_rate = 1.0 / (32.0 + 16.0 * heads_float)
    slow_rate = jnp.exp2(-(heads_float - middle)) / total
    return jnp.where(head_ids < middle, fast_rate, slow_rate)


def per_device(
    n_sp,
    n_tp,
    tokens,
    gain,
    w_ret_q,
    w_ret_k,
    w_ret_v,
    w_fox_q,
    w_fox_k,
    w_fox_v,
    fox_gates,
    w_out_ret,
    w_out_fox,
):
    f32 = jnp.float32
    rows, width = tokens.shape
    ret_heads = w_ret_q.shape[1] // RET_DIM
    fox_heads = w_fox_q.shape[1] // FOX_DIM
    group = math.gcd(math.gcd(ret_heads, fox_heads), n_sp)
    depth = n_sp // group
    hret = ret_heads // group
    hfox = fox_heads // group
    run = rows * n_tp * group
    if group == 4 and n_tp == 2 and depth == 4:
        return fused(
            tokens,
            gain.reshape(1, width),
            fox_gates.T,
            w_out_ret,
            w_out_fox,
            (w_ret_q, w_ret_k, w_ret_v, w_fox_q, w_fox_k, w_fox_v),
            hret,
            hfox,
            n_sp,
        )
    sp = lax.axis_index("sp")
    g = lax.rem(sp, group)
    z = sp // group

    positions = z * run + jnp.arange(run, dtype=jnp.int32)
    half = RET_DIM // 2
    inverse = 10000.0 ** (-jnp.arange(half, dtype=f32) / half)
    angles = positions.astype(f32)[:, None] * inverse[None, :]
    rq, rk, rv, fq, fkv, gall, wz = gather(
        tokens,
        gain.reshape(1, width),
        fox_gates.T,
        w_out_ret,
        w_out_fox,
        jnp.cos(angles),
        jnp.sin(angles),
        (w_ret_q, w_ret_k, w_ret_v, w_fox_q, w_fox_k, w_fox_v),
        hret,
        hfox,
        n_sp,
        n_tp,
        group,
    )

    head_ids = (
        lax.axis_index("tp") * ret_heads + g * hret + jnp.arange(hret, dtype=jnp.int32)
    )
    rates = decay_rates(head_ids, float(run * depth))
    offsets = jnp.arange(BLOCK, dtype=f32)
    spread = offsets[:, None] - offsets[None, :]
    causal = spread >= 0
    within = jnp.where(
        causal[None], jnp.exp(-rates[:, None, None] * jnp.where(causal, spread, 0.0)[None]), 0.0
    )
    steps = jnp.arange(run, dtype=f32)
    qdec = jnp.exp(-rates[:, None] * (steps[None, :] + 1.0))[:, :, None]
    kdec = jnp.exp(-rates[:, None] * (BLOCK - 1.0 - offsets[None, :]))[:, :, None]
    lengths = jnp.array([BLOCK, run], f32)
    bdec = jnp.broadcast_to(
        jnp.exp(-rates[:, None] * lengths[None, :])[:, :, None], (hret, 2, RET_DIM)
    )

    own_gates = lax.dynamic_slice_in_dim(gall, g * hfox, hfox, 1)
    line = own_gates.transpose(1, 0, 2).reshape(hfox, depth, 1, run)
    gq = lax.dynamic_index_in_dim(line, z, 1, False).reshape(hfox, run, 1)
    return mixer(
        rq, rk, rv, fq, fkv, gq, line, within, qdec, kdec, bdec, wz, rows, n_sp, n_tp, group
    )


def solution(mesh):
    in_specs = (
        P(("sp", "tp"), None),
        P(),
        P(None, "tp"),
        P(None, "tp"),
        P(None, "tp"),
        P(None, "tp"),
        P(None, "tp"),
        P(None, "tp"),
        P("sp", "tp"),
        P("tp", "sp"),
        P("tp", "sp"),
    )
    out_specs = P(("sp", "tp"), None)
    return jax.shard_map(
        functools.partial(per_device, mesh.shape["sp"], mesh.shape["tp"]),
        mesh=mesh,
        in_specs=in_specs,
        out_specs=out_specs,
        check_vma=False,
    )
```

```python
import functools
import math

import jax
import jax.numpy as jnp
from jax import lax
from jax.experimental import pallas as pl
from jax.experimental.pallas import tpu as pltpu
from jax.sharding import PartitionSpec as P

RET_HEADS = 8
RET_DIM = 256
FOX_DIM = 128
BLOCK = 128
MESH = pl.DeviceIdType.MESH
VMEM_LIMIT = 60 * 1024 * 1024
FUSED_LIMIT = 52 * 1024 * 1024

eps = 1e-06


def remote(src, dst, send, recv, sp, tp):
    return pltpu.make_async_remote_copy(
        src_ref=src,
        dst_ref=dst,
        send_sem=send,
        recv_sem=recv,
        device_id=(sp, tp),
        device_id_type=MESH,
    )


def gather_kernel(
    n_sp,
    n_tp,
    group,
    tok_ref,
    gain_ref,
    gates_ref,
    wr_ref,
    wf_ref,
    cos_ref,
    sin_ref,
    w_in,
    rq,
    rk,
    rv,
    fq,
    fkv,
    gall,
    wz,
    own,
    xall,
    w_ret,
    w_fox,
    local_sem,
    in_sem,
    tsend,
    trecv,
    dsend,
    drecv,
    psend,
    precv,
    gsend,
    grecv,
    usend,
    urecv,
    nsend,
    nrecv,
):
    sp = lax.axis_index("sp")
    tp = lax.axis_index("tp")
    g = lax.rem(sp, group)
    z = sp // group
    depth = n_sp // group
    rows = tok_ref.shape[0]
    half = rows // 2
    krows = wr_ref.shape[0]

    barrier = pltpu.get_barrier_semaphore()
    for i in range(1, n_sp):
        pl.semaphore_signal(
            barrier, inc=1, device_id=(lax.rem(sp + i, n_sp), tp), device_id_type=MESH
        )
    for i in range(1, n_tp):
        pl.semaphore_signal(
            barrier, inc=1, device_id=(sp, lax.rem(tp + i, n_tp)), device_id_type=MESH
        )

    loads = []
    for i in range(6):
        cut = w_ret if i < 3 else w_fox
        size = cut.shape[2]
        columns = pl.ds(pl.multiple_of(g * size, 128), size)
        loads.append(
            pltpu.make_async_copy(w_in[i].at[:, columns], cut.at[i % 3], in_sem.at[i])
        )

    values = tok_ref[...].astype(jnp.float32)
    scale = lax.rsqrt(jnp.mean(values * values, axis=1, keepdims=True) + eps)
    own[...] = (values * scale * gain_ref[...]).astype(jnp.bfloat16)
    copies = [
        pltpu.make_async_copy(wr_ref, wz.at[z, pl.ds(0, krows)], local_sem.at[0]),
        pltpu.make_async_copy(
            wf_ref, wz.at[z, pl.ds(krows, wf_ref.shape[0])], local_sem.at[1]
        ),
        pltpu.make_async_copy(gates_ref, gall.at[sp], local_sem.at[2]),
    ]
    for copy in copies + loads:
        copy.start()
    pl.semaphore_wait(barrier, n_sp + n_tp - 2)

    def slot(which, core):
        return xall.at[which * n_tp + core]

    mine = pltpu.make_async_copy(own, slot(g, tp), local_sem.at[3])
    mine.start()

    def peer(other):
        return z * group + other

    hyper = group == 4
    direct = []
    for i in range(1, group):
        if hyper and i == 3:
            continue
        other = lax.bitwise_xor(g, i) if hyper else lax.rem(g + i, group)
        direct.append(
            remote(own, slot(g, tp), tsend.at[i], trecv.at[i], peer(other), tp)
        )
    for copy in direct:
        copy.start()
    pair = []
    for i in range(1, n_tp):
        copy = remote(
            own, slot(g, tp), psend.at[0, i], precv.at[0, i], sp, lax.rem(tp + i, n_tp)
        )
        copy.start()
        pair.append(copy)
    gate_copies = []
    for i in range(1, n_sp):
        copy = remote(
            gates_ref, gall.at[sp], gsend.at[i], grecv.at[i], lax.rem(sp + i, n_sp), tp
        )
        copy.start()
        gate_copies.append(copy)

    copies[0].wait()
    copies[1].wait()

    def up(block):
        return remote(
            wz.at[block],
            wz.at[block],
            usend.at[block],
            urecv.at[block],
            lax.rem(sp + group, n_sp),
            tp,
        )

    def down(block):
        return remote(
            wz.at[block],
            wz.at[block],
            nsend.at[block],
            nrecv.at[block],
            lax.rem(sp + n_sp - group, n_sp),
            tp,
        )

    @pl.when(z < depth - 1)
    def _():
        up(z).start()

    @pl.when(z > 0)
    def _():
        down(z).start()

    ready = {0: pair[:]}

    def forward(which, row):
        ready[row] = []
        for i in range(1, n_tp):
            copy = remote(
                slot(which, tp),
                slot(which, tp),
                psend.at[row, i],
                precv.at[row, i],
                sp,
                lax.rem(tp + i, n_tp),
            )
            copy.start()
            pair.append(copy)
            ready[row].append(copy)

    count = n_tp * rows
    half_head = RET_DIM // 2

    def project(which, row):
        for copy in ready[row]:
            copy.wait_recv()
        x = xall[pl.ds(which * n_tp, n_tp)].reshape(count, xall.shape[2])
        span = pl.ds(pl.multiple_of(which * count, count), count)
        for i in range(6):
            cut = w_ret if i < 3 else w_fox
            y = jnp.dot(x, cut[i % 3], preferred_element_type=jnp.float32)
            y = y.astype(jnp.bfloat16)
            if i < 2:
                cosine = cos_ref[span, :]
                sine = sin_ref[span, :]
            for h in range(rq.shape[0] if i < 3 else fq.shape[0]):
                if i < 2:
                    lo = h * RET_DIM
                    a = y[:, lo : lo + half_head].astype(jnp.float32)
                    b = y[:, lo + half_head : lo + RET_DIM].astype(jnp.float32)
                    to = rq if i == 0 else rk
                    by = 1.0 if i == 0 else RET_DIM ** (-0.5)
                    first = (a * cosine - b * sine) * by
                    second = (a * sine + b * cosine) * by
                    to[h, span, :half_head] = first.astype(jnp.bfloat16)
                    to[h, span, half_head:] = second.astype(jnp.bfloat16)
                elif i == 2:
                    rv[h, span, :] = y[:, h * RET_DIM : (h + 1) * RET_DIM]
                elif i == 3:
                    fq[h, span, :] = y[:, h * FOX_DIM : (h + 1) * FOX_DIM]
                else:
                    fkv[i - 4, h, span, :] = y[:, h * FOX_DIM : (h + 1) * FOX_DIM]

    mine.wait()
    for copy in loads:
        copy.wait()
    if not hyper:
        project(g, 0)

    if hyper:
        relays = []
        for i in (1, 2):
            direct[i - 1].wait_recv()
            source = lax.bitwise_xor(g, i)
            target = lax.bitwise_xor(g, 3 - i)
            part = pl.ds((i - 1) * half, half)
            copy = remote(
                slot(source, tp).at[part],
                slot(source, tp).at[part],
                dsend.at[i],
                drecv.at[i],
                peer(target),
                tp,
            )
            copy.start()
            relays.append(copy)
            forward(source, i)
        project(g, 0)
    else:
        for i in range(1, group):
            direct[i - 1].wait_recv()
            forward(lax.rem(g + group - i, group), i)
            project(lax.rem(g + group - i, group), i)

    def line(step, carry):
        below = z - step
        above = z + step

        @pl.when(below >= 0)
        def _():
            up(below).wait_recv()

            @pl.when(z < depth - 1)
            def _():
                up(below).start()

        @pl.when(above <= depth - 1)
        def _():
            down(above).wait_recv()

            @pl.when(z > 0)
            def _():
                down(above).start()

        return carry

    split = depth // 2 if hyper else depth
    lax.fori_loop(1, split, line, 0)
    if hyper:
        project(lax.bitwise_xor(g, 1), 1)
        for copy in relays:
            copy.wait_recv()
        forward(lax.bitwise_xor(g, 3), 3)
    lax.fori_loop(split, depth - 1, line, 0)
    if hyper:
        project(lax.bitwise_xor(g, 2), 2)
        project(lax.bitwise_xor(g, 3), 3)
    lax.fori_loop(max(split, depth - 1), depth, line, 0)

    def settle(step, carry):
        @pl.when((z < depth - 1) & (step <= z))
        def _():
            up(step).wait_send()

        @pl.when((z > 0) & (step >= z))
        def _():
            down(step).wait_send()

        return carry

    lax.fori_loop(0, depth, settle, 0)
    for copy in direct:
        copy.wait_send()
    if hyper:
        for copy in relays:
            copy.wait_send()
    for copy in gate_copies:
        copy.wait()
    for copy in pair:
        copy.wait_send()
    copies[2].wait()


def gather(
    tokens, gain, gates, w_ret, w_fox, cosine, sine, w_in, hret, hfox, n_sp, n_tp, group
):
    rows, width = tokens.shape
    depth = n_sp // group
    out_rows = w_ret.shape[0] + w_fox.shape[0]
    vmem = pl.BlockSpec(memory_space=pltpu.VMEM)
    hbm = pl.BlockSpec(memory_space=pl.ANY)
    dma = pltpu.SemaphoreType.DMA
    run = rows * n_tp * group
    bf16 = jnp.bfloat16

    def body(*refs):
        gather_kernel(n_sp, n_tp, group, *refs[:7], refs[7:13], *refs[13:])

    return pl.pallas_call(
        body,
        out_shape=(
            jax.ShapeDtypeStruct((hret, run, RET_DIM), bf16),
            jax.ShapeDtypeStruct((hret, run, RET_DIM), bf16),
            jax.ShapeDtypeStruct((hret, run, RET_DIM), bf16),
            jax.ShapeDtypeStruct((hfox, run, FOX_DIM), bf16),
            jax.ShapeDtypeStruct((2, hfox, run, FOX_DIM), bf16),
            jax.ShapeDtypeStruct((n_sp,) + gates.shape, jnp.float32),
            jax.ShapeDtypeStruct((depth, out_rows, w_ret.shape[1]), jnp.bfloat16),
        ),
        in_specs=[vmem, vmem, vmem, hbm, hbm, vmem, vmem] + [hbm] * 6,
        out_specs=(vmem,) * 7,
        scratch_shapes=[
            pltpu.VMEM((rows, width), bf16),
            pltpu.VMEM((group * n_tp, rows, width), bf16),
            pltpu.VMEM((3, width, hret * RET_DIM), bf16),
            pltpu.VMEM((3, width, hfox * FOX_DIM), bf16),
            dma((4,)),
            dma((6,)),
            dma((max(group, 2),)),
            dma((max(group, 2),)),
            dma((3,)),
            dma((3,)),
            dma((group, n_tp)),
            dma((group, n_tp)),
            dma((n_sp,)),
            dma((n_sp,)),
            dma((depth,)),
            dma((depth,)),
            dma((depth,)),
            dma((depth,)),
        ],
        compiler_params=pltpu.CompilerParams(
            collective_id=0, has_side_effects=True, vmem_limit_bytes=VMEM_LIMIT
        ),
        name="gather",
    )(tokens, gain, gates, w_ret, w_fox, cosine, sine, *w_in)


def normalize(values):
    return (
        values * lax.rsqrt(jnp.mean(values * values, axis=1, keepdims=True) + eps)
    ).astype(jnp.bfloat16)


def mixer_kernel(
    n_sp,
    n_tp,
    group,
    rq,
    rk,
    rv,
    fq,
    fkv,
    gq,
    gk,
    within,
    qdec,
    kdec,
    bdec,
    wz,
    out,
    w_all,
    slots,
    raw,
    state,
    state_in,
    state_out,
    numer,
    denom,
    ret_buf,
    fox_buf,
    mixed,
    part,
    got,
    local_sem,
    ksend,
    krecv,
    ssend,
    srecv,
    wsend,
    wrecv,
    dsend,
    drecv,
    asend,
    arecv,
    osend,
    orecv,
):
    sp = lax.axis_index("sp")
    tp = lax.axis_index("tp")
    g = lax.rem(sp, group)
    z = sp // group
    depth = n_sp // group
    hret = rq.shape[0]
    hfox = fq.shape[0]
    run = rq.shape[1]
    tok = run // group
    rows = out.shape[0]
    after = lax.rem(sp + group, n_sp)
    before = lax.rem(sp + n_sp - group, n_sp)
    f32 = jnp.float32

    def peer(other):
        return z * group + other

    barrier = pltpu.get_barrier_semaphore()
    for i in range(1, group):
        pl.semaphore_signal(
            barrier, inc=1, device_id=(peer(lax.rem(g + i, group)), tp), device_id_type=MESH
        )
    for i in range(1, n_tp):
        pl.semaphore_signal(
            barrier, inc=1, device_id=(sp, lax.rem(tp + i, n_tp)), device_id_type=MESH
        )
    if depth > 1:

        @pl.when(z < depth - 1)
        def _():
            pl.semaphore_signal(barrier, inc=1, device_id=(after, tp), device_id_type=MESH)

        @pl.when(z > 0)
        def _():
            pl.semaphore_signal(barrier, inc=1, device_id=(before, tp), device_id_type=MESH)

    ends = (z + depth - 1) // depth + (2 * depth - 2 - z) // depth
    pl.semaphore_wait(barrier, group + n_tp - 2 + ends)

    def first_hop():
        return remote(fkv, slots.at[z], ksend.at[z], krecv.at[z], after, tp)

    def hop(block):
        return remote(
            slots.at[block], slots.at[block], ksend.at[block], krecv.at[block], after, tp
        )

    if depth > 1:

        @pl.when(z < depth - 1)
        def _():
            first_hop().start()

    hyper = group == 4
    mine = pltpu.make_async_copy(wz, w_all.at[g], local_sem.at[0])
    mine.start()
    direct = []
    for i in range(1, group):
        if hyper and i == 3:
            continue
        other = lax.bitwise_xor(g, i) if hyper else lax.rem(g + i, group)
        direct.append(
            remote(wz, w_all.at[g], wsend.at[i], wrecv.at[i], peer(other), tp)
        )
    for copy in direct:
        copy.start()

    def relay(i):
        source = lax.bitwise_xor(g, i)
        target = lax.bitwise_xor(g, 3 - i)
        span = pl.ds((i - 1) * (depth // 2), depth // 2)
        return remote(
            w_all.at[source, span],
            w_all.at[source, span],
            dsend.at[i],
            drecv.at[i],
            peer(target),
            tp,
        )

    for h in range(hret):
        state[h] = jnp.zeros(state.shape[1:], f32)

        def ret_step(b, carry):
            span = pl.ds(pl.multiple_of(b * BLOCK, BLOCK), BLOCK)
            q = rq[h, span, :]
            k = rk[h, span, :]
            v = rv[h, span, :]
            scores = (
                lax.dot_general(q, k, (((1,), (1,)), ((), ())), preferred_element_type=f32)
                * within[h]
            )
            inner = jnp.dot(scores.astype(jnp.bfloat16), v, preferred_element_type=f32)
            held = state[h]
            cross = jnp.dot(q, held.astype(jnp.bfloat16), preferred_element_type=f32)
            raw[h, span, :] = inner + cross * qdec[h, pl.ds(0, BLOCK), :]
            scaled = (k.astype(f32) * kdec[h]).astype(jnp.bfloat16)
            update = lax.dot_general(
                scaled, v, (((0,), (0,)), ((), ())), preferred_element_type=f32
            )
            state[h] = held * bdec[h, 0:1, :] + update
            return carry

        lax.fori_loop(0, run // BLOCK, ret_step, 0)

    def state_hop():
        return remote(state_out, state_in, ssend.at[0], srecv.at[0], after, tp)

    if depth > 1:

        @pl.when(z == 0)
        def _():
            state_out[...] = state[...]
            state_hop().start()

    tile = math.gcd(run, 256)
    inverse = FOX_DIM ** (-0.5)

    def attend(h, t, keys, values, key_gates, diagonal, fresh):
        span = pl.ds(pl.multiple_of(t * tile, tile), tile)
        scores = (
            lax.dot_general(
                fq[h, span, :], keys, (((1,), (1,)), ((), ())), preferred_element_type=f32
            )
            * inverse
        )
        scores = scores + gq[h, span, :] - key_gates
        if diagonal:
            row = lax.broadcasted_iota(jnp.int32, scores.shape, 0)
            col = lax.broadcasted_iota(jnp.int32, scores.shape, 1)
            scores = jnp.where(col <= row, scores, -jnp.inf)
        weights = jnp.exp(scores)
        total = jnp.sum(weights, axis=1, keepdims=True)
        product = jnp.dot(weights.astype(jnp.bfloat16), values, preferred_element_type=f32)
        if fresh:
            numer[h, span, :] = product
            denom[h, span, :] = total
        else:
            numer[h, span, :] += product
            denom[h, span, :] += total

    for h in range(hfox):
        for t in range(run // tile):
            for s in range(t, -1, -1):
                span = pl.ds(s * tile, tile)
                attend(
                    h,
                    t,
                    fkv[0, h, span, :],
                    fkv[1, h, span, :],
                    gk[h, z, :, span],
                    s == t,
                    s == t,
                )

    def carried():
        state_hop().wait_recv()

        @pl.when(z < depth - 1)
        def _():
            for h in range(hret):
                state_out[h] = state_in[h] * bdec[h, 1:2, :] + state[h]
            state_hop().start()

        for h in range(hret):
            held = state_in[h].astype(jnp.bfloat16)

            def cross_step(b, carry):
                span = pl.ds(pl.multiple_of(b * tile, tile), tile)
                cross = jnp.dot(rq[h, span, :], held, preferred_element_type=f32)
                raw[h, span, :] += cross * qdec[h, span, :]
                return carry

            lax.fori_loop(0, run // tile, cross_step, 0)

    def earlier(step, carry):
        @pl.when(step <= z)
        def _():
            block = z - step
            hop(block).wait_recv()

            @pl.when(z < depth - 1)
            def _():
                hop(block).start()

            for h in range(hfox):

                def query_step(t, c):
                    attend(
                        h,
                        t,
                        slots[block, 0, h],
                        slots[block, 1, h],
                        gk[h, block],
                        False,
                        False,
                    )
                    return c

                lax.fori_loop(0, run // tile, query_step, 0)

        return carry

    if depth > 1:
        lax.fori_loop(1, 2, earlier, 0)

        @pl.when(z > 0)
        def _():
            carried()

        if hyper:
            direct[0].wait_recv()
            relay(1).start()
            direct[1].wait_recv()
            relay(2).start()
        lax.fori_loop(2, depth, earlier, 0)
    elif hyper:
        direct[0].wait_recv()
        relay(1).start()
        direct[1].wait_recv()
        relay(2).start()

    rw = hret * RET_DIM
    fw = hfox * FOX_DIM
    for t in range(group):
        span = pl.ds(t * tok, tok)
        for h in range(hret):
            ret_buf[t, :, h * RET_DIM : (h + 1) * RET_DIM] = normalize(raw[h, span, :])
        for h in range(hfox):
            fox_buf[t, :, h * FOX_DIM : (h + 1) * FOX_DIM] = normalize(
                numer[h, span, :] / denom[h, span, :]
            )
    ret_cols = pl.ds(pl.multiple_of(g * rw, 128), rw)
    fox_cols = pl.ds(pl.multiple_of(group * rw + g * fw, 128), fw)
    exchange = []
    for i in range(1, group):
        other = lax.rem(g + i, group)
        for kind, (buf, cols) in enumerate(((ret_buf, ret_cols), (fox_buf, fox_cols))):
            copy = remote(
                buf.at[other],
                mixed.at[:, cols],
                asend.at[kind, i],
                arecv.at[kind, i],
                peer(other),
                tp,
            )
            copy.start()
            exchange.append(copy)
    mixed[:, ret_cols] = ret_buf[g]
    mixed[:, fox_cols] = fox_buf[g]
    for copy in exchange:
        copy.wait_recv()
    mine.wait()
    if hyper:
        relay(1).wait_recv()
        relay(2).wait_recv()
    else:
        for copy in direct:
            copy.wait_recv()

    cols = w_all.shape[3]
    pack = max(1, 128 // cols)
    wide = pack * cols
    for t in range(n_tp):
        left = mixed[t * rows : (t + 1) * rows, :]

        def column(p, carry, left=left, t=t):
            blocks = [
                w_all[lax.rem(p * pack + i, group), (p * pack + i) // group]
                for i in range(pack)
            ]
            right = blocks[0] if pack == 1 else jnp.concatenate(blocks, axis=1)
            product = jnp.dot(left, right, preferred_element_type=f32)
            at = pl.ds(pl.multiple_of(p * wide, wide), wide)
            part[t, :, at] = product.astype(jnp.bfloat16)
            return carry

        lax.fori_loop(0, n_sp // pack, column, 0)
    final = []
    for i in range(1, n_tp):
        other = lax.rem(tp + i, n_tp)
        copy = remote(part.at[other], got.at[i], osend.at[i], orecv.at[i], sp, other)
        copy.start()
        final.append(copy)
    total = part[tp].astype(f32)
    for i in range(1, n_tp):
        final[i - 1].wait_recv()
        total = total + got[i].astype(f32)
    out[...] = total.astype(jnp.bfloat16)

    for copy in final + exchange + direct:
        copy.wait_send()
    if hyper:
        relay(1).wait_send()
        relay(2).wait_send()
    if depth > 1:

        @pl.when(z < depth - 1)
        def _():
            first_hop().wait_send()
            state_hop().wait_send()

            def settle(block, carry):
                @pl.when(block < z)
                def _():
                    hop(block).wait_send()

                return carry

            lax.fori_loop(0, depth, settle, 0)


def mixer(rq, rk, rv, fq, fkv, gq, gk, within, qdec, kdec, bdec, wz, rows, n_sp, n_tp, group):
    depth = n_sp // group
    hret, run, _ = rq.shape
    hfox = fq.shape[0]
    tok = run // group
    out_rows, cols = wz.shape[1:]
    width = n_sp * cols
    vmem = pl.BlockSpec(memory_space=pltpu.VMEM)
    dma = pltpu.SemaphoreType.DMA
    f32 = jnp.float32
    bf16 = jnp.bfloat16
    square = (hret, RET_DIM, RET_DIM)
    return pl.pallas_call(
        functools.partial(mixer_kernel, n_sp, n_tp, group),
        out_shape=jax.ShapeDtypeStruct((rows, width), bf16),
        in_specs=[vmem] * 11 + [pl.BlockSpec(memory_space=pl.ANY)],
        out_specs=vmem,
        scratch_shapes=[
            pltpu.VMEM((group,) + wz.shape, bf16),
            pltpu.VMEM((depth,) + fkv.shape, bf16),
            pltpu.VMEM((hret, run, RET_DIM), f32),
            pltpu.VMEM(square, f32),
            pltpu.VMEM(square, f32),
            pltpu.VMEM(square, f32),
            pltpu.VMEM((hfox, run, FOX_DIM), f32),
            pltpu.VMEM((hfox, run, 1), f32),
            pltpu.VMEM((group, tok, hret * RET_DIM), bf16),
            pltpu.VMEM((group, tok, hfox * FOX_DIM), bf16),
            pltpu.VMEM((tok, out_rows), bf16),
            pltpu.VMEM((n_tp, rows, width), bf16),
            pltpu.VMEM((n_tp, rows, width), bf16),
            dma((1,)),
            dma((depth,)),
            dma((depth,)),
            dma((1,)),
            dma((1,)),
            dma((max(group, 2),)),
            dma((max(group, 2),)),
            dma((3,)),
            dma((3,)),
            dma((2, group)),
            dma((2, group)),
            dma((n_tp,)),
            dma((n_tp,)),
        ],
        compiler_params=pltpu.CompilerParams(
            collective_id=1, has_side_effects=True, vmem_limit_bytes=VMEM_LIMIT
        ),
        name="mixer",
    )(rq, rk, rv, fq, fkv, gq, gk, within, qdec, kdec, bdec, wz)


def fused_kernel(
    n_sp,
    total,
    tok_in,
    gain_in,
    gates_in,
    wr_ref,
    wf_ref,
    w_in,
    out,
    tok_ref,
    gain_ref,
    gates_ref,
    xall,
    w_ret,
    w_fox,
    wrs,
    wret,
    wfox,
    gall,
    ctab,
    stab,
    within,
    qdec,
    kdec,
    rq,
    rk,
    rv,
    fq,
    guest,
    kv,
    raw,
    update,
    state_in,
    state_out,
    carry_state,
    gcol,
    guest_col,
    numer,
    guest_numer,
    num_out,
    num_in,
    den_out,
    den_in,
    part,
    part_in,
    rsum,
    xa,
    yb,
    second_out,
    second_in,
    fox_buf,
    mixed,
    fpart,
    fgot,
    local_sem,
    tsend,
    trecv,
    dsend,
    drecv,
    psend,
    precv,
    gsend,
    grecv,
    asend,
    arecv,
    usend,
    urecv,
    nsend,
    nrecv,
    fsend,
    frecv,
    ksend,
    krecv,
    qsend,
    qrecv,
    ssend,
    srecv,
    osend,
    orecv,
    psum_send,
    psum_recv,
    rsend,
    rrecv,
    esend,
    erecv,
):
    f32 = jnp.float32
    bf16 = jnp.bfloat16
    group = 4
    sp = lax.axis_index("sp")
    tp = lax.axis_index("tp")
    other_core = 1 - tp
    g = lax.rem(sp, group)
    z = sp // group
    depth = n_sp // group
    last = depth - 1
    host = 1
    rows = tok_ref.shape[0]
    tok = 2 * rows
    hret = rq.shape[1]
    hfox = fq.shape[1]
    ret_rows = hret * RET_DIM
    after = lax.rem(sp + group, n_sp)
    before = lax.rem(sp + n_sp - group, n_sp)

    def near(i):
        return lax.bitwise_xor(g, i)

    def peer(i):
        return z * group + near(i)

    barrier = pltpu.get_barrier_semaphore()
    for i in range(1, n_sp):
        pl.semaphore_signal(
            barrier, inc=1, device_id=(lax.rem(sp + i, n_sp), tp), device_id_type=MESH
        )
    pl.semaphore_signal(barrier, inc=1, device_id=(sp, other_core), device_id_type=MESH)

    first = [
        pltpu.make_async_copy(tok_in, tok_ref, local_sem.at[9]),
        pltpu.make_async_copy(gain_in, gain_ref, local_sem.at[10]),
        pltpu.make_async_copy(gates_in, gates_ref, local_sem.at[11]),
    ]
    for copy in first:
        copy.start()
    locals_ = [
        pltpu.make_async_copy(wr_ref, wrs, local_sem.at[0]),
        pltpu.make_async_copy(
            wr_ref.at[pl.ds(pl.multiple_of(g * ret_rows, ret_rows), ret_rows)],
            wret.at[z, 0],
            local_sem.at[1],
        ),
        pltpu.make_async_copy(wf_ref, wfox.at[0, z], local_sem.at[2]),
    ]
    loads = []
    for i in range(6):
        cut = w_ret if i < 3 else w_fox
        size = cut.shape[2]
        columns = pl.ds(pl.multiple_of(g * size, 128), size)
        loads.append(
            pltpu.make_async_copy(
                w_in[i].at[:, columns], cut.at[i % 3], local_sem.at[3 + i]
            )
        )
    for copy in locals_ + loads:
        copy.start()

    for copy in first:
        copy.wait()
    values = tok_ref[...].astype(f32)
    scale = lax.rsqrt(jnp.mean(values * values, axis=1, keepdims=True) + eps)
    xall[0, tp] = (values * scale * gain_ref[...]).astype(bf16)
    gall[sp] = gates_ref[...]
    with jax.named_scope("barrier"):
        pl.semaphore_wait(barrier, n_sp)

    def token_copy(i):
        return remote(xall.at[0, tp], xall.at[i, tp], tsend.at[i], trecv.at[i], peer(i), tp)

    def token_relay(i):
        span = pl.ds((i - 1) * (rows // 2), rows // 2)
        return remote(
            xall.at[i, tp, span],
            xall.at[3, tp, span],
            dsend.at[i],
            drecv.at[i],
            peer(3 - i),
            tp,
        )

    def pair_copy(i):
        return remote(
            xall.at[i, tp], xall.at[i, tp], psend.at[i], precv.at[i], sp, other_core
        )

    def gate_copy(i):
        return remote(
            gates_ref, gall.at[sp], gsend.at[i], grecv.at[i], lax.rem(sp + i, n_sp), tp
        )

    def rows_copy(i):
        span = pl.ds(pl.multiple_of(near(i) * ret_rows, ret_rows), ret_rows)
        return remote(wrs.at[span], wret.at[z, i], asend.at[i], arecv.at[i], peer(i), tp)

    def cut_of(kind, block):
        if kind == 0:
            return wfox.at[0, block]
        if kind == 1:
            return wret.at[block, 0]
        return wret.at[block, pl.ds(1, group - 1)]

    def up(kind, block):
        ref = cut_of(kind, block)
        return remote(ref, ref, usend.at[kind, block], urecv.at[kind, block], after, tp)

    def down(kind, block):
        ref = cut_of(kind, block)
        return remote(ref, ref, nsend.at[kind, block], nrecv.at[kind, block], before, tp)

    def begin_line(kind):
        @pl.when(z < last)
        def _():
            up(kind, z).start()

        @pl.when(z > 0)
        def _():
            down(kind, z).start()

    def line_up(kind, step):
        below = z - step

        @pl.when(below >= 0)
        def _():
            up(kind, below).wait_recv()

            @pl.when(z < last)
            def _():
                up(kind, below).start()

    def line_down(kind, step):
        above = z + step

        @pl.when(above <= last)
        def _():
            down(kind, above).wait_recv()

            @pl.when(z > 0)
            def _():
                down(kind, above).start()

    def line(kind, step):
        line_up(kind, step)
        line_down(kind, step)

    def settle_line(kind):
        for block in range(depth):

            @pl.when((z < last) & (block <= z))
            def _():
                up(kind, block).wait_send()

            @pl.when((z > 0) & (block >= z))
            def _():
                down(kind, block).wait_send()

    def plane_copy(i):
        return remote(wfox.at[0], wfox.at[i], fsend.at[i], frecv.at[i], peer(i), tp)

    def plane_relay(i):
        span = pl.ds(0, depth // 2) if i == 1 else pl.ds(depth // 2, depth - depth // 2)
        return remote(
            wfox.at[i, span],
            wfox.at[3, span],
            fsend.at[2 + i],
            frecv.at[2 + i],
            peer(3 - i),
            tp,
        )

    def kv_hop(block, i):
        ref = kv.at[block, i]
        return remote(ref, ref, ksend.at[block, i], krecv.at[block, i], after, tp)

    def query_hop(k, i):
        there = lax.rem(sp + n_sp - (k + 1) * group, n_sp)
        return remote(fq.at[i], guest.at[k, i], qsend.at[k, i], qrecv.at[k, i], there, tp)

    slices = 4
    slice_rows = RET_DIM // slices

    def state_hop(c):
        span = pl.ds(c * slice_rows, slice_rows)
        return remote(
            state_out.at[:, span], state_in.at[:, span], ssend.at[c], srecv.at[c], after, tp
        )

    guests = depth - 1 - host

    def num_hop(k, i):
        there = lax.rem(sp + (k + 1) * group, n_sp)
        return remote(
            num_out.at[k, i], num_in.at[i], osend.at[k, i], orecv.at[i], there, tp
        )

    def den_hop(k):
        there = lax.rem(sp + (k + 1) * group, n_sp)
        return remote(
            den_out.at[k], den_in, osend.at[k, group], orecv.at[group], there, tp
        )

    def part_copy(i):
        return remote(
            part.at[i, other_core],
            part_in.at[i],
            psum_send.at[i],
            psum_recv.at[i],
            sp,
            other_core,
        )

    width = out.shape[1]
    half = width // 2
    wide = width // depth
    first_cols = pl.ds(0, half)
    last_cols = pl.ds(half, half)

    def scatter_x(k):
        return remote(
            rsum.at[1 + 2 * k, :, first_cols],
            xa.at[k],
            rsend.at[k],
            rrecv.at[k],
            peer(1),
            tp,
        )

    def scatter_y(k):
        return remote(
            rsum.at[2 + k, :, last_cols],
            yb.at[k],
            rsend.at[2 + k],
            rrecv.at[2 + k],
            peer(2),
            tp,
        )

    def scatter_second(k):
        return remote(
            second_out.at[k],
            second_in.at[k],
            rsend.at[4 + k],
            rrecv.at[4 + k],
            peer(2 if k == 0 else 1),
            tp,
        )

    fw = hfox * FOX_DIM
    my_cols = pl.ds(pl.multiple_of(g * fw, 128), fw)

    def mixed_copy(i):
        return remote(
            fox_buf.at[i], mixed.at[:, my_cols], esend.at[i], erecv.at[i], peer(i), tp
        )

    def final_copy():
        return remote(
            fpart.at[other_core], fgot, esend.at[0], erecv.at[0], sp, other_core
        )

    for i in (1, 2):
        token_copy(i).start()
    pair_copy(0).start()
    with jax.named_scope("first_sends"):
        for i in range(1, n_sp):
            gate_copy(i).start()
        for copy in locals_:
            copy.wait()
        for i in range(1, group):
            rows_copy(i).start()
        begin_line(0)
        begin_line(1)

    head_of = [tp * (group * hret) + g * hret + h for h in range(hret)]
    rates = []
    for h in range(hret):
        ids = jnp.full((1, RET_DIM), head_of[h], jnp.int32)
        heads_float = ids.astype(f32)
        middle = RET_HEADS // 2
        fast_rate = 1.0 / (32.0 + 16.0 * heads_float)
        slow_rate = jnp.exp2(-(heads_float - middle)) / total
        rates.append(jnp.where(ids < middle, fast_rate, slow_rate))
    square = (tok, RET_DIM)
    offset = lax.broadcasted_iota(jnp.int32, square, 0)
    column = lax.broadcasted_iota(jnp.int32, (tok, tok), 1)
    row = lax.broadcasted_iota(jnp.int32, (tok, tok), 0)
    for h in range(hret):
        rate = rates[h]
        spread = jnp.maximum(row - column, 0).astype(f32)
        within[h] = jnp.where(row >= column, jnp.exp(-rate[:, :1] * spread), 0.0)
        steps = offset.astype(f32)
        qdec[h] = jnp.exp(-rate * (steps + 1.0))
        kdec[h] = jnp.exp(-rate * (tok - 1.0 - steps))
    half_head = RET_DIM // 2
    index = lax.broadcasted_iota(jnp.int32, (1, half_head), 1).astype(f32)
    inverse_freq = jnp.exp(index * (-math.log(10000.0) / half_head))
    unit = 16
    low = lax.broadcasted_iota(jnp.int32, (unit, RET_DIM // 2), 0).astype(f32)
    high = lax.broadcasted_iota(jnp.int32, (tok // unit, RET_DIM // 2), 0).astype(f32)
    cos_low, sin_low = jnp.cos(low * inverse_freq), jnp.sin(low * inverse_freq)
    high = high * float(unit) * inverse_freq
    cos_high, sin_high = jnp.cos(high), jnp.sin(high)
    for a in range(tok // unit):
        ca, sa = cos_high[a : a + 1], sin_high[a : a + 1]
        ctab[a * unit : (a + 1) * unit] = cos_low * ca - sin_low * sa
        stab[a * unit : (a + 1) * unit] = sin_low * ca + cos_low * sa

    run_decay = [jnp.exp(-rates[h] * float(group * tok)) for h in range(hret)]
    tok_decay = [jnp.exp(-rates[h] * float(tok)) for h in range(hret)]

    def sum_state():
        for h in range(hret):
            held = update[g, h]
            for p in range(1, group):
                held = held * tok_decay[h] + update[near(p), h]
            carry_state[h] = held

        @pl.when(z == 0)
        def _():
            state_out[...] = carry_state[...].astype(bf16)
            for c in range(slices):
                state_hop(c).start()

    def retain(i):
        for h in range(hret):
            q = rq[i, h]
            k = rk[i, h]
            v = rv[i, h]
            scores = (
                lax.dot_general(q, k, (((1,), (1,)), ((), ())), preferred_element_type=f32)
                * within[h]
            )
            raw[i, h] = jnp.dot(scores.astype(bf16), v, preferred_element_type=f32)

    def gather_state(i):
        for h in range(hret):
            scaled = (rk[i, h].astype(f32) * kdec[h]).astype(bf16)
            update[i, h] = lax.dot_general(
                scaled, rv[i, h], (((0,), (0,)), ((), ())), preferred_element_type=f32
            )

    def queries_of(k):
        @pl.when(z == host + 1 + k)
        def _():
            for i in range(1, group):
                query_hop(k, i).start()

    def project(i):
        x = xall[i].reshape(tok, xall.shape[3])
        start = jnp.full((1, half_head), z * (group * tok) + near(i) * tok, jnp.int32)
        turn = start.astype(f32) * inverse_freq
        cos_turn, sin_turn = jnp.cos(turn), jnp.sin(turn)
        for m in (4, 5, 3, 1, 2, 0) if i < 3 else (1, 2, 4, 5, 3, 0):
            cut = w_ret if m < 3 else w_fox
            y = jnp.dot(x, cut[m % 3], preferred_element_type=f32).astype(bf16)
            if m < 2:
                cosine = ctab[...] * cos_turn - stab[...] * sin_turn
                sine = stab[...] * cos_turn + ctab[...] * sin_turn
            for h in range(hret if m < 3 else hfox):
                if m < 2:
                    lo = h * RET_DIM
                    a = y[:, lo : lo + half_head].astype(f32)
                    b = y[:, lo + half_head : lo + RET_DIM].astype(f32)
                    to = rq if m == 0 else rk
                    by = 1.0 if m == 0 else RET_DIM ** (-0.5)
                    to[i, h, :, :half_head] = ((a * cosine - b * sine) * by).astype(bf16)
                    to[i, h, :, half_head:] = ((a * sine + b * cosine) * by).astype(bf16)
                elif m == 2:
                    rv[i, h] = y[:, h * RET_DIM : (h + 1) * RET_DIM]
                elif m == 3:
                    fq[i, h] = y[:, h * FOX_DIM : (h + 1) * FOX_DIM]
                else:
                    kv[z, i, m - 4, h] = y[:, h * FOX_DIM : (h + 1) * FOX_DIM]
            if m == 2:
                gather_state(i)
                if i == 3:
                    sum_state()
            if m == 5:
                if i == 0:

                    @pl.when(z < last)
                    def _():
                        kv_hop(z, 0).start()

                elif i == 3:

                    @pl.when(z == 0)
                    def _():
                        kv_hop(z, 2).start()
                        kv_hop(z, 3).start()

            if m == 3 and i == 0:
                for k in range(guests):

                    @pl.when(z == host + 1 + k)
                    def _(k=k):
                        query_hop(k, 0).start()

    def second_piece():
        @pl.when(z < last - 1)
        def _():
            kv_hop(z, 1).start()

    def late_pieces():
        @pl.when(z < last)
        def _():
            for c in range(slices):
                state_hop(c).wait_send()

        for i in range(1, group):

            @pl.when((z >= (last - 1 if i == 1 else 1)) & (z < last))
            def _():
                kv_hop(z, i).start()

    def phase(name, *steps):
        with jax.named_scope(name):
            for step in steps:
                step[0](*step[1:])

    def wait_loads():
        for copy in loads:
            copy.wait()
        pair_copy(0).wait_recv()

    def tokens_on(i):
        token_copy(i).wait_recv()
        token_relay(i).start()
        pair_copy(i).start()

    def wait_rows():
        for i in range(1, group):
            rows_copy(i).wait_recv()

    def wait_pair(i):
        pair_copy(i).wait_recv()

    def tokens_last():
        for i in (1, 2):
            token_relay(i).wait_recv()
        pair_copy(3).start()

    def begin_plane():
        for i in (1, 2):
            plane_copy(i).start()

    def pass_state():
        @pl.when(z > 0)
        def _():
            for c in range(slices):
                span = slice(c * slice_rows, (c + 1) * slice_rows)
                state_hop(c).wait_recv()

                @pl.when(z < last)
                def _():
                    for h in range(hret):
                        held = state_in[h, span].astype(f32) * run_decay[h] + carry_state[h, span]
                        state_out[h, span] = held.astype(bf16)
                    state_hop(c).start()

            carry_state[...] = state_in[...].astype(f32)

        @pl.when(z == 0)
        def _():
            carry_state[...] = jnp.zeros(carry_state.shape, f32)

    def gate_row(plane, i, h):
        return gall[plane * group + near(i), pl.ds(g * hfox + h, 1), :]

    def spread_columns(line_row, to, i, h):
        for c in range(tok // 128):
            piece = line_row[:, c * 128 : (c + 1) * 128]
            to[i, h, c * 128 : (c + 1) * 128, :] = jnp.broadcast_to(piece, (128, 128)).T

    def gate_columns():
        for i in range(1, n_sp):
            gate_copy(i).wait_recv()
        for h in range(hfox):
            for i in range(group):
                spread_columns(gate_row(z, i, h), gcol, i, h)

        @pl.when(z == host)
        def _():
            for k in range(guests):
                for h in range(hfox):
                    for i in range(group):
                        spread_columns(gate_row(host + 1 + k, i, h), guest_col.at[k], i, h)

    inverse = FOX_DIM ** (-0.5)

    def weigh(q, column_gates, keys, key_gates, mask=None):
        scores = (
            lax.dot_general(q, keys, (((1,), (1,)), ((), ())), preferred_element_type=f32)
            * inverse
        )
        count = keys.shape[0] // 128
        scores = scores + jnp.concatenate([column_gates] * count, axis=1) - key_gates
        if mask is not None:
            scores = jnp.where(mask, scores, -jnp.inf)
        return jnp.exp(scores).astype(bf16)

    def widen(v):
        return jnp.concatenate([v, jnp.ones(v.shape, bf16)], axis=1)

    def own_attention():
        mask = row >= column
        for h in range(hfox):
            for t in range(group):
                it = near(t)
                weights, vals = [], []
                for s in range(t + 1):
                    js = near(s)
                    weights.append(
                        weigh(
                            fq[it, h],
                            gcol[it, h],
                            kv[z, js, 0, h],
                            gall[z * group + s, pl.ds(g * hfox + h, 1), :],
                            mask if s == t else None,
                        )
                    )
                    vals.append(kv[z, js, 1, h])
                w = weights[0] if t == 0 else jnp.concatenate(weights, axis=1)
                v = vals[0] if t == 0 else jnp.concatenate(vals, axis=0)
                numer[it, h] = jnp.dot(w, widen(v), preferred_element_type=f32)

    def attend(block, queries, columns, to, fresh, done=None):
        for h in range(hfox):
            keys = kv[block, :, 0, h].reshape(group * tok, FOX_DIM)
            vals = widen(kv[block, :, 1, h].reshape(group * tok, FOX_DIM))
            key_gates = jnp.concatenate([gate_row(block, i, h) for i in range(group)], axis=1)

            def query_step(p, carry):
                for j in (2 * p, 2 * p + 1):
                    w = weigh(queries[j, h], columns[j, h], keys, key_gates)
                    product = jnp.dot(w, vals, preferred_element_type=f32)
                    if fresh:
                        to[j, h] = product
                    else:
                        to[j, h] += product
                if done is not None and h == hfox - 1:
                    done(2 * p)
                    done(2 * p + 1)
                return carry

            lax.fori_loop(0, group // 2, query_step, 0)

    lines = tok // 128

    def serve(k):
        def hand_back(j):
            for h in range(hfox):
                num_out[k, j, h] = guest_numer[k, j, h, :, :FOX_DIM].astype(bf16)
                for c in range(lines):
                    at = (j * hfox + h) * lines + c
                    den = guest_numer[k, j, h, c * 128 : (c + 1) * 128, FOX_DIM:]
                    den_out[k, pl.ds(at, 1), :] = den.T[0:1]
            num_hop(k, j).start()

        @pl.when(z == host)
        def _():
            for i in range(group):
                query_hop(k, i).wait_recv()
            for block in range(k + 1):
                attend(
                    block,
                    guest.at[k],
                    guest_col.at[k],
                    guest_numer.at[k],
                    block == 0,
                    hand_back if block == k else None,
                )
            den_hop(k).start()

    def take_back():
        den_hop(0).wait_recv()
        for i in range(group):
            num_hop(0, i).wait_recv()
            for h in range(hfox):
                numer[i, h, :, :FOX_DIM] += num_in[i, h].astype(f32)
                for c in range(lines):
                    at = (i * hfox + h) * lines + c
                    den = jnp.broadcast_to(den_in[at : at + 1, :], (128, 128)).T
                    numer[i, h, c * 128 : (c + 1) * 128, FOX_DIM:] += den

    def earlier():
        @pl.when(z > 0)
        def _():
            attend(z - 1, fq, gcol, numer, False)

    def retention_out():
        for h in range(hret):
            held = carry_state[h]
            for p in range(group):
                ip = near(p)
                cross = jnp.dot(rq[ip, h], held.astype(bf16), preferred_element_type=f32)
                full = raw[ip, h] + cross * qdec[h]
                rq[ip, h] = normalize(full)
                if p < group - 1:
                    held = held * tok_decay[h] + update[ip, h]

    def ret_product(*order):
        left = jnp.concatenate(
            [jnp.concatenate([rq[i, h] for i in order], axis=0) for h in range(hret)], axis=1
        )

        def column_step(p, carry):
            right = jnp.concatenate([wret[p, near(e)] for e in range(group)], axis=1)
            product = jnp.dot(left, right, preferred_element_type=f32).astype(bf16)
            at = pl.ds(pl.multiple_of(p * wide, wide), wide)
            for e in range(2 * len(order)):
                part[order[e // 2], e % 2, :, at] = product[e * rows : (e + 1) * rows]
            return carry

        lax.fori_loop(0, depth, column_step, 0)
        for i in order:
            part_copy(i).start()

    def plane_on():
        for i in (1, 2):
            plane_copy(i).wait_recv()
            plane_relay(i).start()

    def take_all():
        @pl.when((z > 0) & (z != host))
        def _():
            for i in range(group):
                kv_hop(z - 1, i).wait_recv()

    def serve_first():
        @pl.when(z == host)
        def _():
            for i in range(group):
                kv_hop(z - 1, i).wait_recv()

        serve(0)

    def serve_rest():
        for k in range(1, guests):
            serve(k)

    def scatter_first(*order):
        for i in order:
            part_copy(i).wait_recv()
            rsum[i] = (part[i, tp].astype(f32) + part_in[i].astype(f32)).astype(bf16)
            if i == 3:
                scatter_x(1).start()
                scatter_y(1).start()
            elif i == 1:
                scatter_x(0).start()
            elif i == 2:
                scatter_y(0).start()

    def scatter_next():
        scatter_x(1).wait_recv()
        scatter_y(1).wait_recv()
        second_out[0] = (rsum[2, :, :half].astype(f32) + xa[1].astype(f32)).astype(bf16)
        second_out[1] = (rsum[1, :, half:].astype(f32) + yb[1].astype(f32)).astype(bf16)
        for k in range(2):
            scatter_second(k).start()

    def guest_sums():
        @pl.when(z > host)
        def _():
            take_back()

    def send_fox():
        for i in range(group):
            for h in range(hfox):
                fox_buf[i, :, h * FOX_DIM : (h + 1) * FOX_DIM] = normalize(
                    numer[i, h, :, :FOX_DIM] / numer[i, h, :, FOX_DIM:]
                )
            if i > 0:
                mixed_copy(i).start()
        mixed[:, my_cols] = fox_buf[0]

    def wait_fox():
        for i in (1, 2):
            plane_relay(i).wait_recv()
        for i in range(1, group):
            mixed_copy(i).wait_recv()

    def fox_out():
        def fox_column(p, carry):
            right = jnp.concatenate([wfox[near(e), p] for e in range(group)], axis=1)
            product = jnp.dot(mixed[...], right, preferred_element_type=f32).astype(bf16)
            at = pl.ds(pl.multiple_of(p * wide, wide), wide)
            fpart[0, :, at] = product[:rows]
            fpart[1, :, at] = product[rows:]
            return carry

        lax.fori_loop(0, depth, fox_column, 0)
        final_copy().start()

    def wait_final():
        scatter_x(0).wait_recv()
        scatter_y(0).wait_recv()
        for k in range(2):
            scatter_second(k).wait_recv()
        final_copy().wait_recv()

    def finish():
        mine = fpart[tp].astype(f32) + fgot[...].astype(f32)
        ret_low = rsum[0, :, :half].astype(f32) + xa[0].astype(f32) + second_in[0].astype(f32)
        ret_high = rsum[0, :, half:].astype(f32) + yb[0].astype(f32) + second_in[1].astype(f32)
        out[:, :half] = (mine[:, :half] + ret_low).astype(bf16)
        out[:, half:] = (mine[:, half:] + ret_high).astype(bf16)

    phase("w_loads", (wait_loads,))
    phase("project0", (project, 0))
    phase("line01", (line, 0, 1), (line, 1, 1))
    phase("retain0", (retain, 0))
    phase("tokens1", (tokens_on, 1))
    phase("tokens2", (tokens_on, 2))
    phase("line02", (line, 0, 2), (line, 1, 2))
    phase("w_pair1", (wait_pair, 1))
    phase("project1", (project, 1))
    phase("w_rows", (wait_rows,), (begin_line, 2), (second_piece,))
    phase("w_pair2", (wait_pair, 2))
    phase("project2", (project, 2))
    for step in range(3, depth):
        phase("line0" + str(step), (line, 0, step), (line, 1, step))
    phase("begin_plane", (begin_plane,))
    phase("retain1", (retain, 1))
    phase("retain2", (retain, 2))
    phase("tokens3", (tokens_last,))
    phase("w_pair3", (wait_pair, 3))
    phase("up21", (line_up, 2, 1))
    phase("down21", (line_down, 2, 1))
    phase("project3", (project, 3))
    upper = z > host

    @pl.when(upper)
    def _():
        phase("retain3", (retain, 3))
        phase("gates", (gate_columns,))
        phase("query0", (queries_of, 0))
        phase("own_attention", (own_attention,))
        phase("up22", (line_up, 2, 2))

    @pl.when(z == last)
    def _():
        phase("plane_on", (plane_on,), (queries_of, 1))

    phase("pass_state", (pass_state,))

    @pl.when(upper & (z < last))
    def _():
        phase("plane_on", (plane_on,))

    @pl.when(z <= host)
    def _():
        phase("down22", (line_down, 2, 2))
        phase("retain3", (retain, 3))
        phase("gates", (gate_columns,))
        phase("own_attention", (own_attention,))
        phase("plane_on", (plane_on,))

    phase("retention_out", (retention_out,))
    phase("late_pieces", (late_pieces,))
    for step in range(3, depth):
        phase("line2" + str(step), (line, 2, step))
    phase("ret_product1", (ret_product, 3))
    phase("ret_product2", (ret_product, 1, 2))
    phase("scatter1a", (scatter_first, 3))
    phase("ret_product3", (ret_product, 0))
    phase("serve0", (serve_first,))
    phase("scatter1b", (scatter_first, 1, 2, 0))
    phase("serve1", (serve_rest,))
    phase("takes", (take_all,))
    phase("earlier", (earlier,))
    phase("guest_sums", (guest_sums,))
    phase("send_fox", (send_fox,))
    phase("scatter2", (scatter_next,))
    phase("w_fox", (wait_fox,))
    phase("fox_out", (fox_out,))
    phase("w_final", (wait_final,))
    phase("finish", (finish,))

    def settle_all():
        for i in (1, 2):
            token_copy(i).wait_send()
            token_relay(i).wait_send()
            plane_copy(i).wait_send()
            plane_relay(i).wait_send()
        for i in range(group):
            pair_copy(i).wait_send()
            part_copy(i).wait_send()
        for i in range(1, group):
            rows_copy(i).wait_send()
            mixed_copy(i).wait_send()
        for i in range(1, n_sp):
            gate_copy(i).wait_send()
        for kind in range(3):
            settle_line(kind)
        for k in range(2):
            scatter_x(k).wait_send()
            scatter_y(k).wait_send()
            scatter_second(k).wait_send()
        final_copy().wait_send()

        @pl.when(z < last)
        def _():
            for i in range(group):
                kv_hop(z, i).wait_send()

        for k in range(guests):

            @pl.when(z == host + 1 + k)
            def _(k=k):
                for i in range(group):
                    query_hop(k, i).wait_send()

        @pl.when(z == host)
        def _():
            for k in range(guests):
                for i in range(group):
                    num_hop(k, i).wait_send()
                den_hop(k).wait_send()

    phase("settle", (settle_all,))


def fused(tokens, gain, gates, w_ret, w_fox, w_in, hret, hfox, n_sp):
    rows, width = tokens.shape
    group = 4
    tok = 2 * rows
    depth = n_sp // group
    out_cols = n_sp * w_ret.shape[1]
    half = out_cols // 2
    ret_rows = hret * RET_DIM
    fox_rows = group * hfox * FOX_DIM
    vmem = pl.BlockSpec(memory_space=pltpu.VMEM)
    hbm = pl.BlockSpec(memory_space=pltpu.HBM)
    dma = pltpu.SemaphoreType.DMA
    f32 = jnp.float32
    bf16 = jnp.bfloat16
    square = (hret, RET_DIM, RET_DIM)
    heads = (group, hfox, tok, FOX_DIM)
    dens = group * hfox * (tok // 128)
    guests = depth - 2
    total = float(tok * n_sp)

    def body(*refs):
        fused_kernel(n_sp, total, *refs[:5], refs[5:11], *refs[11:])

    V = pltpu.VMEM
    return pl.pallas_call(
        body,
        out_shape=jax.ShapeDtypeStruct((rows, out_cols), bf16),
        in_specs=[hbm] * 11,
        out_specs=vmem,
        scratch_shapes=[
            V(tokens.shape, bf16),
            V(gain.shape, f32),
            V(gates.shape, f32),
            V((group, 2, rows, width), bf16),
            V((3, width, ret_rows), bf16),
            V((3, width, hfox * FOX_DIM), bf16),
            V(w_ret.shape, bf16),
            V((depth, group, ret_rows, w_ret.shape[1]), bf16),
            V((group, depth, fox_rows, w_ret.shape[1]), bf16),
            V((n_sp,) + gates.shape, f32),
            V((tok, RET_DIM // 2), f32),
            V((tok, RET_DIM // 2), f32),
            V((hret, tok, tok), f32),
            V((hret, tok, RET_DIM), f32),
            V((hret, tok, RET_DIM), f32),
            V((group, hret, tok, RET_DIM), bf16),
            V((group, hret, tok, RET_DIM), bf16),
            V((group, hret, tok, RET_DIM), bf16),
            V(heads, bf16),
            V((guests,) + heads, bf16),
            V((depth, group, 2, hfox, tok, FOX_DIM), bf16),
            V((group, hret, tok, RET_DIM), f32),
            V((group,) + square, f32),
            V(square, bf16),
            V(square, bf16),
            V(square, f32),
            V((group, hfox, tok, 128), f32),
            V((guests, group, hfox, tok, 128), f32),
            V((group, hfox, tok, 2 * FOX_DIM), f32),
            V((guests, group, hfox, tok, 2 * FOX_DIM), f32),
            V((guests,) + heads, bf16),
            V(heads, bf16),
            V((guests, dens, 128), f32),
            V((dens, 128), f32),
            V((group, 2, rows, out_cols), bf16),
            V((group, rows, out_cols), bf16),
            V((group, rows, out_cols), bf16),
            V((2, rows, half), bf16),
            V((2, rows, half), bf16),
            V((2, rows, half), bf16),
            V((2, rows, half), bf16),
            V((group, tok, hfox * FOX_DIM), bf16),
            V((tok, fox_rows), bf16),
            V((2, rows, out_cols), bf16),
            V((rows, out_cols), bf16),
            dma((12,)),
            dma((3,)),
            dma((3,)),
            dma((3,)),
            dma((3,)),
            dma((group,)),
            dma((group,)),
            dma((n_sp,)),
            dma((n_sp,)),
            dma((group,)),
            dma((group,)),
            dma((3, depth)),
            dma((3, depth)),
            dma((3, depth)),
            dma((3, depth)),
            dma((5,)),
            dma((5,)),
            dma((depth, group)),
            dma((depth, group)),
            dma((guests, group)),
            dma((guests, group)),
            dma((4,)),
            dma((4,)),
            dma((guests, group + 1)),
            dma((group + 1,)),
            dma((group,)),
            dma((group,)),
            dma((6,)),
            dma((6,)),
            dma((group,)),
            dma((group,)),
        ],
        compiler_params=pltpu.CompilerParams(
            collective_id=2, has_side_effects=True, vmem_limit_bytes=FUSED_LIMIT
        ),
        name="fused",
    )(
        *[
            pltpu.with_memory_space_constraint(array, pltpu.HBM)
            for array in (tokens, gain, gates, w_ret, w_fox, *w_in)
        ]
    )


def decay_rates(head_ids, total):
    heads_float = head_ids.astype(jnp.float32)
    middle = RET_HEADS // 2
    fast_rate = 1.0 / (32.0 + 16.0 * heads_float)
    slow_rate = jnp.exp2(-(heads_float - middle)) / total
    return jnp.where(head_ids < middle, fast_rate, slow_rate)


def per_device(
    n_sp,
    n_tp,
    tokens,
    gain,
    w_ret_q,
    w_ret_k,
    w_ret_v,
    w_fox_q,
    w_fox_k,
    w_fox_v,
    fox_gates,
    w_out_ret,
    w_out_fox,
):
    f32 = jnp.float32
    rows, width = tokens.shape
    ret_heads = w_ret_q.shape[1] // RET_DIM
    fox_heads = w_fox_q.shape[1] // FOX_DIM
    group = math.gcd(math.gcd(ret_heads, fox_heads), n_sp)
    depth = n_sp // group
    hret = ret_heads // group
    hfox = fox_heads // group
    run = rows * n_tp * group
    if group == 4 and n_tp == 2 and depth == 4:
        return fused(
            tokens,
            gain.reshape(1, width),
            fox_gates.T,
            w_out_ret,
            w_out_fox,
            (w_ret_q, w_ret_k, w_ret_v, w_fox_q, w_fox_k, w_fox_v),
            hret,
            hfox,
            n_sp,
        )
    sp = lax.axis_index("sp")
    g = lax.rem(sp, group)
    z = sp // group

    positions = z * run + jnp.arange(run, dtype=jnp.int32)
    half = RET_DIM // 2
    inverse = 10000.0 ** (-jnp.arange(half, dtype=f32) / half)
    angles = positions.astype(f32)[:, None] * inverse[None, :]
    rq, rk, rv, fq, fkv, gall, wz = gather(
        tokens,
        gain.reshape(1, width),
        fox_gates.T,
        w_out_ret,
        w_out_fox,
        jnp.cos(angles),
        jnp.sin(angles),
        (w_ret_q, w_ret_k, w_ret_v, w_fox_q, w_fox_k, w_fox_v),
        hret,
        hfox,
        n_sp,
        n_tp,
        group,
    )

    head_ids = (
        lax.axis_index("tp") * ret_heads + g * hret + jnp.arange(hret, dtype=jnp.int32)
    )
    rates = decay_rates(head_ids, float(run * depth))
    offsets = jnp.arange(BLOCK, dtype=f32)
    spread = offsets[:, None] - offsets[None, :]
    causal = spread >= 0
    within = jnp.where(
        causal[None], jnp.exp(-rates[:, None, None] * jnp.where(causal, spread, 0.0)[None]), 0.0
    )
    steps = jnp.arange(run, dtype=f32)
    qdec = jnp.exp(-rates[:, None] * (steps[None, :] + 1.0))[:, :, None]
    kdec = jnp.exp(-rates[:, None] * (BLOCK - 1.0 - offsets[None, :]))[:, :, None]
    lengths = jnp.array([BLOCK, run], f32)
    bdec = jnp.broadcast_to(
        jnp.exp(-rates[:, None] * lengths[None, :])[:, :, None], (hret, 2, RET_DIM)
    )

    own_gates = lax.dynamic_slice_in_dim(gall, g * hfox, hfox, 1)
    line = own_gates.transpose(1, 0, 2).reshape(hfox, depth, 1, run)
    gq = lax.dynamic_index_in_dim(line, z, 1, False).reshape(hfox, run, 1)
    return mixer(
        rq, rk, rv, fq, fkv, gq, line, within, qdec, kdec, bdec, wz, rows, n_sp, n_tp, group
    )


def solution(mesh):
    in_specs = (
        P(("sp", "tp"), None),
        P(),
        P(None, "tp"),
        P(None, "tp"),
        P(None, "tp"),
        P(None, "tp"),
        P(None, "tp"),
        P(None, "tp"),
        P("sp", "tp"),
        P("tp", "sp"),
        P("tp", "sp"),
    )
    out_specs = P(("sp", "tp"), None)
    return jax.shard_map(
        functools.partial(per_device, mesh.shape["sp"], mesh.shape["tp"]),
        mesh=mesh,
        in_specs=in_specs,
        out_specs=out_specs,
        check_vma=False,
    )
```
